256 devices in a mesh: sp: 64 (over z, x, core), tp: 4 (over y).
Axes of the slice: x: 4, y: 4, z: 8, core: 2. Of those that a mesh axis runs over, the one named last changes fastest.
Arguments:
- tokens: bfloat16 [16384, 1024], P(('sp', 'tp')), may hold values from -6 to 6
- norm_gain: float32 [1024], replicated, may hold values from 0.1 to 1.9
- w_query: bfloat16 [1024, 1024], P('sp', 'tp'), may hold values from -0.1875 to 0.1875
- w_key: bfloat16 [1024, 1024], P('sp', 'tp'), may hold values from -0.1875 to 0.1875
- w_value: bfloat16 [1024, 1024], P('sp', 'tp'), may hold values from -0.1875 to 0.1875
- w_forget: bfloat16 [1024, 16], P('sp', 'tp'), may hold values from -0.375 to 0.375
- forget_offset: float32 [16], P('tp'), may hold values from 1 to 3.5
- w_out_t: bfloat16 [1024, 1024], P('sp', 'tp'), may hold values from -0.1875 to 0.1875
- out_gain: float32 [1024], replicated, may hold values from 0.1 to 1.9
Outputs:
- mixed: bfloat16 [16384, 1024], P(('sp', 'tp'))
The draws below stay inside these ranges and needn't reach their ends.
All inputs are finite; a program needn't handle non-finite values.
Results may differ from the reference program's by a relative error of at most 0.015.
Values may be sent and summed in bfloat16 or wider, within the bound.
No kernel may reach another device: no remote copies, remote signals or barrier semaphores. Data moves between devices by JAX's collectives and lax.ppermute only.
A program may use at most 192 MiB of HBM per device.

```python
import jax
import jax.numpy as jnp
from jax import lax

D = 1024
HEADS = 16
HEAD_DIM = 64
TOK_DEV = 256
TOKENS = 16384
N_SP = 64


def block_scale(key, dims, split, smallest, top_value):
    def one(axis_at, blocks):
        draws = jax.random.uniform(jax.random.fold_in(jax.random.fold_in(key, 6), axis_at), (blocks,), jnp.float32, smallest / len(split), top_value / len(split))
        return jnp.repeat(jnp.exp(draws), dims[axis_at] // blocks).reshape((-1,) + (1,) * (len(dims) - axis_at - 1))

    loudness = one(*split[0])
    for cut in split[1:]:
        loudness = loudness * one(*cut)
    return loudness


def gaussian(rng, shape, spread, limit, shards=(), kind=jnp.bfloat16):
    drawn = jax.random.normal(rng, shape, jnp.float32) * spread
    if len(shards) > 0:
        drawn = block_scale(rng, shape, shards, -0.22, 0.18) * drawn
    return jnp.clip(drawn, min=-limit, max=limit).astype(kind)


def setup_inputs(seed: int = 0) -> dict:
    streams_of = jax.random.split(jax.random.key(seed), 10)
    tokens = gaussian(streams_of[0], (TOKENS, D), 1.0, 6.0, ((0, 256),))
    norm_gain = jnp.clip(1.0 + 0.18 * jax.random.normal(streams_of[1], (D,), jnp.float32), 0.1, 1.9)
    w_query = gaussian(streams_of[2], (D, HEADS * HEAD_DIM), D ** -0.5, 0.1875, ((0, 64), (1, 4)))
    w_key = gaussian(streams_of[3], (D, HEADS * HEAD_DIM), D ** -0.5, 0.1875, ((0, 64), (1, 4)))
    w_value = gaussian(streams_of[4], (D, HEADS * HEAD_DIM), D ** -0.5, 0.1875, ((0, 64), (1, 4)))
    w_forget = gaussian(streams_of[5], (D, HEADS), (D // 4) ** -0.5, 0.375, ((0, 64), (1, 4)))
    forget_offset = jnp.clip(1.0 + 2.5 * jax.random.uniform(streams_of[6], (HEADS,), jnp.float32) ** block_scale(streams_of[6], (HEADS,), ((0, 4),), -0.2, 0.2), 1.0, 3.5)
    w_out_t = gaussian(streams_of[7], (D, HEADS * HEAD_DIM), (HEADS * HEAD_DIM) ** -0.5, 0.1875, ((0, 64), (1, 4)))
    out_gain = jnp.clip(1.0 + 0.18 * jax.random.normal(streams_of[8], (D,), jnp.float32), 0.1, 1.9)
    return {"tokens": tokens, "norm_gain": norm_gain, "w_query": w_query, "w_key": w_key, "w_value": w_value, "w_forget": w_forget, "forget_offset": forget_offset, "w_out_t": w_out_t, "out_gain": out_gain}


norm_eps = 1e-06

def rms_norm(values_in, gain_row):
    floats = values_in.astype(jnp.float32)
    scale_row = lax.rsqrt(lax.optimization_barrier(jnp.mean(floats * floats, axis=-1, keepdims=True)) + norm_eps)
    return (floats * scale_row * gain_row).astype(jnp.bfloat16)

def reference(tokens, norm_gain, w_query, w_key, w_value, w_forget, forget_offset, w_out_t, out_gain):
    normed = rms_norm(tokens, norm_gain)
    queries = jnp.dot(normed, w_query, preferred_element_type=jnp.float32).astype(jnp.bfloat16)
    keys_all = jnp.dot(normed, w_key, preferred_element_type=jnp.float32).astype(jnp.bfloat16)
    values_all = jnp.dot(normed, w_value, preferred_element_type=jnp.float32).astype(jnp.bfloat16)
    logits = jnp.dot(normed, w_forget, preferred_element_type=jnp.float32) + forget_offset + jnp.log(jnp.float32(TOKENS))
    log_gates = jax.nn.log_sigmoid(logits)
    cumulative = jnp.cumsum(log_gates, axis=0)
    head_shape = (TOKENS, HEADS, HEAD_DIM)
    key_heads = keys_all.reshape(head_shape).astype(jnp.float32)
    value_heads = values_all.reshape(head_shape).astype(jnp.float32)
    query_blocks = queries.reshape(N_SP, TOK_DEV, HEADS, HEAD_DIM).astype(jnp.float32)
    cum_blocks = cumulative.reshape(N_SP, TOK_DEV, HEADS)
    key_pos = jnp.arange(TOKENS, dtype=jnp.int32)

    def attend(block_args):
        query_block, cum_block, block_index = block_args
        scores = jnp.einsum('qhd,khd->hqk', query_block, key_heads, precision=lax.Precision.HIGHEST) * HEAD_DIM ** (-0.5)
        scores = scores + cum_block.T[:, :, None] - cumulative.T[:, None, :]
        query_pos = block_index * TOK_DEV + jnp.arange(TOK_DEV, dtype=jnp.int32)
        allowed = key_pos[None, :] <= query_pos[:, None]
        scores = jnp.where(allowed[None], scores, -jnp.inf)
        attn_probs = jax.nn.softmax(scores, axis=-1)
        return jnp.einsum('hqk,khd->qhd', attn_probs, value_heads, precision=lax.Precision.HIGHEST)
    attended = lax.map(attend, (query_blocks, cum_blocks, jnp.arange(N_SP, dtype=jnp.int32)))
    attended = attended.reshape(TOKENS, HEADS * HEAD_DIM).astype(jnp.bfloat16)
    projected = lax.dot_general(attended, w_out_t, (((1,), (1,)), ((), ())), preferred_element_type=jnp.float32)
    return rms_norm(projected, out_gain)
```

```python
import functools
import math

import jax
import jax.numpy as jnp
from jax import lax
from jax.experimental import pallas as pl
from jax.experimental.pallas import tpu as pltpu
from jax.sharding import Mesh
from jax.sharding import PartitionSpec as P

AXES = ("z", "x", "c", "y")
NZ, NX, NC, NY = 8, 4, 2, 4
SIZES = {"z": NZ, "x": NX, "c": NC, "y": NY}
D = 1024
HD = 64
TOTAL = 16384
OWN = 64
BLK = 256
KEYS = 1024
QS = 2048
PAY = 144
EPS = 1e-06
LOW = -1e30
F32 = jnp.float32
BF16 = jnp.bfloat16


VMEM = pl.BlockSpec(memory_space=pltpu.VMEM)
SMEM = pl.BlockSpec(memory_space=pltpu.SMEM)


def call(body, name, outs, ins, scratch=(), flops=1e8):
    return pl.pallas_call(
        body,
        name=name,
        out_shape=outs,
        in_specs=ins,
        out_specs=jax.tree.map(lambda _: VMEM, outs),
        scratch_shapes=list(scratch),
        cost_estimate=pl.CostEstimate(
            flops=int(flops), bytes_accessed=1 << 20, transcendentals=0
        ),
        compiler_params=pltpu.CompilerParams(vmem_limit_bytes=24 << 20),
    )


def shift(x, axis, k):
    n = SIZES[axis]
    return lax.ppermute(x, axis, [(i, (i + k) % n) for i in range(n)])


def direct(x, axis):
    return [x] + [shift(x, axis, k) for k in range(1, SIZES[axis])]


def three_parts(x):
    hi = x.astype(BF16)
    rest = x - hi.astype(F32)
    mid = rest.astype(BF16)
    low = (rest - mid.astype(F32)).astype(BF16)
    return hi, mid, low


def project_body(idx, offs, *refs):
    toks = refs[:8]
    gain, w_own, w_sib = refs[8:11]
    q_out, kv_out, cum_out = refs[11:14]
    w, rows = refs[14:]
    x, c, y = idx[1], idx[2], idx[3]
    for z in range(NZ):
        for xx in range(NX):
            base = z * 128 + xx * 32
            own_at = pl.multiple_of(base + c * 16, 16)
            sib_at = pl.multiple_of(base + (1 - c) * 16, 16)
            w[pl.ds(own_at, 16), :] = w_own[z, xx * 16 : xx * 16 + 16, :]
            w[pl.ds(sib_at, 16), :] = w_sib[z, xx * 16 : xx * 16 + 16, :]
    for half in range(2):
        for outer in range(4):
            tok = toks[half * 4 + outer][...].astype(F32)
            scale = lax.rsqrt(jnp.mean(tok * tok, axis=-1, keepdims=True) + EPS)
            normed = (tok * scale * gain[...]).astype(BF16)
            out = jnp.dot(normed, w[...], preferred_element_type=F32)
            for inner in range(4):
                kx, ky = (outer, inner) if half == 0 else (inner, outer)
                xx = lax.rem(x - kx + NX, NX)
                yy = lax.rem(y - ky + NY, NY)
                at = pl.multiple_of(xx * BLK + yy * OWN + half * 32, 32)
                rows[pl.ds(at, 32), :] = out[inner * 32 : inner * 32 + 32, :]
    before = lax.broadcasted_iota(jnp.int32, (BLK, BLK), 0)
    after = lax.broadcasted_iota(jnp.int32, (BLK, BLK), 1)
    ones = jnp.where(before <= after, 1.0, 0.0).astype(BF16)
    for b in range(4):
        t = rows[b * BLK : (b + 1) * BLK, :].T
        lanes = slice(b * BLK, (b + 1) * BLK)
        q_out[:, lanes] = t[:64].astype(BF16)
        kv_out[:, lanes] = t[64:192].astype(BF16)
        logit = t[192:200] + offs[x] + math.log(TOTAL)
        gate = jnp.minimum(logit, 0.0) - jnp.log1p(jnp.exp(-jnp.abs(logit)))
        hi, mid, low = three_parts(gate)
        cum = jnp.dot(hi, ones, preferred_element_type=F32)
        cum = cum + jnp.dot(mid, ones, preferred_element_type=F32)
        cum = cum + jnp.dot(low, ones, preferred_element_type=F32)
        cum_out[:, lanes] = cum


def prepare_body(idx, q_own, q_sib, kv, cum_own, cum_sib, q_out, pay_out):
    c = idx[2]
    q_out[80:128, :] = jnp.zeros((48, QS), BF16)
    row = lax.broadcasted_iota(jnp.int32, (16, QS), 0)
    q_out[64:80, :] = jnp.where(row < 3, 1.0, 0.0).astype(BF16)
    for b in range(4):
        lanes = slice(b * BLK, (b + 1) * BLK)
        own_at = pl.multiple_of((2 * b + c) * BLK, BLK)
        sib_at = pl.multiple_of((2 * b + 1 - c) * BLK, BLK)
        q_out[0:64, pl.ds(own_at, BLK)] = q_own[:, lanes] * jnp.asarray(0.125, BF16)
        q_out[0:64, pl.ds(sib_at, BLK)] = q_sib[:, lanes] * jnp.asarray(0.125, BF16)
    own = [cum_own[:, b * BLK + BLK - 1 : b * BLK + BLK] for b in range(4)]
    sib = [cum_sib[:, b * BLK + BLK - 1 : b * BLK + BLK] for b in range(4)]
    ahead = jnp.zeros_like(own[0])
    bases = []
    for b in range(4):
        bases.append(ahead + jnp.where(c == 1, sib[b], 0.0))
        ahead = ahead + (own[b] + sib[b])
    total = ahead
    pay_out[0:64, :] = kv[0:64, :]
    pay_out[80:144, :] = kv[64:128, :]
    row = lax.broadcasted_iota(jnp.int32, (16, BLK), 0)
    for b in range(4):
        lanes = slice(b * BLK, (b + 1) * BLK)
        bias = (total - bases[b]) - cum_own[:, lanes]
        parts = [p[0:1].astype(F32) for p in three_parts(bias)]
        totals = [p[0:1].astype(F32) for p in three_parts(jnp.broadcast_to(total, bias.shape))]
        block = jnp.zeros((16, BLK), F32)
        for i, part in enumerate(parts + totals):
            block = jnp.where(row == i, part, block)
        pay_out[64:80, lanes] = block.astype(BF16)


def chunk_total(pay):
    rows = pay[64:80, 0:BLK].astype(F32)
    return rows[3:4] + rows[4:5] + rows[5:6]


def absorb(pay, q, acc, m, kx, vx, move, masked, c):
    fill = jnp.zeros((48, 128), F32)
    for r in range(8):
        lanes = slice(r * 128, (r + 1) * 128)
        tile = jnp.concatenate([pay[0:80, lanes].astype(F32), fill], axis=0)
        kx[lanes, :] = tile.T.astype(BF16)
    vx[0:64, :] = pay[80:144, :]
    vx[64:80, :] = jnp.ones((16, KEYS), BF16)
    if masked:
        key = lax.broadcasted_iota(jnp.int32, (KEYS, BLK), 0)
        key_pos = key + (key // BLK + c) * BLK
        query = lax.broadcasted_iota(jnp.int32, (KEYS, BLK), 1)

    def tile_step(b, carry):
        lanes = pl.ds(pl.multiple_of(b * BLK, BLK), BLK)
        s = jnp.dot(kx[...], q[:, lanes], preferred_element_type=F32)
        if masked:
            s = jnp.where(key_pos <= query + b * BLK, s, LOW)
        old = m[0:1, lanes]
        new = jnp.maximum(old, jnp.max(s, axis=0, keepdims=True) + move)
        p = jnp.exp(s - (new - move)).astype(BF16)
        part = jnp.dot(vx[...], p, preferred_element_type=F32)
        acc[:, lanes] = acc[:, lanes] * jnp.exp(old - new) + part
        m[:, lanes] = jnp.broadcast_to(new, (8, BLK))
        return carry

    lax.fori_loop(0, QS // BLK, tile_step, 0)


def first_body(idx, q, pay, acc, m, sums, kx, vx):
    acc[...] = jnp.zeros_like(acc)
    m[...] = jnp.full(m.shape, LOW, F32)
    absorb(pay, q, acc, m, kx, vx, jnp.zeros((1, BLK), F32), True, idx[2])
    sums[...] = jnp.broadcast_to(chunk_total(pay), sums.shape)


def step_body(k, idx, q, pay_r, acc_r0, m_r0, sums0, *refs):
    z = idx[0]
    left = k < 4
    if left:
        pay_l, refs = refs[0], refs[1:]
    if k > 1:
        acc_l0, m_l0, refs = refs[0], refs[1], refs[2:]
    if left:
        acc_r, m_r, sums, acc_l, m_l, kx, vx = refs
    else:
        out, acc_r, m_r, sums, acc_l, m_l, kx, vx = refs
    acc_r[...] = acc_r0[...]
    m_r[...] = m_r0[...]
    sums[...] = sums0[...]
    if k > 1:
        acc_l[...] = acc_l0[...]
        m_l[...] = m_l0[...]
    else:
        acc_l[...] = jnp.zeros_like(acc_l)
        m_l[...] = jnp.full(m_l.shape, LOW, F32)

    @pl.when(z >= k)
    def _():
        absorb(pay_r, q, acc_r, m_r, kx, vx, sums0[0:1], False, None)
        sums[...] = sums0[...] + jnp.broadcast_to(chunk_total(pay_r), sums.shape)

    if left:

        @pl.when(z + k >= 8)
        def _():
            total = chunk_total(pay_l)
            if k > 1:
                m_l[...] = m_l[...] + total[:, 0:1]
            absorb(pay_l, q, acc_l, m_l, kx, vx, jnp.zeros((1, BLK), F32), False, None)
    else:
        c = idx[2]
        row = lax.broadcasted_iota(jnp.int32, (8, BLK), 0)
        for b in range(4):
            for other in range(2):
                at = 2 * b + (c if other == 0 else 1 - c)
                lanes = pl.ds(pl.multiple_of(at * BLK, BLK), BLK)
                m_a = m_r[0:1, lanes]
                m_b = m_l[0:1, lanes] + sums[0:1]
                top = jnp.maximum(m_a, m_b)
                both = acc_r[:, lanes] * jnp.exp(m_a - top) + acc_l[:, lanes] * jnp.exp(m_b - top)
                to = slice(b * BLK, (b + 1) * BLK)
                out[other, 0:64, to] = both[0:64]
                out[other, 64:72, to] = jnp.where(row < 4, both[64:65], top)


def merge_body(own, sib, out):
    a, b = own[...], sib[...]
    m_a, m_b = a[68:69], b[68:69]
    top = jnp.maximum(m_a, m_b)
    f_a, f_b = jnp.exp(m_a - top), jnp.exp(m_b - top)
    total = a[64:65] * f_a + b[64:65] * f_b
    att = (a[0:64] * f_a + b[0:64] * f_b) / total
    att = jnp.concatenate([att, jnp.zeros_like(att)], axis=0)
    for r in range(8):
        out[r * 128 : (r + 1) * 128, :] = att[:, r * 128 : (r + 1) * 128].T[:, 0:64].astype(BF16)


def final_body(idx, att, gain, w0, w1, w2, w3, out, w):
    x, c, y = idx[1], idx[2], idx[3]
    for ky, ref in enumerate((w0, w1, w2, w3)):
        cols = pl.ds(pl.multiple_of(lax.rem(y - ky + NY, NY) * 256, 256), 256)
        for kx in range(NX):
            xx = lax.rem(x - kx + NX, NX)
            for other in range(2):
                cc = c if other == 0 else 1 - c
                for z in range(NZ):
                    at = pl.multiple_of(z * 128 + xx * 32 + cc * 16, 16)
                    w[pl.ds(at, 16), cols] = ref[kx, other, z]
    pieces = [att[xs * NY + ys] for ys in range(NY) for xs in range(NX)]
    joined = jnp.concatenate(pieces, axis=1)
    proj = lax.dot_general(joined, w[...], (((1,), (1,)), ((), ())), preferred_element_type=F32)
    scale = lax.rsqrt(jnp.mean(proj * proj, axis=-1, keepdims=True) + EPS)
    out[...] = (proj * scale * gain[...]).astype(BF16)


def shards(tokens, norm_gain, w_query, w_key, w_value, w_forget, forget_offset, w_out_t, out_gain):
    sds = jax.ShapeDtypeStruct
    idx = jnp.stack([lax.axis_index(a) for a in AXES]).astype(jnp.int32)

    tok_a = jnp.concatenate(direct(tokens[:32], "y"), axis=0)
    tok_b = jnp.concatenate(direct(tokens[32:], "x"), axis=0)
    toks = direct(tok_a, "x") + direct(tok_b, "y")

    heads = [w.reshape(16, NX, HD) for w in (w_query, w_key, w_value)]
    heads.append(jnp.broadcast_to(w_forget[:, :, None], (16, NX, HD)))
    per_head = jnp.concatenate(heads, axis=2).transpose(1, 0, 2)
    w_x = lax.all_to_all(per_head, "x", 0, 0, tiled=True).reshape(64, 256)
    chunk = jnp.concatenate([w_x, w_out_t], axis=0)
    w_own = lax.all_to_all(jnp.broadcast_to(chunk[None], (NZ, 80, 256)), "z", 0, 0, tiled=True)
    w_sib = shift(w_own, "c", 1)

    q_own, kv, cum_own = call(
        project_body,
        "project",
        (sds((64, KEYS), BF16), sds((128, KEYS), BF16), sds((8, KEYS), F32)),
        [SMEM, SMEM] + [VMEM] * 11,
        [pltpu.VMEM((D, 256), BF16), pltpu.VMEM((KEYS, 256), F32)],
        2e9,
    )(idx, forget_offset, *toks, norm_gain[None], w_own, w_sib)

    q_sib = shift(q_own, "c", 1)
    cum_sib = shift(cum_own, "c", 1)
    q, pay = call(
        prepare_body,
        "prepare",
        (sds((128, QS), BF16), sds((PAY, KEYS), BF16)),
        [SMEM] + [VMEM] * 5,
    )(idx, q_own, q_sib, kv, cum_own, cum_sib)

    w_o = jnp.stack([w_own[:, 64:], w_sib[:, 64:]])
    w_o = jnp.stack(direct(w_o, "x"))
    w_o = direct(w_o, "y")

    acc_t, m_t, sums_t = sds((80, QS), F32), sds((8, QS), F32), sds((8, BLK), F32)
    work = [pltpu.VMEM((KEYS, 128), BF16), pltpu.VMEM((80, KEYS), BF16)]
    right = shift(pay, "z", 1)
    left = shift(pay, "z", -1)
    acc_r, m_r, sums = call(
        first_body, "attend0", (acc_t, m_t, sums_t), [SMEM, VMEM, VMEM], work, 3e9
    )(idx, q, pay)
    state_l = ()
    for k in range(1, 5):
        pays = (right, left) if k < 4 else (right,)
        if k < 4:
            right = shift(pays[0], "z", 1)
        if k < 3:
            left = shift(pays[1], "z", -1)
        ins = (idx, q, pays[0], acc_r, m_r, sums) + pays[1:] + state_l
        if k < 4:
            outs = (acc_t, m_t, sums_t, acc_t, m_t)
            scratch = work
        else:
            outs = sds((2, 72, KEYS), F32)
            scratch = [pltpu.VMEM(t.shape, F32) for t in (acc_t, m_t, sums_t, acc_t, m_t)] + work
        res = call(
            functools.partial(step_body, k),
            f"attend{k}",
            outs,
            [SMEM] + [VMEM] * (len(ins) - 1),
            scratch,
            6e9,
        )(*ins)
        if k < 4:
            acc_r, m_r, sums = res[:3]
            state_l = tuple(res[3:])
    sib = shift(res[1], "c", 1)
    att = call(merge_body, "merge", sds((KEYS, HD), BF16), [VMEM, VMEM])(res[0], sib)
    att = lax.all_to_all(att.reshape(16, 64, HD), ("x", "y"), 0, 0, tiled=True)
    return call(
        final_body,
        "final",
        sds((OWN, D), BF16),
        [SMEM] + [VMEM] * 6,
        [pltpu.VMEM((D, D), BF16)],
    )(idx, att, out_gain[None], *w_o)


def solution(mesh):
    finer = Mesh(mesh.devices.reshape(NZ, NX, NC, NY), AXES)
    sp = ("z", "x", "c")
    return jax.shard_map(
        shards,
        mesh=finer,
        in_specs=(
            P(AXES, None),
            P(),
            P(sp, "y"),
            P(sp, "y"),
            P(sp, "y"),
            P(sp, "y"),
            P("y"),
            P(sp, "y"),
            P(),
        ),
        out_specs=P(AXES, None),
        check_vma=False,
    )
```

```python
import functools
import math

import jax
import jax.numpy as jnp
from jax import lax
from jax.experimental import pallas as pl
from jax.experimental.pallas import tpu as pltpu
from jax.sharding import Mesh
from jax.sharding import PartitionSpec as P


AXES = ("z", "x", "c", "y")
NZ, NX, NC, NY = 8, 4, 2, 4
SIZES = {"z": NZ, "x": NX, "c": NC, "y": NY}
D = 1024
HD = 64
TOTAL = 16384
OWN = 64
BLK = 256
KEYS = 1024
QS = 2048
PAY = 144
EPS = 1e-06
LOW = -1e30
F32 = jnp.float32
BF16 = jnp.bfloat16


VMEM = pl.BlockSpec(memory_space=pltpu.VMEM)
SMEM = pl.BlockSpec(memory_space=pltpu.SMEM)


def call(body, outs, ins, scratch=(), flops=1e8, aliases=None):
    return pl.pallas_call(
        body,
        out_shape=outs,
        in_specs=ins,
        out_specs=jax.tree.map(lambda _: VMEM, outs),
        scratch_shapes=list(scratch),
        input_output_aliases=aliases or {},
        cost_estimate=pl.CostEstimate(
            flops=int(flops), bytes_accessed=1 << 20, transcendentals=0
        ),
        compiler_params=pltpu.CompilerParams(vmem_limit_bytes=24 << 20),
    )


def shift(x, axis, k):
    n = SIZES[axis]
    return lax.ppermute(x, axis, [(i, (i + k) % n) for i in range(n)])


def direct(x, axis):
    return [x] + [shift(x, axis, k) for k in range(1, SIZES[axis])]


def three_parts(x):
    hi = x.astype(BF16)
    rest = x - hi.astype(F32)
    mid = rest.astype(BF16)
    low = (rest - mid.astype(F32)).astype(BF16)
    return hi, mid, low


def project_body(idx, offs, *refs):
    toks = refs[:8]
    gain, w_own, w_sib = refs[8:11]
    q_out, kv_out, cum_out = refs[11:14]
    w, rows = refs[14:]
    x, c, y = idx[1], idx[2], idx[3]
    for z in range(NZ):
        for xx in range(NX):
            base = z * 128 + xx * 32
            own_at = pl.multiple_of(base + c * 16, 16)
            sib_at = pl.multiple_of(base + (1 - c) * 16, 16)
            w[pl.ds(own_at, 16), :] = w_own[z, xx * 16 : xx * 16 + 16, :]
            w[pl.ds(sib_at, 16), :] = w_sib[z, xx * 16 : xx * 16 + 16, :]
    for half in range(2):
        for outer in range(4):
            tok = toks[half * 4 + outer][...].astype(F32)
            scale = lax.rsqrt(jnp.mean(tok * tok, axis=-1, keepdims=True) + EPS)
            normed = (tok * scale * gain[...]).astype(BF16)
            out = jnp.dot(normed, w[...], preferred_element_type=F32)
            for inner in range(4):
                kx, ky = (outer, inner) if half == 0 else (inner, outer)
                xx = lax.rem(x - kx + NX, NX)
                yy = lax.rem(y - ky + NY, NY)
                at = pl.multiple_of(xx * BLK + yy * OWN + half * 32, 32)
                rows[pl.ds(at, 32), :] = out[inner * 32 : inner * 32 + 32, :]
    before = lax.broadcasted_iota(jnp.int32, (BLK, BLK), 0)
    after = lax.broadcasted_iota(jnp.int32, (BLK, BLK), 1)
    ones = jnp.where(before <= after, 1.0, 0.0).astype(BF16)
    for b in range(4):
        t = rows[b * BLK : (b + 1) * BLK, :].T
        lanes = slice(b * BLK, (b + 1) * BLK)
        q_out[:, lanes] = t[:64].astype(BF16)
        kv_out[:, lanes] = t[64:192].astype(BF16)
        logit = t[192:200] + offs[x] + math.log(TOTAL)
        gate = jnp.minimum(logit, 0.0) - jnp.log1p(jnp.exp(-jnp.abs(logit)))
        hi, mid, low = three_parts(gate)
        cum = jnp.dot(hi, ones, preferred_element_type=F32)
        cum = cum + jnp.dot(mid, ones, preferred_element_type=F32)
        cum = cum + jnp.dot(low, ones, preferred_element_type=F32)
        cum_out[:, lanes] = cum


def prepare_body(idx, q_own, q_sib, kv, cum_own, cum_sib, q_out, pay_out):
    c = idx[2]
    q_out[80:128, :] = jnp.zeros((48, QS), BF16)
    row = lax.broadcasted_iota(jnp.int32, (16, QS), 0)
    q_out[64:80, :] = jnp.where(row < 3, 1.0, 0.0).astype(BF16)
    for b in range(4):
        lanes = slice(b * BLK, (b + 1) * BLK)
        own_at = pl.multiple_of((2 * b + c) * BLK, BLK)
        sib_at = pl.multiple_of((2 * b + 1 - c) * BLK, BLK)
        q_out[0:64, pl.ds(own_at, BLK)] = q_own[:, lanes] * jnp.asarray(0.125, BF16)
        q_out[0:64, pl.ds(sib_at, BLK)] = q_sib[:, lanes] * jnp.asarray(0.125, BF16)
    own = [cum_own[:, b * BLK + BLK - 1 : b * BLK + BLK] for b in range(4)]
    sib = [cum_sib[:, b * BLK + BLK - 1 : b * BLK + BLK] for b in range(4)]
    ahead = jnp.zeros_like(own[0])
    bases = []
    for b in range(4):
        bases.append(ahead + jnp.where(c == 1, sib[b], 0.0))
        ahead = ahead + (own[b] + sib[b])
    total = ahead
    pay_out[0:64, :] = kv[0:64, :]
    pay_out[80:144, :] = kv[64:128, :]
    row = lax.broadcasted_iota(jnp.int32, (16, BLK), 0)
    for b in range(4):
        lanes = slice(b * BLK, (b + 1) * BLK)
        bias = (total - bases[b]) - cum_own[:, lanes]
        parts = [p[0:1].astype(F32) for p in three_parts(bias)]
        totals = [p[0:1].astype(F32) for p in three_parts(jnp.broadcast_to(total, bias.shape))]
        block = jnp.zeros((16, BLK), F32)
        for i, part in enumerate(parts + totals):
            block = jnp.where(row == i, part, block)
        pay_out[64:80, lanes] = block.astype(BF16)


def chunk_total(pay):
    rows = pay[64:80, 0:BLK].astype(F32)
    return rows[3:4] + rows[4:5] + rows[5:6]


def place_chunk(pay, i, kx, vx):
    fill = jnp.zeros((48, 128), F32)
    for r in range(8):
        lanes = slice(r * 128, (r + 1) * 128)
        tile = jnp.concatenate([pay[0:80, lanes].astype(F32), fill], axis=0)
        kx[i, lanes, :] = tile.T.astype(BF16)
    vx[i, 0:64, :] = pay[80:144, :]
    vx[i, 64:80, :] = jnp.ones((16, KEYS), BF16)


def absorb(count, q, acc, m, kx, vx, move, c=None):
    if c is not None:
        key = lax.broadcasted_iota(jnp.int32, (KEYS, BLK), 0)
        key_pos = key + (key // BLK + c) * BLK
        query = lax.broadcasted_iota(jnp.int32, (KEYS, BLK), 1)

    def two_tiles(t, carry):
        i = t // 4
        lanes, s = [], []
        for u in range(2):
            b = (t % 4) * 2 + u
            at = pl.ds(pl.multiple_of(b * BLK, BLK), BLK)
            part = jnp.dot(kx[i], q[:, at], preferred_element_type=F32)
            if c is not None:
                part = jnp.where(key_pos <= query + b * BLK, part, LOW)
            lanes.append(at)
            s.append(part)
        by = move[i, 0:1]
        for u in range(2):
            old = m[i, 0:1, lanes[u]]
            new = jnp.maximum(old, jnp.max(s[u], axis=0, keepdims=True) + by)
            p = jnp.exp(s[u] - (new - by)).astype(BF16)
            part = jnp.dot(vx[i], p, preferred_element_type=F32)
            acc[i, :, lanes[u]] = acc[i, :, lanes[u]] * jnp.exp(old - new) + part
            m[i, :, lanes[u]] = jnp.broadcast_to(new, (8, BLK))
        return carry

    lax.fori_loop(0, count * 4, two_tiles, 0)


def first_body(idx, q, pay, acc, m, sums, kx, vx, move):
    acc[...] = jnp.zeros_like(acc)
    m[...] = jnp.full(m.shape, LOW, F32)
    move[...] = jnp.zeros_like(move)
    place_chunk(pay, 0, kx, vx)
    absorb(1, q, acc, m, kx, vx, move, idx[2])
    sums[...] = jnp.broadcast_to(chunk_total(pay), sums.shape)


def step_body(k, idx, q, *refs):
    z = idx[0]
    n_pay = 2 if k < 4 else 1
    pays, refs = refs[:n_pay], refs[n_pay:]
    acc0, m0, sums0, refs = refs[0], refs[1], refs[2], refs[3:]
    if k < 4:
        acc, m, sums, kx, vx, move = refs
    else:
        out, kx, vx, move, sums = refs
        acc, m = acc0, m0
    sums[...] = sums0[...]
    count = (z >= k).astype(jnp.int32)

    @pl.when(z >= k)
    def _():
        place_chunk(pays[0], 0, kx, vx)
        move[0] = sums0[...]
        sums[...] = sums0[...] + jnp.broadcast_to(chunk_total(pays[0]), sums.shape)

    if k < 4:
        count = count + (z + k >= 8).astype(jnp.int32)

        @pl.when(z + k >= 8)
        def _():
            place_chunk(pays[1], 1, kx, vx)
            move[1] = jnp.zeros(sums.shape, F32)
            m[1] = m[1] + chunk_total(pays[1])[:, 0:1]

    absorb(count, q, acc, m, kx, vx, move)
    if k == 4:
        c = idx[2]
        row = lax.broadcasted_iota(jnp.int32, (8, BLK), 0)
        for b in range(4):
            for other in range(2):
                at = 2 * b + (c if other == 0 else 1 - c)
                lanes = pl.ds(pl.multiple_of(at * BLK, BLK), BLK)
                m_a = m[0, 0:1, lanes]
                m_b = m[1, 0:1, lanes] + sums[0:1]
                top = jnp.maximum(m_a, m_b)
                both = acc[0, :, lanes] * jnp.exp(m_a - top) + acc[1, :, lanes] * jnp.exp(m_b - top)
                to = slice(b * BLK, (b + 1) * BLK)
                out[other, 0:64, to] = both[0:64]
                out[other, 64:72, to] = jnp.where(row < 4, both[64:65], top)


def merge_body(own, sib, out):
    a, b = own[...], sib[...]
    m_a, m_b = a[68:69], b[68:69]
    top = jnp.maximum(m_a, m_b)
    f_a, f_b = jnp.exp(m_a - top), jnp.exp(m_b - top)
    total = a[64:65] * f_a + b[64:65] * f_b
    att = (a[0:64] * f_a + b[0:64] * f_b) / total
    att = jnp.concatenate([att, jnp.zeros_like(att)], axis=0)
    for r in range(8):
        out[r * 128 : (r + 1) * 128, :] = att[:, r * 128 : (r + 1) * 128].T[:, 0:64].astype(BF16)


def final_body(idx, att, gain, w_all, out, w):
    c = idx[2]
    for xs in range(NX):
        for ys in range(NY):
            for other in range(2):
                cc = c if other == 0 else 1 - c
                for z in range(NZ):
                    at = pl.multiple_of(z * 128 + xs * 32 + cc * 16, 16)
                    w[pl.ds(at, 16), ys * 256 : ys * 256 + 256] = w_all[xs * NY + ys, other, z]
    pieces = [att[xs * NY + ys] for ys in range(NY) for xs in range(NX)]
    joined = jnp.concatenate(pieces, axis=1)
    proj = lax.dot_general(joined, w[...], (((1,), (1,)), ((), ())), preferred_element_type=F32)
    scale = lax.rsqrt(jnp.mean(proj * proj, axis=-1, keepdims=True) + EPS)
    out[...] = (proj * scale * gain[...]).astype(BF16)


def shards(tokens, norm_gain, w_query, w_key, w_value, w_forget, forget_offset, w_out_t, out_gain):
    sds = jax.ShapeDtypeStruct
    idx = jnp.stack([lax.axis_index(a) for a in AXES]).astype(jnp.int32)

    tok_a = direct(tokens[:32], "y")
    tok_b = direct(tokens[32:], "x")
    toks = direct(jnp.concatenate(tok_a, axis=0), "x")
    toks = toks + direct(jnp.concatenate(tok_b, axis=0), "y")

    heads = [w.reshape(16, NX, HD) for w in (w_query, w_key, w_value)]
    heads.append(jnp.broadcast_to(w_forget[:, :, None], (16, NX, HD)))
    per_head = jnp.concatenate(heads, axis=2).transpose(1, 0, 2)
    w_x = lax.all_to_all(per_head, "x", 0, 0, tiled=True).reshape(64, 256)
    chunk = jnp.concatenate([w_x, w_out_t], axis=0)
    w_own = lax.all_to_all(jnp.broadcast_to(chunk[None], (NZ, 80, 256)), "z", 0, 0, tiled=True)
    w_sib = shift(w_own, "c", 1)

    q_own, kv, cum_own = call(
        project_body,
        (sds((64, KEYS), BF16), sds((128, KEYS), BF16), sds((8, KEYS), F32)),
        [SMEM, SMEM] + [VMEM] * 11,
        [pltpu.VMEM((D, 256), BF16), pltpu.VMEM((KEYS, 256), F32)],
        2e9,
    )(idx, forget_offset, *toks, norm_gain[None], w_own, w_sib)

    q_sib = shift(q_own, "c", 1)
    cum_sib = shift(cum_own, "c", 1)
    q, pay = call(
        prepare_body, (sds((128, QS), BF16), sds((PAY, KEYS), BF16)), [SMEM] + [VMEM] * 5
    )(idx, q_own, q_sib, kv, cum_own, cum_sib)

    acc_t, m_t, sums_t = sds((2, 80, QS), F32), sds((2, 8, QS), F32), sds((8, BLK), F32)
    work = [
        pltpu.VMEM((2, KEYS, 128), BF16),
        pltpu.VMEM((2, 80, KEYS), BF16),
        pltpu.VMEM((2, 8, BLK), F32),
    ]
    right = shift(pay, "z", 1)
    left = shift(pay, "z", -1)
    acc, m, sums = call(
        first_body, (acc_t, m_t, sums_t), [SMEM, VMEM, VMEM], work, 3e9
    )(idx, q, pay)

    w_o = jnp.stack([w_own[:, 64:], w_sib[:, 64:]])
    w_o, _ = lax.optimization_barrier((w_o, sums))
    w_o = jnp.broadcast_to(w_o[None], (16, 2, 8, 16, 256))
    w_o = lax.all_to_all(w_o, ("x", "y"), 0, 0, tiled=True)

    for k in range(1, 5):
        pays = (right, left) if k < 4 else (right,)
        if k < 4:
            right = shift(pays[0], "z", 1)
        if k < 3:
            left = shift(pays[1], "z", -1)
        ins = (idx, q) + pays + (acc, m, sums)
        if k < 4:
            outs, scratch, aliases = (acc_t, m_t, sums_t), work, {4: 0, 5: 1}
        else:
            outs, aliases = sds((2, 72, KEYS), F32), None
            scratch = work + [pltpu.VMEM(sums_t.shape, F32)]
        res = call(
            functools.partial(step_body, k),
            outs,
            [SMEM] + [VMEM] * (len(ins) - 1),
            scratch,
            6e9,
            aliases,
        )(*ins)
        if k < 4:
            acc, m, sums = res
    sib = shift(res[1], "c", 1)
    att = call(merge_body, sds((KEYS, HD), BF16), [VMEM, VMEM])(res[0], sib)
    att = lax.all_to_all(att.reshape(16, 64, HD), ("x", "y"), 0, 0, tiled=True)
    return call(
        final_body, sds((OWN, D), BF16), [SMEM] + [VMEM] * 3, [pltpu.VMEM((D, D), BF16)]
    )(idx, att, out_gain[None], w_o)


def solution(mesh):
    finer = Mesh(mesh.devices.reshape(NZ, NX, NC, NY), AXES)
    sp = ("z", "x", "c")

    return jax.shard_map(
        shards,
        mesh=finer,
        in_specs=(
            P(AXES, None),
            P(),
            P(sp, "y"),
            P(sp, "y"),
            P(sp, "y"),
            P(sp, "y"),
            P("y"),
            P(sp, "y"),
            P(),
        ),
        out_specs=P(AXES, None),
        check_vma=False,
    )
```

```python
import functools
import math

import jax
import jax.numpy as jnp
from jax import lax
from jax.experimental import pallas as pl
from jax.experimental.pallas import tpu as pltpu
from jax.sharding import Mesh
from jax.sharding import PartitionSpec as P


AXES = ("z", "x", "c", "y")
NZ, NX, NC, NY = 8, 4, 2, 4
SIZES = {"z": NZ, "x": NX, "c": NC, "y": NY}
D = 1024
HD = 64
TOTAL = 16384
OWN = 64
BLK = 256
KEYS = 1024
QS = 2048
PAY = 144
EPS = 1e-06
LOW = -1e30
F32 = jnp.float32
BF16 = jnp.bfloat16


VMEM = pl.BlockSpec(memory_space=pltpu.VMEM)
SMEM = pl.BlockSpec(memory_space=pltpu.SMEM)


def call(body, outs, ins, scratch=(), flops=1e8, aliases=None):
    return pl.pallas_call(
        body,
        out_shape=outs,
        in_specs=ins,
        out_specs=jax.tree.map(lambda _: VMEM, outs),
        scratch_shapes=list(scratch),
        input_output_aliases=aliases or {},
        cost_estimate=pl.CostEstimate(
            flops=int(flops), bytes_accessed=1 << 20, transcendentals=0
        ),
        compiler_params=pltpu.CompilerParams(vmem_limit_bytes=24 << 20),
    )


def shift(x, axis, k):
    n = SIZES[axis]
    return lax.ppermute(x, axis, [(i, (i + k) % n) for i in range(n)])


def direct(x, axis):
    return [x] + [shift(x, axis, k) for k in range(1, SIZES[axis])]


def step_right(x, k):
    return lax.ppermute(x, "z", [(i, i + 1) for i in range(k - 1, NZ - 1)])


def step_left(x, k):
    return lax.ppermute(x, "z", [((i - k + 1) % NZ, (i - k) % NZ) for i in range(3)])


def three_parts(x):
    hi = x.astype(BF16)
    rest = x - hi.astype(F32)
    mid = rest.astype(BF16)
    low = (rest - mid.astype(F32)).astype(BF16)
    return hi, mid, low


def pack_body(idx, tok, wq, wk, wv, wf, lo, hi, p0, p1, p2, p3, heads):
    x = idx[1]
    lo[...] = tok[0:32, :]
    hi[...] = tok[32:64, :]
    for h in range(NX):
        lanes = slice(h * HD, (h + 1) * HD)
        gate = jnp.broadcast_to(wf[:, h : h + 1].astype(F32), (16, HD)).astype(BF16)
        heads[h] = jnp.concatenate([wq[:, lanes], wk[:, lanes], wv[:, lanes], gate], axis=1)
    for k, out in enumerate((p0, p1, p2, p3)):
        out[...] = heads[lax.rem(x + k, NX)]


def spread_body(p0, p1, p2, p3, wo, out):
    for z in range(NZ):
        for k, piece in enumerate((p0, p1, p2, p3, wo)):
            out[z, k * 16 : k * 16 + 16, :] = piece[...]


def project_body(idx, offs, *refs):
    toks = refs[:8]
    gain, w_own, w_sib = refs[8:11]
    qc_out, kv_out, cum_out = refs[11:14]
    w, rows = refs[14:]
    x, c, y = idx[1], idx[2], idx[3]
    for z in range(NZ):
        for xx in range(NX):
            base = z * 128 + lax.rem(x - xx + NX, NX) * 32
            own_at = pl.multiple_of(base + c * 16, 16)
            sib_at = pl.multiple_of(base + (1 - c) * 16, 16)
            w[pl.ds(own_at, 16), :] = w_own[z, xx * 16 : xx * 16 + 16, :]
            w[pl.ds(sib_at, 16), :] = w_sib[z, xx * 16 : xx * 16 + 16, :]
    for half in range(2):
        for outer in range(4):
            tok = toks[half * 4 + outer][...].astype(F32)
            scale = lax.rsqrt(jnp.mean(tok * tok, axis=-1, keepdims=True) + EPS)
            normed = (tok * scale * gain[...]).astype(BF16)
            out = jnp.dot(normed, w[...], preferred_element_type=F32)
            for inner in range(4):
                kx, ky = (outer, inner) if half == 0 else (inner, outer)
                xx = lax.rem(x - kx + NX, NX)
                yy = lax.rem(y - ky + NY, NY)
                at = pl.multiple_of(xx * BLK + yy * OWN + half * 32, 32)
                rows[pl.ds(at, 32), :] = out[inner * 32 : inner * 32 + 32, :]
    before = lax.broadcasted_iota(jnp.int32, (BLK, BLK), 0)
    after = lax.broadcasted_iota(jnp.int32, (BLK, BLK), 1)
    ones = jnp.where(before <= after, 1.0, 0.0).astype(BF16)
    for b in range(4):
        t = rows[b * BLK : (b + 1) * BLK, :].T
        lanes = slice(b * BLK, (b + 1) * BLK)
        qc_out[0:64, lanes] = t[:64].astype(BF16)
        kv_out[:, lanes] = t[64:192].astype(BF16)
        logit = t[192:200] + offs[x] + math.log(TOTAL)
        gate = jnp.minimum(logit, 0.0) - jnp.log1p(jnp.exp(-jnp.abs(logit)))
        hi, mid, low = three_parts(gate)
        cum = jnp.dot(hi, ones, preferred_element_type=F32)
        cum = cum + jnp.dot(mid, ones, preferred_element_type=F32)
        cum = cum + jnp.dot(low, ones, preferred_element_type=F32)
        cum_out[:, lanes] = cum
        row = lax.broadcasted_iota(jnp.int32, (16, BLK), 0)
        block = jnp.zeros((16, BLK), F32)
        for i, part in enumerate(three_parts(cum[0:1])):
            block = jnp.where(row == i, part.astype(F32), block)
        qc_out[64:80, lanes] = block.astype(BF16)


def prepare_body(idx, q_own, q_sib, kv, cum_own, q_out, pay_out):
    c = idx[2]
    q_out[80:128, :] = jnp.zeros((48, QS), BF16)
    row = lax.broadcasted_iota(jnp.int32, (16, QS), 0)
    q_out[64:80, :] = jnp.where(row < 3, 1.0, 0.0).astype(BF16)
    for b in range(4):
        lanes = slice(b * BLK, (b + 1) * BLK)
        own_at = pl.multiple_of((2 * b + c) * BLK, BLK)
        sib_at = pl.multiple_of((2 * b + 1 - c) * BLK, BLK)
        q_out[0:64, pl.ds(own_at, BLK)] = q_own[0:64, lanes] * jnp.asarray(0.125, BF16)
        q_out[0:64, pl.ds(sib_at, BLK)] = q_sib[0:64, lanes] * jnp.asarray(0.125, BF16)
    own, sib = [], []
    for b in range(4):
        end = slice(b * BLK + BLK - 1, b * BLK + BLK)
        own.append(cum_own[:, end])
        parts = q_sib[64:80, b * BLK + 128 : b * BLK + BLK].astype(F32)[:, 127:128]
        sib.append(jnp.broadcast_to(parts[0:1] + parts[1:2] + parts[2:3], (8, 1)))
    ahead = jnp.zeros_like(own[0])
    bases = []
    for b in range(4):
        bases.append(ahead + jnp.where(c == 1, sib[b], 0.0))
        ahead = ahead + (own[b] + sib[b])
    total = ahead
    pay_out[0:64, :] = kv[0:64, :]
    pay_out[80:144, :] = kv[64:128, :]
    row = lax.broadcasted_iota(jnp.int32, (16, BLK), 0)
    for b in range(4):
        lanes = slice(b * BLK, (b + 1) * BLK)
        bias = (total - bases[b]) - cum_own[:, lanes]
        parts = [p[0:1].astype(F32) for p in three_parts(bias)]
        totals = [p[0:1].astype(F32) for p in three_parts(jnp.broadcast_to(total, bias.shape))]
        block = jnp.zeros((16, BLK), F32)
        for i, part in enumerate(parts + totals):
            block = jnp.where(row == i, part, block)
        pay_out[64:80, lanes] = block.astype(BF16)


def chunk_total(pay):
    rows = pay[64:80, 0:BLK].astype(F32)
    return rows[3:4] + rows[4:5] + rows[5:6]


def place_chunk(pay, i, kx, vx):
    fill = jnp.zeros((48, 128), F32)
    for r in range(8):
        lanes = slice(r * 128, (r + 1) * 128)
        tile = jnp.concatenate([pay[0:80, lanes].astype(F32), fill], axis=0)
        kx[i, lanes, :] = tile.T.astype(BF16)
    vx[i, 0:64, :] = pay[80:144, :]
    vx[i, 64:80, :] = jnp.ones((16, KEYS), BF16)


def absorb(count, q, acc, m, kx, vx, move, work, c=None):
    tiles = QS // BLK
    bufs, tops, probs, fades = work[0:2], work[2:4], work[4:6], work[6:8]
    if c is not None:
        key = lax.broadcasted_iota(jnp.int32, (KEYS, BLK), 0)
        key_pos = key + (key // BLK + c) * BLK
        query = lax.broadcasted_iota(jnp.int32, (KEYS, BLK), 1)

    def lanes_of(t):
        return pl.ds(pl.multiple_of((t % tiles) * BLK, BLK), BLK)

    def score(t, slot):
        s = jnp.dot(kx[t // tiles], q[:, lanes_of(t)], preferred_element_type=F32)
        if c is not None:
            s = jnp.where(key_pos <= query + (t % tiles) * BLK, s, LOW)
        bufs[slot][...] = s
        tops[slot][...] = jnp.broadcast_to(jnp.max(s, axis=0, keepdims=True), (8, BLK))

    def weigh(t, slot):
        i, lanes = t // tiles, lanes_of(t)
        by = move[i, 0:1]
        old = m[i, 0:1, lanes]
        new = jnp.maximum(old, tops[slot][0:1] + by)
        probs[slot][...] = jnp.exp(bufs[slot][...] - (new - by)).astype(BF16)
        fades[slot][...] = jnp.broadcast_to(jnp.exp(old - new), (8, BLK))
        m[i, :, lanes] = jnp.broadcast_to(new, (8, BLK))

    def add(t, slot):
        i, lanes = t // tiles, lanes_of(t)
        part = jnp.dot(vx[i], probs[slot][...], preferred_element_type=F32)
        acc[i, :, lanes] = acc[i, :, lanes] * fades[slot][0:1] + part

    @pl.when(count > 0)
    def _():
        probs[1][...] = jnp.zeros((KEYS, BLK), BF16)
        fades[1][...] = jnp.ones((8, BLK), F32)
        score(0, 0)
        last = count * tiles - 1

        def two_tiles(j, carry):
            t = 2 * j
            add(jnp.maximum(t - 1, 0), 1)
            weigh(t, 0)
            score(t + 1, 1)
            add(t, 0)
            weigh(t + 1, 1)
            score(jnp.minimum(t + 2, last), 0)
            return carry

        lax.fori_loop(0, count * (tiles // 2), two_tiles, 0)
        add(last, 1)


def first_body(idx, q, pay, acc, m, sums, kx, vx, move, *bufs):
    acc[...] = jnp.zeros_like(acc)
    m[...] = jnp.full(m.shape, LOW, F32)
    move[...] = jnp.zeros_like(move)
    place_chunk(pay, 0, kx, vx)
    absorb(1, q, acc, m, kx, vx, move, bufs, idx[2])
    sums[...] = jnp.broadcast_to(chunk_total(pay), sums.shape)


def step_body(k, idx, q, *refs):
    z = idx[0]
    n_pay = 2 if k < 4 else 1
    pays, refs = refs[:n_pay], refs[n_pay:]
    acc0, m0, sums0, refs = refs[0], refs[1], refs[2], refs[3:]
    if k < 4:
        acc, m, sums, kx, vx, move, *bufs = refs
    else:
        out_own, out_sib, kx, vx, move, *bufs, sums = refs
        acc, m = acc0, m0
    sums[...] = sums0[...]
    count = (z >= k).astype(jnp.int32)

    @pl.when(z >= k)
    def _():
        place_chunk(pays[0], 0, kx, vx)
        move[0] = sums0[...]
        sums[...] = sums0[...] + jnp.broadcast_to(chunk_total(pays[0]), sums.shape)

    if k < 4:
        count = count + (z + k >= 8).astype(jnp.int32)

        @pl.when(z + k >= 8)
        def _():
            place_chunk(pays[1], 1, kx, vx)
            move[1] = jnp.zeros(sums.shape, F32)
            m[1] = m[1] + chunk_total(pays[1])[:, 0:1]

    absorb(count, q, acc, m, kx, vx, move, bufs)
    if k == 4:
        c = idx[2]
        row = lax.broadcasted_iota(jnp.int32, (8, BLK), 0)
        for b in range(4):
            for other in range(2):
                at = 2 * b + (c if other == 0 else 1 - c)
                lanes = pl.ds(pl.multiple_of(at * BLK, BLK), BLK)
                m_a = m[0, 0:1, lanes]
                m_b = m[1, 0:1, lanes] + sums[0:1]
                top = jnp.maximum(m_a, m_b)
                both = acc[0, :, lanes] * jnp.exp(m_a - top) + acc[1, :, lanes] * jnp.exp(m_b - top)
                to = slice(b * BLK, (b + 1) * BLK)
                out = out_own if other == 0 else out_sib
                out[0:64, to] = both[0:64]
                out[64:72, to] = jnp.where(row < 4, both[64:65], top)


def merge_body(own, sib, out):
    a, b = own[...], sib[...]
    m_a, m_b = a[68:69], b[68:69]
    top = jnp.maximum(m_a, m_b)
    f_a, f_b = jnp.exp(m_a - top), jnp.exp(m_b - top)
    total = a[64:65] * f_a + b[64:65] * f_b
    att = (a[0:64] * f_a + b[0:64] * f_b) / total
    att = jnp.concatenate([att, jnp.zeros_like(att)], axis=0)
    for r in range(8):
        out[r * 128 : (r + 1) * 128, :] = att[:, r * 128 : (r + 1) * 128].T[:, 0:64].astype(BF16)


def assemble_body(idx, w0, w1, w2, w3, w):
    x, c, y = idx[1], idx[2], idx[3]
    for ky, ref in enumerate((w0, w1, w2, w3)):
        cols = pl.ds(pl.multiple_of(lax.rem(y - ky + NY, NY) * 256, 256), 256)
        for kx in range(NX):
            xx = lax.rem(x - kx + NX, NX)
            for other in range(2):
                cc = c if other == 0 else 1 - c
                for z in range(NZ):
                    at = pl.multiple_of(z * 128 + xx * 32 + cc * 16, 16)
                    w[pl.ds(at, 16), cols] = ref[kx, other, z]


def final_body(att, gain, w, out):
    pieces = [att[xs * NY + ys] for ys in range(NY) for xs in range(NX)]
    joined = jnp.concatenate(pieces, axis=1)
    proj = lax.dot_general(joined, w[...], (((1,), (1,)), ((), ())), preferred_element_type=F32)
    scale = lax.rsqrt(jnp.mean(proj * proj, axis=-1, keepdims=True) + EPS)
    out[...] = (proj * scale * gain[...]).astype(BF16)


def shards(tokens, norm_gain, w_query, w_key, w_value, w_forget, forget_offset, w_out_t, out_gain):
    sds = jax.ShapeDtypeStruct
    idx = jnp.stack([lax.axis_index(a) for a in AXES]).astype(jnp.int32)

    half, piece = sds((32, D), BF16), sds((16, 256), BF16)
    tok_lo, tok_hi, *pieces = call(
        pack_body,
        (half, half, piece, piece, piece, piece),
        [SMEM] + [VMEM] * 5,
        [pltpu.VMEM((NX, 16, 256), BF16)],
    )(idx, tokens, w_query, w_key, w_value, w_forget)

    pieces = [pieces[0]] + [shift(pieces[k], "x", k) for k in range(1, NX)]
    tok_a = direct(tok_lo, "y")
    tok_b = direct(tok_hi, "x")
    toks = direct(jnp.concatenate(tok_a, axis=0), "x")
    toks = toks + direct(jnp.concatenate(tok_b, axis=0), "y")
    chunk = call(spread_body, sds((NZ, 80, 256), BF16), [VMEM] * 5)(*pieces, w_out_t)
    w_own = lax.all_to_all(chunk, "z", 0, 0, tiled=True)
    w_sib = shift(w_own, "c", 1)

    q_own, kv, cum_own = call(
        project_body,
        (sds((80, KEYS), BF16), sds((128, KEYS), BF16), sds((8, KEYS), F32)),
        [SMEM, SMEM] + [VMEM] * 11,
        [pltpu.VMEM((D, 256), BF16), pltpu.VMEM((KEYS, 256), F32)],
        2e9,
    )(idx, forget_offset, *toks, norm_gain[None], w_own, w_sib)

    q_sib = shift(q_own, "c", 1)
    q, pay = call(
        prepare_body, (sds((128, QS), BF16), sds((PAY, KEYS), BF16)), [SMEM] + [VMEM] * 4
    )(idx, q_own, q_sib, kv, cum_own)

    acc_t, m_t, sums_t = sds((2, 80, QS), F32), sds((2, 8, QS), F32), sds((8, BLK), F32)
    work = [
        pltpu.VMEM((2, KEYS, 128), BF16),
        pltpu.VMEM((2, 80, KEYS), BF16),
        pltpu.VMEM((2, 8, BLK), F32),
        pltpu.VMEM((KEYS, BLK), F32),
        pltpu.VMEM((KEYS, BLK), F32),
        pltpu.VMEM((8, BLK), F32),
        pltpu.VMEM((8, BLK), F32),
        pltpu.VMEM((KEYS, BLK), BF16),
        pltpu.VMEM((KEYS, BLK), BF16),
        pltpu.VMEM((8, BLK), F32),
        pltpu.VMEM((8, BLK), F32),
    ]
    right = step_right(pay, 1)
    left = step_left(pay, 1)
    acc, m, sums = call(
        first_body, (acc_t, m_t, sums_t), [SMEM, VMEM, VMEM], work, 3e9
    )(idx, q, pay)

    w_o = jnp.stack([w_own[:, 64:], w_sib[:, 64:]])
    w_o, _ = lax.optimization_barrier((w_o, sums))
    w_o = direct(w_o, "x")

    for k in range(1, 5):
        pays = (right, left) if k < 4 else (right,)
        if k < 4:
            right = step_right(pays[0], k + 1)
        if k < 3:
            left = step_left(pays[1], k + 1)
        ins = (idx, q) + pays + (acc, m, sums)
        if k < 4:
            outs, scratch, aliases = (acc_t, m_t, sums_t), work, {4: 0, 5: 1}
        else:
            outs, aliases = (sds((72, KEYS), F32), sds((72, KEYS), F32)), None
            scratch = work + [pltpu.VMEM(sums_t.shape, F32)]
        res = call(
            functools.partial(step_body, k),
            outs,
            [SMEM] + [VMEM] * (len(ins) - 1),
            scratch,
            6e9,
            aliases,
        )(*ins)
        if k < 4:
            acc, m, sums = res
        if k == 1:
            w_o, _ = lax.optimization_barrier((jnp.stack(w_o), sums))
            w_o = direct(w_o, "y")
    sib = shift(res[1], "c", 1)
    w_full = call(assemble_body, sds((D, D), BF16), [SMEM] + [VMEM] * 4)(idx, *w_o)
    att = call(merge_body, sds((KEYS, HD), BF16), [VMEM, VMEM])(res[0], sib)
    att = lax.all_to_all(att.reshape(16, 64, HD), ("x", "y"), 0, 0, tiled=True)
    return call(final_body, sds((OWN, D), BF16), [VMEM] * 3)(att, out_gain[None], w_full)


def solution(mesh):
    finer = Mesh(mesh.devices.reshape(NZ, NX, NC, NY), AXES)
    sp = ("z", "x", "c")

    return jax.shard_map(
        shards,
        mesh=finer,
        in_specs=(
            P(AXES, None),
            P(),
            P(sp, "y"),
            P(sp, "y"),
            P(sp, "y"),
            P(sp, "y"),
            P("y"),
            P(sp, "y"),
            P(),
        ),
        out_specs=P(AXES, None),
        check_vma=False,
    )
```

```python
import functools
import math

import jax
import jax.numpy as jnp
from jax import lax
from jax.experimental import pallas as pl
from jax.experimental.pallas import tpu as pltpu
from jax.sharding import Mesh
from jax.sharding import PartitionSpec as P


AXES = ("z", "x", "c", "y")
NZ, NX, NC, NY = 8, 4, 2, 4
SIZES = {"z": NZ, "x": NX, "c": NC, "y": NY}
D = 1024
HD = 64
TOTAL = 16384
OWN = 64
BLK = 256
KEYS = 1024
QS = 2048
PAY = 144
EPS = 1e-06
LOW = -1e30
F32 = jnp.float32
BF16 = jnp.bfloat16


VMEM = pl.BlockSpec(memory_space=pltpu.VMEM)
SMEM = pl.BlockSpec(memory_space=pltpu.SMEM)


def call(body, outs, ins, scratch=(), flops=1e8, aliases=None):
    return pl.pallas_call(
        body,
        out_shape=outs,
        in_specs=ins,
        out_specs=jax.tree.map(lambda _: VMEM, outs),
        scratch_shapes=list(scratch),
        input_output_aliases=aliases or {},
        cost_estimate=pl.CostEstimate(
            flops=int(flops), bytes_accessed=1 << 20, transcendentals=0
        ),
        compiler_params=pltpu.CompilerParams(vmem_limit_bytes=24 << 20),
    )


def shift(x, axis, k):
    n = SIZES[axis]
    return lax.ppermute(x, axis, [(i, (i + k) % n) for i in range(n)])


def direct(x, axis):
    return [x] + [shift(x, axis, k) for k in range(1, SIZES[axis])]


def step_right(x, k):
    return lax.ppermute(x, "z", [(i, i + 1) for i in range(k - 1, NZ - 1)])


def step_left(x, k):
    return lax.ppermute(x, "z", [((i - k + 1) % NZ, (i - k) % NZ) for i in range(3)])


def three_parts(x):
    hi = x.astype(BF16)
    rest = x - hi.astype(F32)
    mid = rest.astype(BF16)
    low = (rest - mid.astype(F32)).astype(BF16)
    return hi, mid, low


def pack_body(idx, tok, wq, wk, wv, wf, wo, lo, hi, p0, o0, s1, s2, s3, qv, kv, vv, fv, heads, sems):
    x = idx[1]
    sends = (s1, s2, s3)
    pairs = [(wq, qv), (wk, kv), (wv, vv), (wf, fv), (wo, o0)]
    pairs += [(tok.at[32:64], s.at[0:32]) for s in sends]
    pairs += [(tok.at[0:32], lo), (tok.at[32:64], hi)]
    copies = [pltpu.make_async_copy(a, b, sems.at[i]) for i, (a, b) in enumerate(pairs)]
    for copy in copies:
        copy.start()
    for s in sends:
        s[32:48, 512:1024] = jnp.zeros((16, 512), BF16)
    for copy in copies[:5]:
        copy.wait()
    head = lax.broadcasted_iota(jnp.int32, (NX, HD), 0)
    gates = fv[...].astype(F32)
    for h in range(NX):
        lanes = slice(h * HD, (h + 1) * HD)
        pick = jnp.where(head == h, 1.0, 0.0)
        gate = lax.dot_general(
            gates, pick, (((0,), (0,)), ((), ())), precision=lax.Precision.HIGHEST,
            preferred_element_type=F32,
        )
        heads[h] = jnp.concatenate([qv[:, lanes], kv[:, lanes], vv[:, lanes], gate.astype(BF16)], axis=1)
    p0[...] = heads[x]
    for k, s in enumerate(sends):
        s[32:48, 0:256] = heads[lax.rem(x + k + 1, NX)]
        s[32:48, 256:512] = o0[...]
    for copy in copies[5:]:
        copy.wait()


def spread_body(hi, p0, o0, r1, r2, r3, out, toks):
    toks[0:32, :] = hi[...]
    for k, r in enumerate((r1, r2, r3)):
        toks[32 * k + 32 : 32 * k + 64, :] = r[0:32, :]
    for z in range(NZ):
        out[z, 0:16, :] = p0[...]
        out[z, 64:80, :] = o0[...]
        for k, r in enumerate((r1, r2, r3)):
            out[z, 16 * k + 16 : 16 * k + 32, :] = r[32:48, 0:256]
            out[z, 16 * k + 80 : 16 * k + 96, :] = r[32:48, 256:512]


def project_body(idx, offs, *refs):
    toks = refs[:8]
    gain, w_own, w_sib = refs[8:11]
    qc_out, kv_out, cum_out = refs[11:14]
    w, rows = refs[14:]
    x, c, y = idx[1], idx[2], idx[3]
    for z in range(NZ):
        for xx in range(NX):
            base = z * 128 + lax.rem(x - xx + NX, NX) * 32
            own_at = pl.multiple_of(base + c * 16, 16)
            sib_at = pl.multiple_of(base + (1 - c) * 16, 16)
            w[pl.ds(own_at, 16), :] = w_own[z, xx * 16 : xx * 16 + 16, :]
            w[pl.ds(sib_at, 16), :] = w_sib[z, xx * 16 : xx * 16 + 16, :]
    for half in range(2):
        for outer in range(4):
            tok = toks[half * 4 + outer][...].astype(F32)
            scale = lax.rsqrt(jnp.mean(tok * tok, axis=-1, keepdims=True) + EPS)
            normed = (tok * scale * gain[...]).astype(BF16)
            out = jnp.dot(normed, w[...], preferred_element_type=F32)
            for inner in range(4):
                kx, ky = (outer, inner) if half == 0 else (inner, outer)
                xx = lax.rem(x - kx + NX, NX)
                yy = lax.rem(y - ky + NY, NY)
                at = pl.multiple_of(xx * BLK + yy * OWN + half * 32, 32)
                rows[pl.ds(at, 32), :] = out[inner * 32 : inner * 32 + 32, :]
    before = lax.broadcasted_iota(jnp.int32, (BLK, BLK), 0)
    after = lax.broadcasted_iota(jnp.int32, (BLK, BLK), 1)
    ones = jnp.where(before <= after, 1.0, 0.0).astype(BF16)
    for b in range(4):
        t = rows[b * BLK : (b + 1) * BLK, :].T
        lanes = slice(b * BLK, (b + 1) * BLK)
        qc_out[0:64, lanes] = t[:64].astype(BF16)
        kv_out[:, lanes] = t[64:192].astype(BF16)
        logit = t[192:200] + offs[x] + math.log(TOTAL)
        gate = jnp.minimum(logit, 0.0) - jnp.log1p(jnp.exp(-jnp.abs(logit)))
        hi, mid, low = three_parts(gate)
        cum = jnp.dot(hi, ones, preferred_element_type=F32)
        cum = cum + jnp.dot(mid, ones, preferred_element_type=F32)
        cum = cum + jnp.dot(low, ones, preferred_element_type=F32)
        cum_out[:, lanes] = cum
        row = lax.broadcasted_iota(jnp.int32, (16, BLK), 0)
        block = jnp.zeros((16, BLK), F32)
        for i, part in enumerate(three_parts(cum[0:1])):
            block = jnp.where(row == i, part.astype(F32), block)
        qc_out[64:80, lanes] = block.astype(BF16)


def prepare_body(idx, q_own, q_sib, kv, cum_own, q_out, pay_out):
    c = idx[2]
    q_out[80:128, :] = jnp.zeros((48, QS), BF16)
    row = lax.broadcasted_iota(jnp.int32, (16, QS), 0)
    q_out[64:80, :] = jnp.where(row < 3, 1.0, 0.0).astype(BF16)
    for b in range(4):
        lanes = slice(b * BLK, (b + 1) * BLK)
        own_at = pl.multiple_of((2 * b + c) * BLK, BLK)
        sib_at = pl.multiple_of((2 * b + 1 - c) * BLK, BLK)
        q_out[0:64, pl.ds(own_at, BLK)] = q_own[0:64, lanes] * jnp.asarray(0.125, BF16)
        q_out[0:64, pl.ds(sib_at, BLK)] = q_sib[0:64, lanes] * jnp.asarray(0.125, BF16)
    own, sib = [], []
    for b in range(4):
        end = slice(b * BLK + BLK - 1, b * BLK + BLK)
        own.append(cum_own[:, end])
        parts = q_sib[64:80, b * BLK + 128 : b * BLK + BLK].astype(F32)[:, 127:128]
        sib.append(jnp.broadcast_to(parts[0:1] + parts[1:2] + parts[2:3], (8, 1)))
    ahead = jnp.zeros_like(own[0])
    bases = []
    for b in range(4):
        bases.append(ahead + jnp.where(c == 1, sib[b], 0.0))
        ahead = ahead + (own[b] + sib[b])
    total = ahead
    pay_out[0:64, :] = kv[0:64, :]
    pay_out[80:144, :] = kv[64:128, :]
    row = lax.broadcasted_iota(jnp.int32, (16, BLK), 0)
    for b in range(4):
        lanes = slice(b * BLK, (b + 1) * BLK)
        bias = (total - bases[b]) - cum_own[:, lanes]
        parts = [p[0:1].astype(F32) for p in three_parts(bias)]
        totals = [p[0:1].astype(F32) for p in three_parts(jnp.broadcast_to(total, bias.shape))]
        block = jnp.zeros((16, BLK), F32)
        for i, part in enumerate(parts + totals):
            block = jnp.where(row == i, part, block)
        pay_out[64:80, lanes] = block.astype(BF16)


def chunk_total(pay):
    rows = pay[64:80, 0:BLK].astype(F32)
    return rows[3:4] + rows[4:5] + rows[5:6]


def place_chunk(pay, i, kx, vx):
    fill = jnp.zeros((48, 128), F32)
    for r in range(8):
        lanes = slice(r * 128, (r + 1) * 128)
        tile = jnp.concatenate([pay[0:80, lanes].astype(F32), fill], axis=0)
        kx[i, lanes, :] = tile.T.astype(BF16)
    vx[i, 0:64, :] = pay[80:144, :]
    vx[i, 64:80, :] = jnp.ones((16, KEYS), BF16)


def absorb(count, q, acc, m, kx, vx, move, work, c=None):
    tiles = QS // BLK
    bufs, tops, probs, fades = work[0:2], work[2:4], work[4:6], work[6:8]
    if c is not None:
        key = lax.broadcasted_iota(jnp.int32, (KEYS, BLK), 0)
        key_pos = key + (key // BLK + c) * BLK
        query = lax.broadcasted_iota(jnp.int32, (KEYS, BLK), 1)

    def lanes_of(t):
        return pl.ds(pl.multiple_of((t % tiles) * BLK, BLK), BLK)

    def score(t, slot):
        s = jnp.dot(kx[t // tiles], q[:, lanes_of(t)], preferred_element_type=F32)
        if c is not None:
            s = jnp.where(key_pos <= query + (t % tiles) * BLK, s, LOW)
        bufs[slot][...] = s
        tops[slot][...] = jnp.broadcast_to(jnp.max(s, axis=0, keepdims=True), (8, BLK))

    def weigh(t, slot):
        i, lanes = t // tiles, lanes_of(t)
        by = move[i, 0:1]
        old = m[i, 0:1, lanes]
        new = jnp.maximum(old, tops[slot][0:1] + by)
        probs[slot][...] = jnp.exp(bufs[slot][...] - (new - by)).astype(BF16)
        fades[slot][...] = jnp.broadcast_to(jnp.exp(old - new), (8, BLK))
        m[i, :, lanes] = jnp.broadcast_to(new, (8, BLK))

    def add(t, slot):
        i, lanes = t // tiles, lanes_of(t)
        part = jnp.dot(vx[i], probs[slot][...], preferred_element_type=F32)
        acc[i, :, lanes] = acc[i, :, lanes] * fades[slot][0:1] + part

    @pl.when(count > 0)
    def _():
        probs[1][...] = jnp.zeros((KEYS, BLK), BF16)
        fades[1][...] = jnp.ones((8, BLK), F32)
        score(0, 0)
        last = count * tiles - 1

        def two_tiles(j, carry):
            t = 2 * j
            add(jnp.maximum(t - 1, 0), 1)
            weigh(t, 0)
            score(t + 1, 1)
            add(t, 0)
            weigh(t + 1, 1)
            score(jnp.minimum(t + 2, last), 0)
            return carry

        lax.fori_loop(0, count * (tiles // 2), two_tiles, 0)
        add(last, 1)


def first_body(idx, q, pay, acc, m, sums, kx, vx, move, *bufs):
    acc[...] = jnp.zeros_like(acc)
    m[...] = jnp.full(m.shape, LOW, F32)
    move[...] = jnp.zeros_like(move)
    place_chunk(pay, 0, kx, vx)
    absorb(1, q, acc, m, kx, vx, move, bufs, idx[2])
    sums[...] = jnp.broadcast_to(chunk_total(pay), sums.shape)


def step_body(k, idx, q, *refs):
    z = idx[0]
    n_pay = 2 if k < 4 else 1
    pays, refs = refs[:n_pay], refs[n_pay:]
    acc0, m0, sums0, refs = refs[0], refs[1], refs[2], refs[3:]
    if k < 4:
        acc, m, sums, kx, vx, move, *bufs = refs
    else:
        out_own, out_sib, kx, vx, move, *bufs, sums = refs
        acc, m = acc0, m0
    sums[...] = sums0[...]
    count = (z >= k).astype(jnp.int32)

    @pl.when(z >= k)
    def _():
        place_chunk(pays[0], 0, kx, vx)
        move[0] = sums0[...]
        sums[...] = sums0[...] + jnp.broadcast_to(chunk_total(pays[0]), sums.shape)

    if k < 4:
        count = count + (z + k >= 8).astype(jnp.int32)

        @pl.when(z + k >= 8)
        def _():
            place_chunk(pays[1], 1, kx, vx)
            move[1] = jnp.zeros(sums.shape, F32)
            m[1] = m[1] + chunk_total(pays[1])[:, 0:1]

    absorb(count, q, acc, m, kx, vx, move, bufs)
    if k == 4:
        c = idx[2]
        row = lax.broadcasted_iota(jnp.int32, (8, BLK), 0)
        for b in range(4):
            for other in range(2):
                at = 2 * b + (c if other == 0 else 1 - c)
                lanes = pl.ds(pl.multiple_of(at * BLK, BLK), BLK)
                m_a = m[0, 0:1, lanes]
                m_b = m[1, 0:1, lanes] + sums[0:1]
                top = jnp.maximum(m_a, m_b)
                both = acc[0, :, lanes] * jnp.exp(m_a - top) + acc[1, :, lanes] * jnp.exp(m_b - top)
                to = slice(b * BLK, (b + 1) * BLK)
                out = out_own if other == 0 else out_sib
                out[0:64, to] = both[0:64]
                out[64:72, to] = jnp.where(row < 4, both[64:65], top)


def merge_body(own, sib, out):
    a, b = own[...], sib[...]
    m_a, m_b = a[68:69], b[68:69]
    top = jnp.maximum(m_a, m_b)
    f_a, f_b = jnp.exp(m_a - top), jnp.exp(m_b - top)
    total = a[64:65] * f_a + b[64:65] * f_b
    att = (a[0:64] * f_a + b[0:64] * f_b) / total
    att = jnp.concatenate([att, jnp.zeros_like(att)], axis=0)
    for r in range(8):
        out[r * 128 : (r + 1) * 128, :] = att[:, r * 128 : (r + 1) * 128].T[:, 0:64].astype(BF16)


def assemble_body(idx, w0, w1, w2, w3, w):
    x, c, y = idx[1], idx[2], idx[3]
    for ky, ref in enumerate((w0, w1, w2, w3)):
        cols = pl.ds(pl.multiple_of(lax.rem(y - ky + NY, NY) * 256, 256), 256)
        for kx in range(NX):
            xx = lax.rem(x - kx + NX, NX)
            for other in range(2):
                cc = c if other == 0 else 1 - c
                for z in range(NZ):
                    at = pl.multiple_of(z * 128 + xx * 32 + cc * 16, 16)
                    w[pl.ds(at, 16), cols] = ref[other, z, kx * 16 : kx * 16 + 16, :]


def final_body(att, gain, w, out):
    pieces = [att[xs * NY + ys] for ys in range(NY) for xs in range(NX)]
    joined = jnp.concatenate(pieces, axis=1)
    proj = lax.dot_general(joined, w[...], (((1,), (1,)), ((), ())), preferred_element_type=F32)
    scale = lax.rsqrt(jnp.mean(proj * proj, axis=-1, keepdims=True) + EPS)
    out[...] = (proj * scale * gain[...]).astype(BF16)


def shards(tokens, norm_gain, w_query, w_key, w_value, w_forget, forget_offset, w_out_t, out_gain):
    sds = jax.ShapeDtypeStruct
    idx = jnp.stack([lax.axis_index(a) for a in AXES]).astype(jnp.int32)

    half, piece, send = sds((32, D), BF16), sds((16, 256), BF16), sds((48, D), BF16)
    own_w = pltpu.VMEM((16, 256), BF16)
    lo, hi, p0, o0, *sends = call(
        pack_body,
        (half, half, piece, piece, send, send, send),
        [SMEM] + [pl.BlockSpec(memory_space=pl.ANY)] * 6,
        [own_w, own_w, own_w, pltpu.VMEM((NX, 16), BF16), pltpu.VMEM((NX, 16, 256), BF16)]
        + [pltpu.SemaphoreType.DMA((10,))],
    )(idx, tokens, w_query, w_key, w_value, w_forget.T, w_out_t)

    got = [shift(sends[k - 1], "x", k) for k in range(1, NX)]
    tok_a = direct(lo, "y")
    chunk, tok_b = call(
        spread_body, (sds((NZ, 128, 256), BF16), sds((128, D), BF16)), [VMEM] * 6
    )(hi, p0, o0, *got)
    w_own = lax.all_to_all(chunk, "z", 0, 0, tiled=True)
    toks = direct(jnp.concatenate(tok_a, axis=0), "x") + direct(tok_b, "y")
    w_sib = shift(w_own, "c", 1)

    q_own, kv, cum_own = call(
        project_body,
        (sds((80, KEYS), BF16), sds((128, KEYS), BF16), sds((8, KEYS), F32)),
        [SMEM, SMEM] + [VMEM] * 11,
        [pltpu.VMEM((D, 256), BF16), pltpu.VMEM((KEYS, 256), F32)],
        2e9,
    )(idx, forget_offset, *toks, norm_gain[None], w_own, w_sib)

    q_sib = shift(q_own, "c", 1)
    q, pay = call(
        prepare_body, (sds((128, QS), BF16), sds((PAY, KEYS), BF16)), [SMEM] + [VMEM] * 4
    )(idx, q_own, q_sib, kv, cum_own)

    acc_t, m_t, sums_t = sds((2, 80, QS), F32), sds((2, 8, QS), F32), sds((8, BLK), F32)
    work = [
        pltpu.VMEM((2, KEYS, 128), BF16),
        pltpu.VMEM((2, 80, KEYS), BF16),
        pltpu.VMEM((2, 8, BLK), F32),
        pltpu.VMEM((KEYS, BLK), F32),
        pltpu.VMEM((KEYS, BLK), F32),
        pltpu.VMEM((8, BLK), F32),
        pltpu.VMEM((8, BLK), F32),
        pltpu.VMEM((KEYS, BLK), BF16),
        pltpu.VMEM((KEYS, BLK), BF16),
        pltpu.VMEM((8, BLK), F32),
        pltpu.VMEM((8, BLK), F32),
    ]
    right = step_right(pay, 1)
    left = step_left(pay, 1)
    acc, m, sums = call(
        first_body, (acc_t, m_t, sums_t), [SMEM, VMEM, VMEM], work, 3e9
    )(idx, q, pay)

    w_o = jnp.stack([w_own[:, 64:], w_sib[:, 64:]])
    w_o, _ = lax.optimization_barrier((w_o, sums))
    w_o = direct(w_o, "y")

    for k in range(1, 5):
        pays = (right, left) if k < 4 else (right,)
        if k < 4:
            right = step_right(pays[0], k + 1)
        if k < 3:
            left = step_left(pays[1], k + 1)
        ins = (idx, q) + pays + (acc, m, sums)
        if k < 4:
            outs, scratch, aliases = (acc_t, m_t, sums_t), work, {4: 0, 5: 1}
        else:
            outs, aliases = (sds((72, KEYS), F32), sds((72, KEYS), F32)), None
            scratch = work + [pltpu.VMEM(sums_t.shape, F32)]
        res = call(
            functools.partial(step_body, k),
            outs,
            [SMEM] + [VMEM] * (len(ins) - 1),
            scratch,
            6e9,
            aliases,
        )(*ins)
        if k < 4:
            acc, m, sums = res
    sib = shift(res[1], "c", 1)
    w_full = call(assemble_body, sds((D, D), BF16), [SMEM] + [VMEM] * 4)(idx, *w_o)
    att = call(merge_body, sds((KEYS, HD), BF16), [VMEM, VMEM])(res[0], sib)
    att = lax.all_to_all(att.reshape(16, 64, HD), ("x", "y"), 0, 0, tiled=True)
    return call(final_body, sds((OWN, D), BF16), [VMEM] * 3)(att, out_gain[None], w_full)


def solution(mesh):
    finer = Mesh(mesh.devices.reshape(NZ, NX, NC, NY), AXES)
    sp = ("z", "x", "c")

    return jax.shard_map(
        shards,
        mesh=finer,
        in_specs=(
            P(AXES, None),
            P(),
            P(sp, "y"),
            P(sp, "y"),
            P(sp, "y"),
            P(sp, "y"),
            P("y"),
            P(sp, "y"),
            P(),
        ),
        out_specs=P(AXES, None),
        check_vma=False,
    )
```

```python
import functools
import math

import jax
import jax.numpy as jnp
from jax import lax
from jax.experimental import pallas as pl
from jax.experimental.pallas import tpu as pltpu
from jax.sharding import Mesh
from jax.sharding import PartitionSpec as P


AXES = ("z", "x", "c", "y")
NZ, NX, NC, NY = 8, 4, 2, 4
SIZES = {"z": NZ, "x": NX, "c": NC, "y": NY}
D = 1024
HD = 64
TOTAL = 16384
OWN = 64
BLK = 256
KEYS = 1024
QS = 2048
PAY = 144
EPS = 1e-06
LOW = -1e30
F32 = jnp.float32
BF16 = jnp.bfloat16


VMEM = pl.BlockSpec(memory_space=pltpu.VMEM)
SMEM = pl.BlockSpec(memory_space=pltpu.SMEM)


def call(body, outs, ins, scratch=(), flops=1e8, aliases=None):
    return pl.pallas_call(
        body,
        out_shape=outs,
        in_specs=ins,
        out_specs=jax.tree.map(lambda _: VMEM, outs),
        scratch_shapes=list(scratch),
        input_output_aliases=aliases or {},
        cost_estimate=pl.CostEstimate(
            flops=int(flops), bytes_accessed=1 << 20, transcendentals=0
        ),
        compiler_params=pltpu.CompilerParams(vmem_limit_bytes=24 << 20),
    )


def shift(x, axis, k):
    n = SIZES[axis]
    return lax.ppermute(x, axis, [(i, (i + k) % n) for i in range(n)])


def direct(x, axis):
    return [x] + [shift(x, axis, k) for k in range(1, SIZES[axis])]


def step_right(x, k):
    return lax.ppermute(x, "z", [(i, i + 1) for i in range(k - 1, NZ - 1)])


def step_left(x, k):
    return lax.ppermute(x, "z", [((i - k + 1) % NZ, (i - k) % NZ) for i in range(3)])


def three_parts(x):
    hi = x.astype(BF16)
    rest = x - hi.astype(F32)
    mid = rest.astype(BF16)
    low = (rest - mid.astype(F32)).astype(BF16)
    return hi, mid, low


def pack_body(idx, tok, w, lo, hi, p0, o0, s1, s2, s3, heads):
    x = idx[1]
    lo[...] = tok[0:32, :]
    hi[...] = tok[32:64, :]
    o0[...] = w[48:64, :]
    head = lax.broadcasted_iota(jnp.int32, (16, HD), 0)
    gates = w[64:80, 0:128].astype(F32)
    for h in range(NX):
        lanes = slice(h * HD, (h + 1) * HD)
        pick = jnp.where(head == h, 1.0, 0.0)
        gate = lax.dot_general(
            gates, pick, (((0,), (0,)), ((), ())), precision=lax.Precision.HIGHEST,
            preferred_element_type=F32,
        )[0:16]
        mine = [w[0:16, lanes], w[16:32, lanes], w[32:48, lanes], gate.astype(BF16)]
        heads[h] = jnp.concatenate(mine, axis=1)
    p0[...] = heads[x]
    for k, s in enumerate((s1, s2, s3)):
        s[0:32, :] = tok[32:64, :]
        s[32:48, 0:256] = heads[lax.rem(x + k + 1, NX)]
        s[32:48, 256:512] = w[48:64, :]
        s[32:48, 512:1024] = jnp.zeros((16, 512), BF16)


def spread_body(hi, p0, o0, r1, r2, r3, out, toks):
    toks[0:32, :] = hi[...]
    for k, r in enumerate((r1, r2, r3)):
        toks[32 * k + 32 : 32 * k + 64, :] = r[0:32, :]
    for z in range(NZ):
        out[z, 0:16, :] = p0[...]
        out[z, 64:80, :] = o0[...]
        for k, r in enumerate((r1, r2, r3)):
            out[z, 16 * k + 16 : 16 * k + 32, :] = r[32:48, 0:256]
            out[z, 16 * k + 80 : 16 * k + 96, :] = r[32:48, 256:512]


def project_body(idx, offs, *refs):
    toks = refs[:8]
    gain, w_own, w_sib = refs[8:11]
    qc_out, kv_out, cum_out = refs[11:14]
    w, rows = refs[14:]
    x, c, y = idx[1], idx[2], idx[3]
    for z in range(NZ):
        for xx in range(NX):
            base = z * 128 + lax.rem(x - xx + NX, NX) * 32
            own_at = pl.multiple_of(base + c * 16, 16)
            sib_at = pl.multiple_of(base + (1 - c) * 16, 16)
            w[pl.ds(own_at, 16), :] = w_own[z, xx * 16 : xx * 16 + 16, :]
            w[pl.ds(sib_at, 16), :] = w_sib[z, xx * 16 : xx * 16 + 16, :]
    for half in range(2):
        for outer in range(4):
            tok = toks[half * 4 + outer][...].astype(F32)
            scale = lax.rsqrt(jnp.mean(tok * tok, axis=-1, keepdims=True) + EPS)
            normed = (tok * scale * gain[...]).astype(BF16)
            out = jnp.dot(normed, w[...], preferred_element_type=F32)
            for inner in range(4):
                kx, ky = (outer, inner) if half == 0 else (inner, outer)
                xx = lax.rem(x - kx + NX, NX)
                yy = lax.rem(y - ky + NY, NY)
                at = pl.multiple_of(xx * BLK + yy * OWN + half * 32, 32)
                rows[pl.ds(at, 32), :] = out[inner * 32 : inner * 32 + 32, :]
    before = lax.broadcasted_iota(jnp.int32, (BLK, BLK), 0)
    after = lax.broadcasted_iota(jnp.int32, (BLK, BLK), 1)
    ones = jnp.where(before <= after, 1.0, 0.0).astype(BF16)
    for b in range(4):
        t = rows[b * BLK : (b + 1) * BLK, :].T
        lanes = slice(b * BLK, (b + 1) * BLK)
        qc_out[0:64, lanes] = t[:64].astype(BF16)
        kv_out[:, lanes] = t[64:192].astype(BF16)
        logit = t[192:200] + offs[x] + math.log(TOTAL)
        gate = jnp.minimum(logit, 0.0) - jnp.log1p(jnp.exp(-jnp.abs(logit)))
        hi, mid, low = three_parts(gate)
        cum = jnp.dot(hi, ones, preferred_element_type=F32)
        cum = cum + jnp.dot(mid, ones, preferred_element_type=F32)
        cum = cum + jnp.dot(low, ones, preferred_element_type=F32)
        cum_out[:, lanes] = cum
        row = lax.broadcasted_iota(jnp.int32, (16, BLK), 0)
        block = jnp.zeros((16, BLK), F32)
        for i, part in enumerate(three_parts(cum[0:1])):
            block = jnp.where(row == i, part.astype(F32), block)
        qc_out[64:80, lanes] = block.astype(BF16)


def prepare_body(idx, q_own, q_sib, kv, cum_own, q_out, pay_out):
    c = idx[2]
    q_out[80:128, :] = jnp.zeros((48, QS), BF16)
    row = lax.broadcasted_iota(jnp.int32, (16, QS), 0)
    q_out[64:80, :] = jnp.where(row < 3, 1.0, 0.0).astype(BF16)
    for b in range(4):
        lanes = slice(b * BLK, (b + 1) * BLK)
        own_at = pl.multiple_of((2 * b + c) * BLK, BLK)
        sib_at = pl.multiple_of((2 * b + 1 - c) * BLK, BLK)
        q_out[0:64, pl.ds(own_at, BLK)] = q_own[0:64, lanes] * jnp.asarray(0.125, BF16)
        q_out[0:64, pl.ds(sib_at, BLK)] = q_sib[0:64, lanes] * jnp.asarray(0.125, BF16)
    own, sib = [], []
    for b in range(4):
        end = slice(b * BLK + BLK - 1, b * BLK + BLK)
        own.append(cum_own[:, end])
        parts = q_sib[64:80, b * BLK + 128 : b * BLK + BLK].astype(F32)[:, 127:128]
        sib.append(jnp.broadcast_to(parts[0:1] + parts[1:2] + parts[2:3], (8, 1)))
    ahead = jnp.zeros_like(own[0])
    bases = []
    for b in range(4):
        bases.append(ahead + jnp.where(c == 1, sib[b], 0.0))
        ahead = ahead + (own[b] + sib[b])
    total = ahead
    pay_out[0:64, :] = kv[0:64, :]
    pay_out[80:144, :] = kv[64:128, :]
    row = lax.broadcasted_iota(jnp.int32, (16, BLK), 0)
    for b in range(4):
        lanes = slice(b * BLK, (b + 1) * BLK)
        bias = (total - bases[b]) - cum_own[:, lanes]
        parts = [p[0:1].astype(F32) for p in three_parts(bias)]
        totals = [p[0:1].astype(F32) for p in three_parts(jnp.broadcast_to(total, bias.shape))]
        block = jnp.zeros((16, BLK), F32)
        for i, part in enumerate(parts + totals):
            block = jnp.where(row == i, part, block)
        pay_out[64:80, lanes] = block.astype(BF16)


def chunk_total(pay):
    rows = pay[64:80, 0:BLK].astype(F32)
    return rows[3:4] + rows[4:5] + rows[5:6]


def place_chunk(pay, i, kx, vx):
    fill = jnp.zeros((48, 128), F32)
    for r in range(8):
        lanes = slice(r * 128, (r + 1) * 128)
        tile = jnp.concatenate([pay[0:80, lanes].astype(F32), fill], axis=0)
        kx[i, lanes, :] = tile.T.astype(BF16)
    vx[i, 0:64, :] = pay[80:144, :]
    vx[i, 64:80, :] = jnp.ones((16, KEYS), BF16)


def stages(q, acc, m, kx, vx, move, work):
    tiles = QS // BLK
    bufs, tops, probs, fades = work[0:2], work[2:4], work[4:6], work[6:8]

    def lanes_of(t):
        if isinstance(t, int):
            return slice((t % tiles) * BLK, (t % tiles + 1) * BLK)
        return pl.ds(pl.multiple_of((t % tiles) * BLK, BLK), BLK)

    def score(t, slot, n=KEYS, allowed=None):
        s = jnp.dot(kx[t // tiles, 0:n], q[:, lanes_of(t)], preferred_element_type=F32)
        if allowed is not None:
            last = jnp.where(allowed, s[n - BLK : n], LOW)
            s = last if n == BLK else jnp.concatenate([s[0 : n - BLK], last], axis=0)
        bufs[slot][0:n] = s
        tops[slot][...] = jnp.broadcast_to(jnp.max(s, axis=0, keepdims=True), (8, BLK))

    def weigh(t, slot, n=KEYS):
        i, lanes = t // tiles, lanes_of(t)
        by = move[i, 0:1]
        old = m[i, 0:1, lanes]
        new = jnp.maximum(old, tops[slot][0:1] + by)
        probs[slot][0:n] = jnp.exp(bufs[slot][0:n] - (new - by)).astype(BF16)
        fades[slot][...] = jnp.broadcast_to(jnp.exp(old - new), (8, BLK))
        m[i, :, lanes] = jnp.broadcast_to(new, (8, BLK))

    def add(t, slot, n=KEYS):
        i, lanes = t // tiles, lanes_of(t)
        part = jnp.dot(vx[i, :, 0:n], probs[slot][0:n], preferred_element_type=F32)
        acc[i, :, lanes] = acc[i, :, lanes] * fades[slot][0:1] + part

    return score, weigh, add


def absorb(count, q, acc, m, kx, vx, move, work):
    tiles = QS // BLK
    score, weigh, add = stages(q, acc, m, kx, vx, move, work)
    probs, fades = work[4:6], work[6:8]

    @pl.when(count > 0)
    def _():
        probs[1][...] = jnp.zeros((KEYS, BLK), BF16)
        fades[1][...] = jnp.ones((8, BLK), F32)
        score(0, 0)
        last = count * tiles - 1

        def two_tiles(j, carry):
            t = 2 * j
            add(jnp.maximum(t - 1, 0), 1)
            weigh(t, 0)
            score(t + 1, 1)
            add(t, 0)
            weigh(t + 1, 1)
            score(jnp.minimum(t + 2, last), 0)
            return carry

        lax.fori_loop(0, count * (tiles // 2), two_tiles, 0)
        add(last, 1)


def first_body(idx, q, pay, acc, m, sums, kx, vx, move, *bufs):
    acc[...] = jnp.zeros_like(acc)
    m[...] = jnp.full(m.shape, LOW, F32)
    move[...] = jnp.zeros_like(move)
    place_chunk(pay, 0, kx, vx)
    score, weigh, add = stages(q, acc, m, kx, vx, move, bufs)
    key = lax.broadcasted_iota(jnp.int32, (BLK, BLK), 0)
    query = lax.broadcasted_iota(jnp.int32, (BLK, BLK), 1)
    tiles = QS // BLK
    meets = [(b // 2 + 1) * BLK for b in range(tiles)]
    masks = [key + (idx[2] - odd) * BLK <= query for odd in range(2)]
    for b in range(tiles + 2):
        if b < tiles:
            score(b, b % 2, meets[b], masks[b % 2])
        if 0 <= b - 1 < tiles:
            weigh(b - 1, (b - 1) % 2, meets[b - 1])
        if 0 <= b - 2:
            add(b - 2, (b - 2) % 2, meets[b - 2])
    sums[...] = jnp.broadcast_to(chunk_total(pay), sums.shape)


def step_body(k, idx, q, *refs):
    z = idx[0]
    n_pay = 2 if k < 4 else 1
    pays, refs = refs[:n_pay], refs[n_pay:]
    acc0, m0, sums0, refs = refs[0], refs[1], refs[2], refs[3:]
    if k < 4:
        acc, m, sums, kx, vx, move, *bufs = refs
    else:
        out_own, out_sib, kx, vx, move, *bufs, sums = refs
        acc, m = acc0, m0
    sums[...] = sums0[...]
    count = (z >= k).astype(jnp.int32)

    @pl.when(z >= k)
    def _():
        place_chunk(pays[0], 0, kx, vx)
        move[0] = sums0[...]
        sums[...] = sums0[...] + jnp.broadcast_to(chunk_total(pays[0]), sums.shape)

    if k < 4:
        count = count + (z + k >= 8).astype(jnp.int32)

        @pl.when(z + k >= 8)
        def _():
            place_chunk(pays[1], 1, kx, vx)
            move[1] = jnp.zeros(sums.shape, F32)
            m[1] = m[1] + chunk_total(pays[1])[:, 0:1]

    absorb(count, q, acc, m, kx, vx, move, bufs)
    if k == 4:
        c = idx[2]
        row = lax.broadcasted_iota(jnp.int32, (8, BLK), 0)
        for b in range(4):
            for other in range(2):
                at = 2 * b + (c if other == 0 else 1 - c)
                lanes = pl.ds(pl.multiple_of(at * BLK, BLK), BLK)
                m_a = m[0, 0:1, lanes]
                m_b = m[1, 0:1, lanes] + sums[0:1]
                top = jnp.maximum(m_a, m_b)
                both = acc[0, :, lanes] * jnp.exp(m_a - top) + acc[1, :, lanes] * jnp.exp(m_b - top)
                to = slice(b * BLK, (b + 1) * BLK)
                out = out_own if other == 0 else out_sib
                out[0:64, to] = both[0:64]
                out[64:72, to] = jnp.where(row < 4, both[64:65], top)


def merge_body(idx, own, sib, *outs):
    x = idx[1]
    outs, parts = outs[:NX], outs[NX]
    a, b = own[...], sib[...]
    m_a, m_b = a[68:69], b[68:69]
    top = jnp.maximum(m_a, m_b)
    f_a, f_b = jnp.exp(m_a - top), jnp.exp(m_b - top)
    total = a[64:65] * f_a + b[64:65] * f_b
    att = (a[0:64] * f_a + b[0:64] * f_b) / total
    att = jnp.concatenate([att, jnp.zeros_like(att)], axis=0)
    for r in range(8):
        tile = att[:, r * 128 : (r + 1) * 128].T[:, 0:64].astype(BF16)
        parts[r // 2, (r % 2) * 128 : (r % 2) * 128 + 128, :] = tile
    for k, out in enumerate(outs):
        out[...] = parts[lax.rem(x + k, NX)]


def regroup_body(idx, h0, h1, h2, h3, *outs):
    x, y = idx[1], idx[3]
    outs, heads = outs[:NY], outs[NY]
    for k, h in enumerate((h0, h1, h2, h3)):
        heads[lax.rem(x - k + NX, NX)] = h[...]
    for k, out in enumerate(outs):
        rows = pl.ds(pl.multiple_of(lax.rem(y + k, NY) * OWN, OWN), OWN)
        out[...] = jnp.concatenate([heads[i, rows, :] for i in range(NX)], axis=1)


def assemble_body(idx, w0, w1, w2, w3, w):
    x, c, y = idx[1], idx[2], idx[3]
    for ky, ref in enumerate((w0, w1, w2, w3)):
        cols = pl.ds(pl.multiple_of(lax.rem(y - ky + NY, NY) * 256, 256), 256)
        for kx in range(NX):
            xx = lax.rem(x - kx + NX, NX)
            for other in range(2):
                cc = c if other == 0 else 1 - c
                for z in range(NZ):
                    at = pl.multiple_of(z * 128 + xx * 32 + cc * 16, 16)
                    w[pl.ds(at, 16), cols] = ref[other, z, kx * 16 : kx * 16 + 16, :]


def final_body(idx, a0, a1, a2, a3, gain, w, out, joined):
    y = idx[3]
    for k, a in enumerate((a0, a1, a2, a3)):
        cols = pl.ds(pl.multiple_of(lax.rem(y - k + NY, NY) * 256, 256), 256)
        joined[:, cols] = a[...]
    proj = lax.dot_general(
        joined[...], w[...], (((1,), (1,)), ((), ())), preferred_element_type=F32
    )
    scale = lax.rsqrt(jnp.mean(proj * proj, axis=-1, keepdims=True) + EPS)
    out[...] = (proj * scale * gain[...]).astype(BF16)


def shards(tokens, norm_gain, w_query, w_key, w_value, w_forget, forget_offset, w_out_t, out_gain):
    sds = jax.ShapeDtypeStruct
    idx = jnp.stack([lax.axis_index(a) for a in AXES]).astype(jnp.int32)

    half, piece, send = sds((32, D), BF16), sds((16, 256), BF16), sds((48, D), BF16)
    gate_rows = jnp.pad(w_forget.T, ((0, 16 - NX), (0, 256 - 16)))
    weights = jnp.concatenate([w_query, w_key, w_value, w_out_t, gate_rows], axis=0)
    lo, hi, p0, o0, *sends = call(
        pack_body,
        (half, half, piece, piece, send, send, send),
        [SMEM, VMEM, VMEM],
        [pltpu.VMEM((NX, 16, 256), BF16)],
    )(idx, tokens, weights)

    got = [shift(sends[k - 1], "x", k) for k in range(1, NX)]
    tok_a = direct(lo, "y")
    chunk, tok_b = call(
        spread_body, (sds((NZ, 128, 256), BF16), sds((128, D), BF16)), [VMEM] * 6
    )(hi, p0, o0, *got)
    w_own = lax.all_to_all(chunk, "z", 0, 0, tiled=True)
    toks = direct(jnp.concatenate(tok_a, axis=0), "x") + direct(tok_b, "y")
    w_sib = shift(w_own, "c", 1)

    q_own, kv, cum_own = call(
        project_body,
        (sds((80, KEYS), BF16), sds((128, KEYS), BF16), sds((8, KEYS), F32)),
        [SMEM, SMEM] + [VMEM] * 11,
        [pltpu.VMEM((D, 256), BF16), pltpu.VMEM((KEYS, 256), F32)],
        2e9,
    )(idx, forget_offset, *toks, norm_gain[None], w_own, w_sib)

    q_sib = shift(q_own, "c", 1)
    w_o = direct(jnp.stack([w_own[:, 64:], w_sib[:, 64:]]), "y")
    q, pay = call(
        prepare_body,
        (sds((128, QS), BF16), sds((PAY, KEYS), BF16)),
        [SMEM] + [VMEM] * 4,
    )(idx, q_own, q_sib, kv, cum_own)

    acc_t, m_t, sums_t = sds((2, 80, QS), F32), sds((2, 8, QS), F32), sds((8, BLK), F32)
    work = [
        pltpu.VMEM((2, KEYS, 128), BF16),
        pltpu.VMEM((2, 80, KEYS), BF16),
        pltpu.VMEM((2, 8, BLK), F32),
        pltpu.VMEM((KEYS, BLK), F32),
        pltpu.VMEM((KEYS, BLK), F32),
        pltpu.VMEM((8, BLK), F32),
        pltpu.VMEM((8, BLK), F32),
        pltpu.VMEM((KEYS, BLK), BF16),
        pltpu.VMEM((KEYS, BLK), BF16),
        pltpu.VMEM((8, BLK), F32),
        pltpu.VMEM((8, BLK), F32),
    ]
    right = step_right(pay, 1)
    left = step_left(pay, 1)
    acc, m, sums = call(
        first_body, (acc_t, m_t, sums_t), [SMEM, VMEM, VMEM], work, 3e9
    )(idx, q, pay)

    for k in range(1, 5):
        pays = (right, left) if k < 4 else (right,)
        if k < 4:
            right = step_right(pays[0], k + 1)
        if k < 3:
            left = step_left(pays[1], k + 1)
        ins = (idx, q) + pays + (acc, m, sums)
        if k < 4:
            outs, scratch, aliases = (acc_t, m_t, sums_t), work, {4: 0, 5: 1}
        else:
            outs, aliases = (sds((72, KEYS), F32), sds((72, KEYS), F32)), None
            scratch = work + [pltpu.VMEM(sums_t.shape, F32)]
        res = call(
            functools.partial(step_body, k),
            outs,
            [SMEM] + [VMEM] * (len(ins) - 1),
            scratch,
            6e9,
            aliases,
        )(*ins)
        if k < 4:
            acc, m, sums = res
    sib = shift(res[1], "c", 1)
    w_full = call(assemble_body, sds((D, D), BF16), [SMEM] + [VMEM] * 4)(idx, *w_o)
    rows = sds((BLK, HD), BF16)
    parts = call(
        merge_body, (rows,) * NX, [SMEM, VMEM, VMEM], [pltpu.VMEM((NX, BLK, HD), BF16)]
    )(idx, res[0], sib)
    parts = [parts[0]] + [shift(parts[k], "x", k) for k in range(1, NX)]
    parts = call(
        regroup_body,
        (sds((OWN, 256), BF16),) * NY,
        [SMEM] + [VMEM] * NX,
        [pltpu.VMEM((NX, BLK, HD), BF16)],
    )(idx, *parts)
    parts = [parts[0]] + [shift(parts[k], "y", k) for k in range(1, NY)]
    return call(
        final_body,
        sds((OWN, D), BF16),
        [SMEM] + [VMEM] * (NY + 2),
        [pltpu.VMEM((OWN, D), BF16)],
    )(idx, *parts, out_gain[None], w_full)


def solution(mesh):
    finer = Mesh(mesh.devices.reshape(NZ, NX, NC, NY), AXES)
    sp = ("z", "x", "c")

    return jax.shard_map(
        shards,
        mesh=finer,
        in_specs=(
            P(AXES, None),
            P(),
            P(sp, "y"),
            P(sp, "y"),
            P(sp, "y"),
            P(sp, "y"),
            P("y"),
            P(sp, "y"),
            P(),
        ),
        out_specs=P(AXES, None),
        check_vma=False,
    )
```

```python
import functools
import math

import jax
import jax.numpy as jnp
from jax import lax
from jax.experimental import pallas as pl
from jax.experimental.pallas import tpu as pltpu
from jax.sharding import Mesh
from jax.sharding import PartitionSpec as P


AXES = ("z", "x", "c", "y")
NZ, NX, NC, NY = 8, 4, 2, 4
SIZES = {"z": NZ, "x": NX, "c": NC, "y": NY}
D = 1024
HD = 64
TOTAL = 16384
OWN = 64
BLK = 256
KEYS = 1024
QS = 2048
PAY = 144
EPS = 1e-06
LOW = -1e30
F32 = jnp.float32
BF16 = jnp.bfloat16


VMEM = pl.BlockSpec(memory_space=pltpu.VMEM)
SMEM = pl.BlockSpec(memory_space=pltpu.SMEM)


def call(body, outs, ins, scratch=(), flops=1e8, aliases=None):
    return pl.pallas_call(
        body,
        out_shape=outs,
        in_specs=ins,
        out_specs=jax.tree.map(lambda _: VMEM, outs),
        scratch_shapes=list(scratch),
        input_output_aliases=aliases or {},
        cost_estimate=pl.CostEstimate(
            flops=int(flops), bytes_accessed=1 << 20, transcendentals=0
        ),
        compiler_params=pltpu.CompilerParams(vmem_limit_bytes=24 << 20),
    )


def shift(x, axis, k):
    n = SIZES[axis]
    return lax.ppermute(x, axis, [(i, (i + k) % n) for i in range(n)])


def direct(x, axis):
    return [x] + [shift(x, axis, k) for k in range(1, SIZES[axis])]


def step_right(x, k):
    return lax.ppermute(x, "z", [(i, i + 1) for i in range(k - 1, NZ - 1)])


def step_left(x, k):
    return lax.ppermute(x, "z", [((i - k + 1) % NZ, (i - k) % NZ) for i in range(3)])


def three_parts(x):
    hi = x.astype(BF16)
    rest = x - hi.astype(F32)
    mid = rest.astype(BF16)
    low = (rest - mid.astype(F32)).astype(BF16)
    return hi, mid, low


def pack_body(idx, rows, lo, hi, p0, o0, s1, s2, s3, heads):
    x = idx[1]
    lo[...] = rows[0:32, :]
    hi[...] = rows[32:64, :]
    o0[...] = rows[64:80, 768:1024]
    head = lax.broadcasted_iota(jnp.int32, (16, HD), 0)
    gates = rows[80:96, 0:128].astype(F32)
    for h in range(NX):
        pick = jnp.where(head == h, 1.0, 0.0)
        gate = lax.dot_general(
            gates, pick, (((0,), (0,)), ((), ())), precision=lax.Precision.HIGHEST,
            preferred_element_type=F32,
        )[0:16]
        mine = [rows[64:80, i * 256 + h * HD : i * 256 + h * HD + HD] for i in range(3)]
        heads[h] = jnp.concatenate(mine + [gate.astype(BF16)], axis=1)
    p0[...] = heads[x]
    for k, s in enumerate((s1, s2, s3)):
        s[0:32, :] = rows[32:64, :]
        s[32:48, 0:256] = heads[lax.rem(x + k + 1, NX)]
        s[32:48, 256:512] = rows[64:80, 768:1024]
        s[32:48, 512:1024] = jnp.zeros((16, 512), BF16)


def spread_body(hi, p0, o0, r1, r2, r3, out, toks):
    toks[0:32, :] = hi[...]
    for k, r in enumerate((r1, r2, r3)):
        toks[32 * k + 32 : 32 * k + 64, :] = r[0:32, :]
    for z in range(NZ):
        out[z, 0:16, :] = p0[...]
        out[z, 64:80, :] = o0[...]
        for k, r in enumerate((r1, r2, r3)):
            out[z, 16 * k + 16 : 16 * k + 32, :] = r[32:48, 0:256]
            out[z, 16 * k + 80 : 16 * k + 96, :] = r[32:48, 256:512]


def project_body(idx, offs, *refs):
    toks = refs[:8]
    gain, w_own, w_sib = refs[8:11]
    qc_out, kv_out, cum_out = refs[11:14]
    w, rows = refs[14:]
    x, c, y = idx[1], idx[2], idx[3]
    for z in range(NZ):
        for xx in range(NX):
            base = z * 128 + lax.rem(x - xx + NX, NX) * 32
            own_at = pl.multiple_of(base + c * 16, 16)
            sib_at = pl.multiple_of(base + (1 - c) * 16, 16)
            w[pl.ds(own_at, 16), :] = w_own[z, xx * 16 : xx * 16 + 16, :]
            w[pl.ds(sib_at, 16), :] = w_sib[z, xx * 16 : xx * 16 + 16, :]
    for half in range(2):
        for outer in range(4):
            tok = toks[half * 4 + outer][...].astype(F32)
            scale = lax.rsqrt(jnp.mean(tok * tok, axis=-1, keepdims=True) + EPS)
            normed = (tok * scale * gain[...]).astype(BF16)
            out = jnp.dot(normed, w[...], preferred_element_type=F32)
            for inner in range(4):
                kx, ky = (outer, inner) if half == 0 else (inner, outer)
                xx = lax.rem(x - kx + NX, NX)
                yy = lax.rem(y - ky + NY, NY)
                at = pl.multiple_of(xx * BLK + yy * OWN + half * 32, 32)
                rows[pl.ds(at, 32), :] = out[inner * 32 : inner * 32 + 32, :]
    before = lax.broadcasted_iota(jnp.int32, (BLK, BLK), 0)
    after = lax.broadcasted_iota(jnp.int32, (BLK, BLK), 1)
    ones = jnp.where(before <= after, 1.0, 0.0).astype(BF16)
    for b in range(4):
        t = rows[b * BLK : (b + 1) * BLK, :].T
        lanes = slice(b * BLK, (b + 1) * BLK)
        qc_out[0:64, lanes] = t[:64].astype(BF16)
        kv_out[:, lanes] = t[64:192].astype(BF16)
        logit = t[192:200] + offs[x] + math.log(TOTAL)
        gate = jnp.minimum(logit, 0.0) - jnp.log1p(jnp.exp(-jnp.abs(logit)))
        hi, mid, low = three_parts(gate)
        cum = jnp.dot(hi, ones, preferred_element_type=F32)
        cum = cum + jnp.dot(mid, ones, preferred_element_type=F32)
        cum = cum + jnp.dot(low, ones, preferred_element_type=F32)
        cum_out[:, lanes] = cum
        row = lax.broadcasted_iota(jnp.int32, (16, BLK), 0)
        block = jnp.zeros((16, BLK), F32)
        for i, part in enumerate(three_parts(cum[0:1])):
            block = jnp.where(row == i, part.astype(F32), block)
        qc_out[64:80, lanes] = block.astype(BF16)


def prepare_body(idx, q_own, q_sib, kv, cum_own, q_out, pay_out):
    c = idx[2]
    q_out[80:128, :] = jnp.zeros((48, QS), BF16)
    row = lax.broadcasted_iota(jnp.int32, (16, QS), 0)
    q_out[64:80, :] = jnp.where(row < 3, 1.0, 0.0).astype(BF16)
    for b in range(4):
        lanes = slice(b * BLK, (b + 1) * BLK)
        own_at = pl.multiple_of((2 * b + c) * BLK, BLK)
        sib_at = pl.multiple_of((2 * b + 1 - c) * BLK, BLK)
        q_out[0:64, pl.ds(own_at, BLK)] = q_own[0:64, lanes] * jnp.asarray(0.125, BF16)
        q_out[0:64, pl.ds(sib_at, BLK)] = q_sib[0:64, lanes] * jnp.asarray(0.125, BF16)
    own, sib = [], []
    for b in range(4):
        end = slice(b * BLK + BLK - 1, b * BLK + BLK)
        own.append(cum_own[:, end])
        parts = q_sib[64:80, b * BLK + 128 : b * BLK + BLK].astype(F32)[:, 127:128]
        sib.append(jnp.broadcast_to(parts[0:1] + parts[1:2] + parts[2:3], (8, 1)))
    ahead = jnp.zeros_like(own[0])
    bases = []
    for b in range(4):
        bases.append(ahead + jnp.where(c == 1, sib[b], 0.0))
        ahead = ahead + (own[b] + sib[b])
    total = ahead
    pay_out[0:64, :] = kv[0:64, :]
    pay_out[80:144, :] = kv[64:128, :]
    row = lax.broadcasted_iota(jnp.int32, (16, BLK), 0)
    for b in range(4):
        lanes = slice(b * BLK, (b + 1) * BLK)
        bias = (total - bases[b]) - cum_own[:, lanes]
        parts = [p[0:1].astype(F32) for p in three_parts(bias)]
        totals = [p[0:1].astype(F32) for p in three_parts(jnp.broadcast_to(total, bias.shape))]
        block = jnp.zeros((16, BLK), F32)
        for i, part in enumerate(parts + totals):
            block = jnp.where(row == i, part, block)
        pay_out[64:80, lanes] = block.astype(BF16)


def chunk_total(pay):
    rows = pay[64:80, 0:BLK].astype(F32)
    return rows[3:4] + rows[4:5] + rows[5:6]


def place_chunk(pay, i, kx, vx):
    fill = jnp.zeros((48, 128), F32)
    for r in range(8):
        lanes = slice(r * 128, (r + 1) * 128)
        tile = jnp.concatenate([pay[0:80, lanes].astype(F32), fill], axis=0)
        kx[i, lanes, :] = tile.T.astype(BF16)
    vx[i, 0:64, :] = pay[80:144, :]
    vx[i, 64:80, :] = jnp.ones((16, KEYS), BF16)


def stages(q, acc, m, kx, vx, move, work):
    tiles = QS // BLK
    bufs, tops, probs, fades = work[0:2], work[2:4], work[4:6], work[6:8]

    def lanes_of(t):
        if isinstance(t, int):
            return slice((t % tiles) * BLK, (t % tiles + 1) * BLK)
        return pl.ds(pl.multiple_of((t % tiles) * BLK, BLK), BLK)

    def score(t, slot, n=KEYS, allowed=None):
        s = jnp.dot(kx[t // tiles, 0:n], q[:, lanes_of(t)], preferred_element_type=F32)
        if allowed is not None:
            last = jnp.where(allowed, s[n - BLK : n], LOW)
            s = last if n == BLK else jnp.concatenate([s[0 : n - BLK], last], axis=0)
        bufs[slot][0:n] = s
        tops[slot][...] = jnp.broadcast_to(jnp.max(s, axis=0, keepdims=True), (8, BLK))

    def weigh(t, slot, n=KEYS):
        i, lanes = t // tiles, lanes_of(t)
        by = move[i, 0:1]
        old = m[i, 0:1, lanes]
        new = jnp.maximum(old, tops[slot][0:1] + by)
        probs[slot][0:n] = jnp.exp(bufs[slot][0:n] - (new - by)).astype(BF16)
        fades[slot][...] = jnp.broadcast_to(jnp.exp(old - new), (8, BLK))
        m[i, :, lanes] = jnp.broadcast_to(new, (8, BLK))

    def add(t, slot, n=KEYS):
        i, lanes = t // tiles, lanes_of(t)
        part = jnp.dot(vx[i, :, 0:n], probs[slot][0:n], preferred_element_type=F32)
        acc[i, :, lanes] = acc[i, :, lanes] * fades[slot][0:1] + part

    return score, weigh, add


def absorb(count, q, acc, m, kx, vx, move, work):
    tiles = QS // BLK
    score, weigh, add = stages(q, acc, m, kx, vx, move, work)
    probs, fades = work[4:6], work[6:8]

    @pl.when(count > 0)
    def _():
        probs[1][...] = jnp.zeros((KEYS, BLK), BF16)
        fades[1][...] = jnp.ones((8, BLK), F32)
        score(0, 0)
        last = count * tiles - 1

        def two_tiles(j, carry):
            t = 2 * j
            add(jnp.maximum(t - 1, 0), 1)
            weigh(t, 0)
            score(t + 1, 1)
            add(t, 0)
            weigh(t + 1, 1)
            score(jnp.minimum(t + 2, last), 0)
            return carry

        lax.fori_loop(0, count * (tiles // 2), two_tiles, 0)
        add(last, 1)


def first_body(idx, q, pay, acc, m, sums, kx, vx, move, *bufs):
    acc[...] = jnp.zeros_like(acc)
    m[...] = jnp.full(m.shape, LOW, F32)
    move[...] = jnp.zeros_like(move)
    place_chunk(pay, 0, kx, vx)
    score, weigh, add = stages(q, acc, m, kx, vx, move, bufs)
    key = lax.broadcasted_iota(jnp.int32, (BLK, BLK), 0)
    query = lax.broadcasted_iota(jnp.int32, (BLK, BLK), 1)
    tiles = QS // BLK
    meets = [(b // 2 + 1) * BLK for b in range(tiles)]
    masks = [key + (idx[2] - odd) * BLK <= query for odd in range(2)]
    for b in range(tiles + 2):
        if b < tiles:
            score(b, b % 2, meets[b], masks[b % 2])
        if 0 <= b - 1 < tiles:
            weigh(b - 1, (b - 1) % 2, meets[b - 1])
        if 0 <= b - 2:
            add(b - 2, (b - 2) % 2, meets[b - 2])
    sums[...] = jnp.broadcast_to(chunk_total(pay), sums.shape)


def step_body(k, idx, q, *refs):
    z = idx[0]
    n_pay = 2 if k < 4 else 1
    pays, refs = refs[:n_pay], refs[n_pay:]
    acc0, m0, sums0, refs = refs[0], refs[1], refs[2], refs[3:]
    if k < 4:
        acc, m, sums, kx, vx, move, *bufs = refs
    else:
        out_own, out_sib, kx, vx, move, *bufs, sums = refs
        acc, m = acc0, m0
    sums[...] = sums0[...]
    count = (z >= k).astype(jnp.int32)

    @pl.when(z >= k)
    def _():
        place_chunk(pays[0], 0, kx, vx)
        move[0] = sums0[...]
        sums[...] = sums0[...] + jnp.broadcast_to(chunk_total(pays[0]), sums.shape)

    if k < 4:
        count = count + (z + k >= 8).astype(jnp.int32)

        @pl.when(z + k >= 8)
        def _():
            place_chunk(pays[1], 1, kx, vx)
            move[1] = jnp.zeros(sums.shape, F32)
            m[1] = m[1] + chunk_total(pays[1])[:, 0:1]

    absorb(count, q, acc, m, kx, vx, move, bufs)
    if k == 4:
        c = idx[2]
        row = lax.broadcasted_iota(jnp.int32, (8, BLK), 0)
        for b in range(4):
            for other in range(2):
                at = 2 * b + (c if other == 0 else 1 - c)
                lanes = pl.ds(pl.multiple_of(at * BLK, BLK), BLK)
                m_a = m[0, 0:1, lanes]
                m_b = m[1, 0:1, lanes] + sums[0:1]
                top = jnp.maximum(m_a, m_b)
                both = acc[0, :, lanes] * jnp.exp(m_a - top) + acc[1, :, lanes] * jnp.exp(m_b - top)
                to = slice(b * BLK, (b + 1) * BLK)
                out = out_own if other == 0 else out_sib
                out[0:64, to] = both[0:64]
                out[64:72, to] = jnp.where(row < 4, both[64:65], top)


def merge_body(own, sib, out):
    a, b = own[...], sib[...]
    m_a, m_b = a[68:69], b[68:69]
    top = jnp.maximum(m_a, m_b)
    f_a, f_b = jnp.exp(m_a - top), jnp.exp(m_b - top)
    total = a[64:65] * f_a + b[64:65] * f_b
    att = (a[0:64] * f_a + b[0:64] * f_b) / total
    att = jnp.concatenate([att, jnp.zeros_like(att)], axis=0)
    for r in range(8):
        out[r * 128 : (r + 1) * 128, :] = att[:, r * 128 : (r + 1) * 128].T[:, 0:64].astype(BF16)


def assemble_body(idx, w0, w1, w2, w3, w):
    x, c, y = idx[1], idx[2], idx[3]
    for ky, ref in enumerate((w0, w1, w2, w3)):
        cols = pl.ds(pl.multiple_of(lax.rem(y - ky + NY, NY) * 256, 256), 256)
        for kx in range(NX):
            xx = lax.rem(x - kx + NX, NX)
            for other in range(2):
                cc = c if other == 0 else 1 - c
                for z in range(NZ):
                    at = pl.multiple_of(z * 128 + xx * 32 + cc * 16, 16)
                    w[pl.ds(at, 16), cols] = ref[other, z, kx * 16 : kx * 16 + 16, :]


def final_body(att, gain, w, out):
    pieces = [att[xs * NY + ys] for ys in range(NY) for xs in range(NX)]
    joined = jnp.concatenate(pieces, axis=1)
    proj = lax.dot_general(joined, w[...], (((1,), (1,)), ((), ())), preferred_element_type=F32)
    scale = lax.rsqrt(jnp.mean(proj * proj, axis=-1, keepdims=True) + EPS)
    out[...] = (proj * scale * gain[...]).astype(BF16)


def shards(tokens, norm_gain, w_query, w_key, w_value, w_forget, forget_offset, w_out_t, out_gain):
    sds = jax.ShapeDtypeStruct
    idx = jnp.stack([lax.axis_index(a) for a in AXES]).astype(jnp.int32)

    half, piece, send = sds((32, D), BF16), sds((16, 256), BF16), sds((48, D), BF16)
    rows = jnp.pad(tokens, ((0, 32), (0, 0)))
    for i, w in enumerate((w_query, w_key, w_value, w_out_t)):
        rows = rows + jnp.pad(w, ((64, 16), (256 * i, 768 - 256 * i)))
    rows = rows + jnp.pad(w_forget.T, ((80, 16 - NX), (0, D - 16)))
    lo, hi, p0, o0, *sends = call(
        pack_body,
        (half, half, piece, piece, send, send, send),
        [SMEM, VMEM],
        [pltpu.VMEM((NX, 16, 256), BF16)],
    )(idx, rows)

    got = [shift(sends[k - 1], "x", k) for k in range(1, NX)]
    tok_a = direct(lo, "y")
    chunk, tok_b = call(
        spread_body, (sds((NZ, 128, 256), BF16), sds((128, D), BF16)), [VMEM] * 6
    )(hi, p0, o0, *got)
    w_own = lax.all_to_all(chunk, "z", 0, 0, tiled=True)
    toks = direct(jnp.concatenate(tok_a, axis=0), "x") + direct(tok_b, "y")
    w_sib = shift(w_own, "c", 1)

    q_own, kv, cum_own = call(
        project_body,
        (sds((80, KEYS), BF16), sds((128, KEYS), BF16), sds((8, KEYS), F32)),
        [SMEM, SMEM] + [VMEM] * 11,
        [pltpu.VMEM((D, 256), BF16), pltpu.VMEM((KEYS, 256), F32)],
        2e9,
    )(idx, forget_offset, *toks, norm_gain[None], w_own, w_sib)

    q_sib = shift(q_own, "c", 1)
    q, pay = call(
        prepare_body, (sds((128, QS), BF16), sds((PAY, KEYS), BF16)), [SMEM] + [VMEM] * 4
    )(idx, q_own, q_sib, kv, cum_own)

    acc_t, m_t, sums_t = sds((2, 80, QS), F32), sds((2, 8, QS), F32), sds((8, BLK), F32)
    work = [
        pltpu.VMEM((2, KEYS, 128), BF16),
        pltpu.VMEM((2, 80, KEYS), BF16),
        pltpu.VMEM((2, 8, BLK), F32),
        pltpu.VMEM((KEYS, BLK), F32),
        pltpu.VMEM((KEYS, BLK), F32),
        pltpu.VMEM((8, BLK), F32),
        pltpu.VMEM((8, BLK), F32),
        pltpu.VMEM((KEYS, BLK), BF16),
        pltpu.VMEM((KEYS, BLK), BF16),
        pltpu.VMEM((8, BLK), F32),
        pltpu.VMEM((8, BLK), F32),
    ]
    right = step_right(pay, 1)
    left = step_left(pay, 1)
    acc, m, sums = call(
        first_body, (acc_t, m_t, sums_t), [SMEM, VMEM, VMEM], work, 3e9
    )(idx, q, pay)

    w_o = jnp.stack([w_own[:, 64:], w_sib[:, 64:]])
    w_o, _ = lax.optimization_barrier((w_o, sums))
    w_o = direct(w_o, "y")

    for k in range(1, 5):
        pays = (right, left) if k < 4 else (right,)
        if k < 4:
            right = step_right(pays[0], k + 1)
        if k < 3:
            left = step_left(pays[1], k + 1)
        ins = (idx, q) + pays + (acc, m, sums)
        if k < 4:
            outs, scratch, aliases = (acc_t, m_t, sums_t), work, {4: 0, 5: 1}
        else:
            outs, aliases = (sds((72, KEYS), F32), sds((72, KEYS), F32)), None
            scratch = work + [pltpu.VMEM(sums_t.shape, F32)]
        res = call(
            functools.partial(step_body, k),
            outs,
            [SMEM] + [VMEM] * (len(ins) - 1),
            scratch,
            6e9,
            aliases,
        )(*ins)
        if k < 4:
            acc, m, sums = res
    sib = shift(res[1], "c", 1)
    w_full = call(assemble_body, sds((D, D), BF16), [SMEM] + [VMEM] * 4)(idx, *w_o)
    att = call(merge_body, sds((KEYS, HD), BF16), [VMEM, VMEM])(res[0], sib)
    att = lax.all_to_all(att.reshape(16, 64, HD), ("x", "y"), 0, 0, tiled=True)
    return call(final_body, sds((OWN, D), BF16), [VMEM] * 3)(att, out_gain[None], w_full)


def solution(mesh):
    finer = Mesh(mesh.devices.reshape(NZ, NX, NC, NY), AXES)
    sp = ("z", "x", "c")

    return jax.shard_map(
        shards,
        mesh=finer,
        in_specs=(
            P(AXES, None),
            P(),
            P(sp, "y"),
            P(sp, "y"),
            P(sp, "y"),
            P(sp, "y"),
            P("y"),
            P(sp, "y"),
            P(),
        ),
        out_specs=P(AXES, None),
        check_vma=False,
    )
```

```python
import functools
import math

import jax
import jax.numpy as jnp
from jax import lax
from jax.experimental import pallas as pl
from jax.experimental.pallas import tpu as pltpu
from jax.sharding import Mesh
from jax.sharding import PartitionSpec as P


AXES = ("z", "x", "c", "y")
NZ, NX, NC, NY = 8, 4, 2, 4
SIZES = {"z": NZ, "x": NX, "c": NC, "y": NY}
D = 1024
HD = 64
TOTAL = 16384
OWN = 64
BLK = 256
KEYS = 1024
QS = 2048
PAY = 144
EPS = 1e-06
LOW = -1e30
F32 = jnp.float32
BF16 = jnp.bfloat16


VMEM = pl.BlockSpec(memory_space=pltpu.VMEM)
SMEM = pl.BlockSpec(memory_space=pltpu.SMEM)


def call(body, outs, ins, scratch=(), flops=1e8, aliases=None):
    return pl.pallas_call(
        body,
        out_shape=outs,
        in_specs=ins,
        out_specs=jax.tree.map(lambda _: VMEM, outs),
        scratch_shapes=list(scratch),
        input_output_aliases=aliases or {},
        cost_estimate=pl.CostEstimate(
            flops=int(flops), bytes_accessed=1 << 20, transcendentals=0
        ),
        compiler_params=pltpu.CompilerParams(vmem_limit_bytes=24 << 20),
    )


def shift(x, axis, k):
    n = SIZES[axis]
    return lax.ppermute(x, axis, [(i, (i + k) % n) for i in range(n)])


def gather(x, axis):
    one, three = shift(x, axis, 1), shift(x, axis, -1)
    two = shift(one, axis, 1)
    return [x, one, two, three]


def step_right(x, k):
    return lax.ppermute(x, "z", [(i, i + 1) for i in range(k - 1, NZ - 1)])


def step_left(x, k):
    return lax.ppermute(x, "z", [((i - k + 1) % NZ, (i - k) % NZ) for i in range(3)])


def three_parts(x):
    hi = x.astype(BF16)
    rest = x - hi.astype(F32)
    mid = rest.astype(BF16)
    low = (rest - mid.astype(F32)).astype(BF16)
    return hi, mid, low


def pack_body(idx, rows, lo, hi, p0, o0, s1, s3, heads):
    x = idx[1]
    lo[...] = rows[0:32, :]
    hi[...] = rows[32:64, :]
    o0[...] = rows[64:80, 768:1024]
    head = lax.broadcasted_iota(jnp.int32, (16, HD), 0)
    gates = rows[80:96, 0:128].astype(F32)
    for h in range(NX):
        pick = jnp.where(head == h, 1.0, 0.0)
        gate = lax.dot_general(
            gates, pick, (((0,), (0,)), ((), ())), precision=lax.Precision.HIGHEST,
            preferred_element_type=F32,
        )[0:16]
        mine = [rows[64:80, i * 256 + h * HD : i * 256 + h * HD + HD] for i in range(3)]
        heads[h] = jnp.concatenate(mine + [gate.astype(BF16)], axis=1)
    p0[...] = heads[x]
    for k, s in ((1, s1), (3, s3)):
        s[0:32, :] = rows[32:64, :]
        s[32:48, 0:256] = heads[lax.rem(x + k, NX)]
        s[32:48, 256:512] = rows[64:80, 768:1024]
        s[32:48, 512:768] = heads[lax.rem(x + 2, NX)]
        s[32:48, 768:1024] = jnp.zeros((16, 256), BF16)


def spread_body(hi, p0, o0, r1, r2, r3, out, toks):
    toks[0:32, :] = hi[...]
    for k, r in enumerate((r1, r2, r3)):
        toks[32 * k + 32 : 32 * k + 64, :] = r[0:32, :]
    for z in range(NZ):
        out[z, 0:16, :] = p0[...]
        out[z, 64:80, :] = o0[...]
        for k, r in enumerate((r1, r2, r3)):
            piece = 512 if k == 1 else 0
            out[z, 16 * k + 16 : 16 * k + 32, :] = r[32:48, piece : piece + 256]
            out[z, 16 * k + 80 : 16 * k + 96, :] = r[32:48, 256:512]


def project_body(idx, offs, *refs):
    toks = refs[:8]
    gain, w_own, w_sib = refs[8:11]
    qc_out, kv_out, cum_out = refs[11:14]
    w, rows = refs[14:]
    x, c, y = idx[1], idx[2], idx[3]
    for z in range(NZ):
        for xx in range(NX):
            base = z * 128 + lax.rem(x - xx + NX, NX) * 32
            own_at = pl.multiple_of(base + c * 16, 16)
            sib_at = pl.multiple_of(base + (1 - c) * 16, 16)
            w[pl.ds(own_at, 16), :] = w_own[z, xx * 16 : xx * 16 + 16, :]
            w[pl.ds(sib_at, 16), :] = w_sib[z, xx * 16 : xx * 16 + 16, :]
    for half in range(2):
        for outer in range(4):
            tok = toks[half * 4 + outer][...].astype(F32)
            scale = lax.rsqrt(jnp.mean(tok * tok, axis=-1, keepdims=True) + EPS)
            normed = (tok * scale * gain[...]).astype(BF16)
            out = jnp.dot(normed, w[...], preferred_element_type=F32)
            for inner in range(4):
                kx, ky = (outer, inner) if half == 0 else (inner, outer)
                xx = lax.rem(x - kx + NX, NX)
                yy = lax.rem(y - ky + NY, NY)
                at = pl.multiple_of(xx * BLK + yy * OWN + half * 32, 32)
                rows[pl.ds(at, 32), :] = out[inner * 32 : inner * 32 + 32, :]
    before = lax.broadcasted_iota(jnp.int32, (BLK, BLK), 0)
    after = lax.broadcasted_iota(jnp.int32, (BLK, BLK), 1)
    ones = jnp.where(before <= after, 1.0, 0.0).astype(BF16)
    for b in range(4):
        t = rows[b * BLK : (b + 1) * BLK, :].T
        lanes = slice(b * BLK, (b + 1) * BLK)
        qc_out[0:64, lanes] = t[:64].astype(BF16)
        kv_out[:, lanes] = t[64:192].astype(BF16)
        logit = t[192:200] + offs[x] + math.log(TOTAL)
        gate = jnp.minimum(logit, 0.0) - jnp.log1p(jnp.exp(-jnp.abs(logit)))
        hi, mid, low = three_parts(gate)
        cum = jnp.dot(hi, ones, preferred_element_type=F32)
        cum = cum + jnp.dot(mid, ones, preferred_element_type=F32)
        cum = cum + jnp.dot(low, ones, preferred_element_type=F32)
        cum_out[:, lanes] = cum
        row = lax.broadcasted_iota(jnp.int32, (16, BLK), 0)
        block = jnp.zeros((16, BLK), F32)
        for i, part in enumerate(three_parts(cum[0:1])):
            block = jnp.where(row == i, part.astype(F32), block)
        qc_out[64:80, lanes] = block.astype(BF16)


def prepare_body(idx, q_own, q_sib, kv, cum_own, q_out, pay_out):
    c = idx[2]
    q_out[80:128, :] = jnp.zeros((48, QS), BF16)
    row = lax.broadcasted_iota(jnp.int32, (16, QS), 0)
    q_out[64:80, :] = jnp.where(row < 3, 1.0, 0.0).astype(BF16)
    for b in range(4):
        lanes = slice(b * BLK, (b + 1) * BLK)
        own_at = pl.multiple_of((2 * b + c) * BLK, BLK)
        sib_at = pl.multiple_of((2 * b + 1 - c) * BLK, BLK)
        q_out[0:64, pl.ds(own_at, BLK)] = q_own[0:64, lanes] * jnp.asarray(0.125, BF16)
        q_out[0:64, pl.ds(sib_at, BLK)] = q_sib[0:64, lanes] * jnp.asarray(0.125, BF16)
    own, sib = [], []
    for b in range(4):
        end = slice(b * BLK + BLK - 1, b * BLK + BLK)
        own.append(cum_own[:, end])
        parts = q_sib[64:80, b * BLK + 128 : b * BLK + BLK].astype(F32)[:, 127:128]
        sib.append(jnp.broadcast_to(parts[0:1] + parts[1:2] + parts[2:3], (8, 1)))
    ahead = jnp.zeros_like(own[0])
    bases = []
    for b in range(4):
        bases.append(ahead + jnp.where(c == 1, sib[b], 0.0))
        ahead = ahead + (own[b] + sib[b])
    total = ahead
    pay_out[0:64, :] = kv[0:64, :]
    pay_out[80:144, :] = kv[64:128, :]
    row = lax.broadcasted_iota(jnp.int32, (16, BLK), 0)
    for b in range(4):
        lanes = slice(b * BLK, (b + 1) * BLK)
        bias = (total - bases[b]) - cum_own[:, lanes]
        parts = [p[0:1].astype(F32) for p in three_parts(bias)]
        totals = [p[0:1].astype(F32) for p in three_parts(jnp.broadcast_to(total, bias.shape))]
        block = jnp.zeros((16, BLK), F32)
        for i, part in enumerate(parts + totals):
            block = jnp.where(row == i, part, block)
        pay_out[64:80, lanes] = block.astype(BF16)


def chunk_total(pay):
    rows = pay[64:80, 0:BLK].astype(F32)
    return rows[3:4] + rows[4:5] + rows[5:6]


def place_chunk(pay, i, kx, vx):
    fill = jnp.zeros((48, 128), F32)
    for r in range(8):
        lanes = slice(r * 128, (r + 1) * 128)
        tile = jnp.concatenate([pay[0:80, lanes].astype(F32), fill], axis=0)
        kx[i, lanes, :] = tile.T.astype(BF16)
    vx[i, 0:64, :] = pay[80:144, :]
    vx[i, 64:80, :] = jnp.ones((16, KEYS), BF16)


def stages(q, acc, m, kx, vx, move, work):
    tiles = QS // BLK
    bufs, tops, probs, fades = work[0:2], work[2:4], work[4:6], work[6:8]

    def lanes_of(t):
        if isinstance(t, int):
            return slice((t % tiles) * BLK, (t % tiles + 1) * BLK)
        return pl.ds(pl.multiple_of((t % tiles) * BLK, BLK), BLK)

    def score(t, slot, n=KEYS, allowed=None):
        s = jnp.dot(kx[t // tiles, 0:n], q[:, lanes_of(t)], preferred_element_type=F32)
        if allowed is not None:
            last = jnp.where(allowed, s[n - BLK : n], LOW)
            s = last if n == BLK else jnp.concatenate([s[0 : n - BLK], last], axis=0)
        bufs[slot][0:n] = s
        tops[slot][...] = jnp.broadcast_to(jnp.max(s, axis=0, keepdims=True), (8, BLK))

    def weigh(t, slot, n=KEYS):
        i, lanes = t // tiles, lanes_of(t)
        by = move[i, 0:1]
        old = m[i, 0:1, lanes]
        new = jnp.maximum(old, tops[slot][0:1] + by)
        probs[slot][0:n] = jnp.exp(bufs[slot][0:n] - (new - by)).astype(BF16)
        fades[slot][...] = jnp.broadcast_to(jnp.exp(old - new), (8, BLK))
        m[i, :, lanes] = jnp.broadcast_to(new, (8, BLK))

    def add(t, slot, n=KEYS):
        i, lanes = t // tiles, lanes_of(t)
        part = jnp.dot(vx[i, :, 0:n], probs[slot][0:n], preferred_element_type=F32)
        acc[i, :, lanes] = acc[i, :, lanes] * fades[slot][0:1] + part

    return score, weigh, add


def absorb(count, q, acc, m, kx, vx, move, work):
    tiles = QS // BLK
    score, weigh, add = stages(q, acc, m, kx, vx, move, work)
    probs, fades = work[4:6], work[6:8]

    @pl.when(count > 0)
    def _():
        probs[1][...] = jnp.zeros((KEYS, BLK), BF16)
        fades[1][...] = jnp.ones((8, BLK), F32)
        score(0, 0)
        last = count * tiles - 1

        def two_tiles(j, carry):
            t = 2 * j
            add(jnp.maximum(t - 1, 0), 1)
            weigh(t, 0)
            score(t + 1, 1)
            add(t, 0)
            weigh(t + 1, 1)
            score(jnp.minimum(t + 2, last), 0)
            return carry

        lax.fori_loop(0, count * (tiles // 2), two_tiles, 0)
        add(last, 1)


def first_body(idx, q, pay, acc, m, sums, kx, vx, move, *bufs):
    acc[...] = jnp.zeros_like(acc)
    m[...] = jnp.full(m.shape, LOW, F32)
    move[...] = jnp.zeros_like(move)
    place_chunk(pay, 0, kx, vx)
    score, weigh, add = stages(q, acc, m, kx, vx, move, bufs)
    key = lax.broadcasted_iota(jnp.int32, (BLK, BLK), 0)
    query = lax.broadcasted_iota(jnp.int32, (BLK, BLK), 1)
    tiles = QS // BLK
    meets = [(b // 2 + 1) * BLK for b in range(tiles)]
    masks = [key + (idx[2] - odd) * BLK <= query for odd in range(2)]
    for b in range(tiles + 2):
        if b < tiles:
            score(b, b % 2, meets[b], masks[b % 2])
        if 0 <= b - 1 < tiles:
            weigh(b - 1, (b - 1) % 2, meets[b - 1])
        if 0 <= b - 2:
            add(b - 2, (b - 2) % 2, meets[b - 2])
    sums[...] = jnp.broadcast_to(chunk_total(pay), sums.shape)


def step_body(k, idx, q, *refs):
    z = idx[0]
    n_pay = 2 if k < 4 else 1
    pays, refs = refs[:n_pay], refs[n_pay:]
    acc0, m0, sums0, refs = refs[0], refs[1], refs[2], refs[3:]
    if k < 4:
        acc, m, sums, kx, vx, move, *bufs = refs
    else:
        out_own, out_sib, kx, vx, move, *bufs, sums = refs
        acc, m = acc0, m0
    sums[...] = sums0[...]
    count = (z >= k).astype(jnp.int32)

    @pl.when(z >= k)
    def _():
        place_chunk(pays[0], 0, kx, vx)
        move[0] = sums0[...]
        sums[...] = sums0[...] + jnp.broadcast_to(chunk_total(pays[0]), sums.shape)

    if k < 4:
        count = count + (z + k >= 8).astype(jnp.int32)

        @pl.when(z + k >= 8)
        def _():
            place_chunk(pays[1], 1, kx, vx)
            move[1] = jnp.zeros(sums.shape, F32)
            m[1] = m[1] + chunk_total(pays[1])[:, 0:1]

    absorb(count, q, acc, m, kx, vx, move, bufs)
    if k == 4:
        c = idx[2]
        row = lax.broadcasted_iota(jnp.int32, (8, BLK), 0)
        for b in range(4):
            for other in range(2):
                at = 2 * b + (c if other == 0 else 1 - c)
                lanes = pl.ds(pl.multiple_of(at * BLK, BLK), BLK)
                m_a = m[0, 0:1, lanes]
                m_b = m[1, 0:1, lanes] + sums[0:1]
                top = jnp.maximum(m_a, m_b)
                both = acc[0, :, lanes] * jnp.exp(m_a - top) + acc[1, :, lanes] * jnp.exp(m_b - top)
                to = slice(b * BLK, (b + 1) * BLK)
                out = out_own if other == 0 else out_sib
                out[0:64, to] = both[0:64]
                out[64:72, to] = jnp.where(row < 4, both[64:65], top)


def merge_body(own, sib, out):
    a, b = own[...], sib[...]
    m_a, m_b = a[68:69], b[68:69]
    top = jnp.maximum(m_a, m_b)
    f_a, f_b = jnp.exp(m_a - top), jnp.exp(m_b - top)
    total = a[64:65] * f_a + b[64:65] * f_b
    att = (a[0:64] * f_a + b[0:64] * f_b) / total
    att = jnp.concatenate([att, jnp.zeros_like(att)], axis=0)
    for r in range(8):
        out[r * 128 : (r + 1) * 128, :] = att[:, r * 128 : (r + 1) * 128].T[:, 0:64].astype(BF16)


def assemble_body(idx, w0, w1, w2, w3, w):
    x, c, y = idx[1], idx[2], idx[3]
    for ky, ref in enumerate((w0, w1, w2, w3)):
        cols = pl.ds(pl.multiple_of(lax.rem(y - ky + NY, NY) * 256, 256), 256)
        for kx in range(NX):
            xx = lax.rem(x - kx + NX, NX)
            for other in range(2):
                cc = c if other == 0 else 1 - c
                for z in range(NZ):
                    at = pl.multiple_of(z * 128 + xx * 32 + cc * 16, 16)
                    w[pl.ds(at, 16), cols] = ref[other, z, kx * 16 : kx * 16 + 16, :]


def final_body(att, gain, w, out):
    pieces = [att[xs * NY + ys] for ys in range(NY) for xs in range(NX)]
    joined = jnp.concatenate(pieces, axis=1)
    proj = lax.dot_general(joined, w[...], (((1,), (1,)), ((), ())), preferred_element_type=F32)
    scale = lax.rsqrt(jnp.mean(proj * proj, axis=-1, keepdims=True) + EPS)
    out[...] = (proj * scale * gain[...]).astype(BF16)


def shards(tokens, norm_gain, w_query, w_key, w_value, w_forget, forget_offset, w_out_t, out_gain):
    sds = jax.ShapeDtypeStruct
    idx = jnp.stack([lax.axis_index(a) for a in AXES]).astype(jnp.int32)

    half, piece, send = sds((32, D), BF16), sds((16, 256), BF16), sds((48, D), BF16)
    rows = jnp.pad(tokens, ((0, 32), (0, 0)))
    for i, w in enumerate((w_query, w_key, w_value, w_out_t)):
        rows = rows + jnp.pad(w, ((64, 16), (256 * i, 768 - 256 * i)))
    rows = rows + jnp.pad(w_forget.T, ((80, 16 - NX), (0, D - 16)))
    lo, hi, p0, o0, ahead, behind = call(
        pack_body,
        (half, half, piece, piece, send, send),
        [SMEM, VMEM],
        [pltpu.VMEM((NX, 16, 256), BF16)],
    )(idx, rows)

    got_1, got_3 = shift(ahead, "x", 1), shift(behind, "x", -1)
    got = (got_1, shift(got_1, "x", 1), got_3)
    tok_a = gather(lo, "y")
    chunk, tok_b = call(
        spread_body, (sds((NZ, 128, 256), BF16), sds((128, D), BF16)), [VMEM] * 6
    )(hi, p0, o0, *got)
    w_own = lax.all_to_all(chunk, "z", 0, 0, tiled=True)
    toks_b = gather(tok_b, "y")
    toks = gather(jnp.concatenate(tok_a, axis=0), "x") + toks_b
    w_sib = shift(w_own, "c", 1)

    q_own, kv, cum_own = call(
        project_body,
        (sds((80, KEYS), BF16), sds((128, KEYS), BF16), sds((8, KEYS), F32)),
        [SMEM, SMEM] + [VMEM] * 11,
        [pltpu.VMEM((D, 256), BF16), pltpu.VMEM((KEYS, 256), F32)],
        2e9,
    )(idx, forget_offset, *toks, norm_gain[None], w_own, w_sib)

    q_sib = shift(q_own, "c", 1)
    q, pay = call(
        prepare_body, (sds((128, QS), BF16), sds((PAY, KEYS), BF16)), [SMEM] + [VMEM] * 4
    )(idx, q_own, q_sib, kv, cum_own)

    acc_t, m_t, sums_t = sds((2, 80, QS), F32), sds((2, 8, QS), F32), sds((8, BLK), F32)
    work = [
        pltpu.VMEM((2, KEYS, 128), BF16),
        pltpu.VMEM((2, 80, KEYS), BF16),
        pltpu.VMEM((2, 8, BLK), F32),
        pltpu.VMEM((KEYS, BLK), F32),
        pltpu.VMEM((KEYS, BLK), F32),
        pltpu.VMEM((8, BLK), F32),
        pltpu.VMEM((8, BLK), F32),
        pltpu.VMEM((KEYS, BLK), BF16),
        pltpu.VMEM((KEYS, BLK), BF16),
        pltpu.VMEM((8, BLK), F32),
        pltpu.VMEM((8, BLK), F32),
    ]
    right = step_right(pay, 1)
    left = step_left(pay, 1)
    acc, m, sums = call(
        first_body, (acc_t, m_t, sums_t), [SMEM, VMEM, VMEM], work, 3e9
    )(idx, q, pay)

    w_o = jnp.stack([w_own[:, 64:], w_sib[:, 64:]])
    w_o, _ = lax.optimization_barrier((w_o, sums))
    w_o = gather(w_o, "y")

    for k in range(1, 5):
        pays = (right, left) if k < 4 else (right,)
        if k < 4:
            right = step_right(pays[0], k + 1)
        if k < 3:
            left = step_left(pays[1], k + 1)
        ins = (idx, q) + pays + (acc, m, sums)
        if k < 4:
            outs, scratch, aliases = (acc_t, m_t, sums_t), work, {4: 0, 5: 1}
        else:
            outs, aliases = (sds((72, KEYS), F32), sds((72, KEYS), F32)), None
            scratch = work + [pltpu.VMEM(sums_t.shape, F32)]
        res = call(
            functools.partial(step_body, k),
            outs,
            [SMEM] + [VMEM] * (len(ins) - 1),
            scratch,
            6e9,
            aliases,
        )(*ins)
        if k < 4:
            acc, m, sums = res
    sib = shift(res[1], "c", 1)
    w_full = call(assemble_body, sds((D, D), BF16), [SMEM] + [VMEM] * 4)(idx, *w_o)
    att = call(merge_body, sds((KEYS, HD), BF16), [VMEM, VMEM])(res[0], sib)
    att = lax.all_to_all(att.reshape(16, 64, HD), ("x", "y"), 0, 0, tiled=True)
    return call(final_body, sds((OWN, D), BF16), [VMEM] * 3)(att, out_gain[None], w_full)


def solution(mesh):
    finer = Mesh(mesh.devices.reshape(NZ, NX, NC, NY), AXES)
    sp = ("z", "x", "c")

    return jax.shard_map(
        shards,
        mesh=finer,
        in_specs=(
            P(AXES, None),
            P(),
            P(sp, "y"),
            P(sp, "y"),
            P(sp, "y"),
            P(sp, "y"),
            P("y"),
            P(sp, "y"),
            P(),
        ),
        out_specs=P(AXES, None),
        check_vma=False,
    )
```

```python
import functools
import math

import jax
import jax.numpy as jnp
from jax import lax
from jax.experimental import pallas as pl
from jax.experimental.pallas import tpu as pltpu
from jax.sharding import Mesh
from jax.sharding import PartitionSpec as P


AXES = ("z", "x", "c", "y")
NZ, NX, NC, NY = 8, 4, 2, 4
SIZES = {"z": NZ, "x": NX, "c": NC, "y": NY}
D = 1024
HD = 64
TOTAL = 16384
OWN = 64
BLK = 256
KEYS = 1024
QS = 2048
PAY = 136
EPS = 1e-06
LOW = -1e30
F32 = jnp.float32
BF16 = jnp.bfloat16


VMEM = pl.BlockSpec(memory_space=pltpu.VMEM)
SMEM = pl.BlockSpec(memory_space=pltpu.SMEM)


def call(body, outs, ins, scratch=(), flops=1e8, aliases=None):
    return pl.pallas_call(
        body,
        out_shape=outs,
        in_specs=ins,
        out_specs=jax.tree.map(lambda _: VMEM, outs),
        scratch_shapes=list(scratch),
        input_output_aliases=aliases or {},
        cost_estimate=pl.CostEstimate(
            flops=int(flops), bytes_accessed=1 << 20, transcendentals=0
        ),
        compiler_params=pltpu.CompilerParams(vmem_limit_bytes=24 << 20),
    )


def shift(x, axis, k):
    n = SIZES[axis]
    return lax.ppermute(x, axis, [(i, (i + k) % n) for i in range(n)])


def direct(x, axis):
    return [x] + [shift(x, axis, k) for k in range(1, SIZES[axis])]


def gather(x, axis):
    one, three = shift(x, axis, 1), shift(x, axis, -1)
    two = shift(one, axis, 1)
    return [x, one, two, three]


def step_right(x, k):
    return lax.ppermute(x, "z", [(i, i + 1) for i in range(k - 1, NZ - 1)])


def step_left(x, k):
    return lax.ppermute(x, "z", [((i - k + 1) % NZ, (i - k) % NZ) for i in range(3)])


def three_parts(x):
    hi = x.astype(BF16)
    rest = x - hi.astype(F32)
    mid = rest.astype(BF16)
    low = (rest - mid.astype(F32)).astype(BF16)
    return hi, mid, low


def pack_body(idx, rows, lo, hi, p0, o0, s1, s2, s3, heads):
    x = idx[1]
    lo[...] = rows[0:32, :]
    hi[...] = rows[32:64, :]
    o0[...] = rows[64:80, 768:1024]
    head = lax.broadcasted_iota(jnp.int32, (16, HD), 0)
    gates = rows[80:96, 0:128].astype(F32)
    for h in range(NX):
        pick = jnp.where(head == h, 1.0, 0.0)
        gate = lax.dot_general(
            gates, pick, (((0,), (0,)), ((), ())), precision=lax.Precision.HIGHEST,
            preferred_element_type=F32,
        )[0:16]
        mine = [rows[64:80, i * 256 + h * HD : i * 256 + h * HD + HD] for i in range(3)]
        heads[h] = jnp.concatenate(mine + [gate.astype(BF16)], axis=1)
    p0[...] = heads[x]
    for k, s in enumerate((s1, s2, s3)):
        s[0:32, :] = rows[32:64, :]
        s[32:48, 0:256] = heads[lax.rem(x + k + 1, NX)]
        s[32:48, 256:512] = rows[64:80, 768:1024]
        s[32:48, 512:1024] = jnp.zeros((16, 512), BF16)


def spread_body(hi, p0, o0, r1, r2, r3, out, toks):
    toks[0:32, :] = hi[...]
    for k, r in enumerate((r1, r2, r3)):
        toks[32 * k + 32 : 32 * k + 64, :] = r[0:32, :]
    for z in range(NZ):
        out[z, 0:16, :] = p0[...]
        out[z, 64:80, :] = o0[...]
        for k, r in enumerate((r1, r2, r3)):
            out[z, 16 * k + 16 : 16 * k + 32, :] = r[32:48, 0:256]
            out[z, 16 * k + 80 : 16 * k + 96, :] = r[32:48, 256:512]


def project_body(idx, offs, *refs):
    toks = refs[:8]
    gain, w_own, w_sib = refs[8:11]
    qc_out, kv_out, cum_out = refs[11:14]
    w, rows = refs[14:]
    x, c, y = idx[1], idx[2], idx[3]
    for z in range(NZ):
        for xx in range(NX):
            base = z * 128 + lax.rem(x - xx + NX, NX) * 32
            own_at = pl.multiple_of(base + c * 16, 16)
            sib_at = pl.multiple_of(base + (1 - c) * 16, 16)
            w[pl.ds(own_at, 16), :] = w_own[z, xx * 16 : xx * 16 + 16, :]
            w[pl.ds(sib_at, 16), :] = w_sib[z, xx * 16 : xx * 16 + 16, :]
    for half in range(2):
        for outer in range(4):
            tok = toks[half * 4 + outer][...].astype(F32)
            scale = lax.rsqrt(jnp.mean(tok * tok, axis=-1, keepdims=True) + EPS)
            normed = (tok * scale * gain[...]).astype(BF16)
            out = jnp.dot(normed, w[...], preferred_element_type=F32)
            for inner in range(4):
                kx, ky = (outer, inner) if half == 0 else (inner, outer)
                xx = lax.rem(x - kx + NX, NX)
                yy = lax.rem(y - ky + NY, NY)
                at = pl.multiple_of(xx * BLK + yy * OWN + half * 32, 32)
                rows[pl.ds(at, 32), :] = out[inner * 32 : inner * 32 + 32, :]
    before = lax.broadcasted_iota(jnp.int32, (BLK, BLK), 0)
    after = lax.broadcasted_iota(jnp.int32, (BLK, BLK), 1)
    ones = jnp.where(before <= after, 1.0, 0.0).astype(BF16)
    for b in range(4):
        t = rows[b * BLK : (b + 1) * BLK, :].T
        lanes = slice(b * BLK, (b + 1) * BLK)
        qc_out[0:64, lanes] = t[:64].astype(BF16)
        kv_out[:, lanes] = t[64:192].astype(BF16)
        logit = t[192:200] + offs[x] + math.log(TOTAL)
        gate = jnp.minimum(logit, 0.0) - jnp.log1p(jnp.exp(-jnp.abs(logit)))
        hi, mid, low = three_parts(gate)
        cum = jnp.dot(hi, ones, preferred_element_type=F32)
        cum = cum + jnp.dot(mid, ones, preferred_element_type=F32)
        cum = cum + jnp.dot(low, ones, preferred_element_type=F32)
        cum_out[:, lanes] = cum
        row = lax.broadcasted_iota(jnp.int32, (16, BLK), 0)
        block = jnp.zeros((16, BLK), F32)
        for i, part in enumerate(three_parts(cum[0:1])):
            block = jnp.where(row == i, part.astype(F32), block)
        qc_out[64:80, lanes] = block.astype(BF16)


def prepare_body(idx, q_own, q_sib, kv, cum_own, q_out, pay_out):
    c = idx[2]
    q_out[80:128, :] = jnp.zeros((48, QS), BF16)
    row = lax.broadcasted_iota(jnp.int32, (16, QS), 0)
    q_out[64:80, :] = jnp.where(row < 3, 1.0, 0.0).astype(BF16)
    for b in range(4):
        lanes = slice(b * BLK, (b + 1) * BLK)
        own_at = pl.multiple_of((2 * b + c) * BLK, BLK)
        sib_at = pl.multiple_of((2 * b + 1 - c) * BLK, BLK)
        q_out[0:64, pl.ds(own_at, BLK)] = q_own[0:64, lanes] * jnp.asarray(0.125, BF16)
        q_out[0:64, pl.ds(sib_at, BLK)] = q_sib[0:64, lanes] * jnp.asarray(0.125, BF16)
    own, sib = [], []
    for b in range(4):
        end = slice(b * BLK + BLK - 1, b * BLK + BLK)
        own.append(cum_own[:, end])
        parts = q_sib[64:80, b * BLK + 128 : b * BLK + BLK].astype(F32)[:, 127:128]
        sib.append(jnp.broadcast_to(parts[0:1] + parts[1:2] + parts[2:3], (8, 1)))
    ahead = jnp.zeros_like(own[0])
    bases = []
    for b in range(4):
        bases.append(ahead + jnp.where(c == 1, sib[b], 0.0))
        ahead = ahead + (own[b] + sib[b])
    total = ahead
    pay_out[0:64, :] = kv[64:128, :]
    pay_out[64:128, :] = kv[0:64, :]
    row = lax.broadcasted_iota(jnp.int32, (8, BLK), 0)
    for b in range(4):
        lanes = slice(b * BLK, (b + 1) * BLK)
        bias = (total - bases[b]) - cum_own[:, lanes]
        parts = [p[0:1].astype(F32) for p in three_parts(bias)]
        totals = [p[0:1].astype(F32) for p in three_parts(jnp.broadcast_to(total, bias.shape))]
        block = jnp.zeros((8, BLK), F32)
        for i, part in enumerate(parts + totals):
            block = jnp.where(row == i, part, block)
        pay_out[128:136, lanes] = block.astype(BF16)


def chunk_total(pay):
    rows = pay[128:136, 0:BLK].astype(F32)
    return rows[3:4] + rows[4:5] + rows[5:6]


def place_chunk(pay, i, kx, vx):
    fill = jnp.zeros((56, 128), F32)
    for r in range(8):
        lanes = slice(r * 128, (r + 1) * 128)
        tile = jnp.concatenate([pay[64:136, lanes].astype(F32), fill], axis=0)
        kx[i, lanes, :] = tile.T.astype(BF16)
    vx[i, 0:64, :] = pay[0:64, :]
    vx[i, 64:80, :] = jnp.ones((16, KEYS), BF16)


def stages(q, acc, m, kx, vx, move, work):
    tiles = QS // BLK
    bufs, tops, probs, fades = work[0:2], work[2:4], work[4:6], work[6:8]

    def lanes_of(t):
        if isinstance(t, int):
            return slice((t % tiles) * BLK, (t % tiles + 1) * BLK)
        return pl.ds(pl.multiple_of((t % tiles) * BLK, BLK), BLK)

    def score(t, slot, n=KEYS, allowed=None):
        s = jnp.dot(kx[t // tiles, 0:n], q[:, lanes_of(t)], preferred_element_type=F32)
        if allowed is not None:
            last = jnp.where(allowed, s[n - BLK : n], LOW)
            s = last if n == BLK else jnp.concatenate([s[0 : n - BLK], last], axis=0)
        bufs[slot][0:n] = s
        tops[slot][...] = jnp.broadcast_to(jnp.max(s, axis=0, keepdims=True), (8, BLK))

    def weigh(t, slot, n=KEYS):
        i, lanes = t // tiles, lanes_of(t)
        by = move[i, 0:1]
        old = m[i, 0:1, lanes]
        new = jnp.maximum(old, tops[slot][0:1] + by)
        probs[slot][0:n] = jnp.exp(bufs[slot][0:n] - (new - by)).astype(BF16)
        fades[slot][...] = jnp.broadcast_to(jnp.exp(old - new), (8, BLK))
        m[i, :, lanes] = jnp.broadcast_to(new, (8, BLK))

    def add(t, slot, n=KEYS):
        i, lanes = t // tiles, lanes_of(t)
        part = jnp.dot(vx[i, :, 0:n], probs[slot][0:n], preferred_element_type=F32)
        acc[i, :, lanes] = acc[i, :, lanes] * fades[slot][0:1] + part

    return score, weigh, add


def absorb(count, q, acc, m, kx, vx, move, work):
    tiles = QS // BLK
    score, weigh, add = stages(q, acc, m, kx, vx, move, work)
    probs, fades = work[4:6], work[6:8]

    @pl.when(count > 0)
    def _():
        probs[1][...] = jnp.zeros((KEYS, BLK), BF16)
        fades[1][...] = jnp.ones((8, BLK), F32)
        score(0, 0)
        last = count * tiles - 1

        def two_tiles(j, carry):
            t = 2 * j
            add(jnp.maximum(t - 1, 0), 1)
            weigh(t, 0)
            score(t + 1, 1)
            add(t, 0)
            weigh(t + 1, 1)
            score(jnp.minimum(t + 2, last), 0)
            return carry

        lax.fori_loop(0, count * (tiles // 2), two_tiles, 0)
        add(last, 1)


def first_body(idx, q, pay, acc, m, sums, kx, vx, move, *bufs):
    acc[...] = jnp.zeros_like(acc)
    m[...] = jnp.full(m.shape, LOW, F32)
    move[...] = jnp.zeros_like(move)
    place_chunk(pay, 0, kx, vx)
    score, weigh, add = stages(q, acc, m, kx, vx, move, bufs)
    key = lax.broadcasted_iota(jnp.int32, (BLK, BLK), 0)
    query = lax.broadcasted_iota(jnp.int32, (BLK, BLK), 1)
    tiles = QS // BLK
    meets = [(b // 2 + 1) * BLK for b in range(tiles)]
    masks = [key + (idx[2] - odd) * BLK <= query for odd in range(2)]
    for b in range(tiles + 2):
        if b < tiles:
            score(b, b % 2, meets[b], masks[b % 2])
        if 0 <= b - 1 < tiles:
            weigh(b - 1, (b - 1) % 2, meets[b - 1])
        if 0 <= b - 2:
            add(b - 2, (b - 2) % 2, meets[b - 2])
    sums[...] = jnp.broadcast_to(chunk_total(pay), sums.shape)


def step_body(k, idx, q, *refs):
    z = idx[0]
    n_pay = 2 if k < 4 else 1
    pays, refs = refs[:n_pay], refs[n_pay:]
    acc0, m0, sums0, refs = refs[0], refs[1], refs[2], refs[3:]
    if k < 4:
        acc, m, sums, kx, vx, move, *bufs = refs
    else:
        out_own, out_sib, kx, vx, move, *bufs, sums = refs
        acc, m = acc0, m0
    sums[...] = sums0[...]
    count = (z >= k).astype(jnp.int32)

    @pl.when(z >= k)
    def _():
        place_chunk(pays[0], 0, kx, vx)
        move[0] = sums0[...]
        sums[...] = sums0[...] + jnp.broadcast_to(chunk_total(pays[0]), sums.shape)

    if k < 4:
        count = count + (z + k >= 8).astype(jnp.int32)

        @pl.when(z + k >= 8)
        def _():
            place_chunk(pays[1], 1, kx, vx)
            move[1] = jnp.zeros(sums.shape, F32)
            m[1] = m[1] + chunk_total(pays[1])[:, 0:1]

    absorb(count, q, acc, m, kx, vx, move, bufs)
    if k == 4:
        c = idx[2]
        row = lax.broadcasted_iota(jnp.int32, (8, BLK), 0)
        for b in range(4):
            for other in range(2):
                at = 2 * b + (c if other == 0 else 1 - c)
                lanes = pl.ds(pl.multiple_of(at * BLK, BLK), BLK)
                m_a = m[0, 0:1, lanes]
                m_b = m[1, 0:1, lanes] + sums[0:1]
                top = jnp.maximum(m_a, m_b)
                both = acc[0, :, lanes] * jnp.exp(m_a - top) + acc[1, :, lanes] * jnp.exp(m_b - top)
                to = slice(b * BLK, (b + 1) * BLK)
                out = out_own if other == 0 else out_sib
                out[0:64, to] = both[0:64]
                out[64:72, to] = jnp.where(row < 4, both[64:65], top)


def merge_body(own, sib, out):
    a, b = own[...], sib[...]
    m_a, m_b = a[68:69], b[68:69]
    top = jnp.maximum(m_a, m_b)
    f_a, f_b = jnp.exp(m_a - top), jnp.exp(m_b - top)
    total = a[64:65] * f_a + b[64:65] * f_b
    att = (a[0:64] * f_a + b[0:64] * f_b) / total
    att = jnp.concatenate([att, jnp.zeros_like(att)], axis=0)
    for r in range(8):
        out[r * 128 : (r + 1) * 128, :] = att[:, r * 128 : (r + 1) * 128].T[:, 0:64].astype(BF16)


def assemble_body(idx, w0, w1, w2, w3, w):
    x, c, y = idx[1], idx[2], idx[3]
    for ky, ref in enumerate((w0, w1, w2, w3)):
        cols = pl.ds(pl.multiple_of(lax.rem(y - ky + NY, NY) * 256, 256), 256)
        for kx in range(NX):
            xx = lax.rem(x - kx + NX, NX)
            for other in range(2):
                cc = c if other == 0 else 1 - c
                for z in range(NZ):
                    at = pl.multiple_of(z * 128 + xx * 32 + cc * 16, 16)
                    w[pl.ds(at, 16), cols] = ref[other, z, kx * 16 : kx * 16 + 16, :]


def final_body(att, gain, w, out):
    pieces = [att[xs * NY + ys] for ys in range(NY) for xs in range(NX)]
    joined = jnp.concatenate(pieces, axis=1)
    proj = lax.dot_general(joined, w[...], (((1,), (1,)), ((), ())), preferred_element_type=F32)
    scale = lax.rsqrt(jnp.mean(proj * proj, axis=-1, keepdims=True) + EPS)
    out[...] = (proj * scale * gain[...]).astype(BF16)


def shards(tokens, norm_gain, w_query, w_key, w_value, w_forget, forget_offset, w_out_t, out_gain):
    sds = jax.ShapeDtypeStruct
    idx = jnp.stack([lax.axis_index(a) for a in AXES]).astype(jnp.int32)

    half, piece, send = sds((32, D), BF16), sds((16, 256), BF16), sds((48, D), BF16)
    rows = jnp.pad(tokens, ((0, 32), (0, 0)))
    for i, w in enumerate((w_query, w_key, w_value, w_out_t)):
        rows = rows + jnp.pad(w, ((64, 16), (256 * i, 768 - 256 * i)))
    rows = rows + jnp.pad(w_forget.T, ((80, 16 - NX), (0, D - 16)))
    lo, hi, p0, o0, *sends = call(
        pack_body,
        (half, half, piece, piece, send, send, send),
        [SMEM, VMEM],
        [pltpu.VMEM((NX, 16, 256), BF16)],
    )(idx, rows)

    got = [shift(sends[k - 1], "x", k) for k in range(1, NX)]
    tok_a = direct(lo, "y")
    chunk, tok_b = call(
        spread_body, (sds((NZ, 128, 256), BF16), sds((128, D), BF16)), [VMEM] * 6
    )(hi, p0, o0, *got)
    w_own = lax.all_to_all(chunk, "z", 0, 0, tiled=True)
    toks_b = gather(tok_b, "y")
    toks = gather(jnp.concatenate(tok_a, axis=0), "x") + toks_b
    w_sib = shift(w_own, "c", 1)

    q_own, kv, cum_own = call(
        project_body,
        (sds((80, KEYS), BF16), sds((128, KEYS), BF16), sds((8, KEYS), F32)),
        [SMEM, SMEM] + [VMEM] * 11,
        [pltpu.VMEM((D, 256), BF16), pltpu.VMEM((KEYS, 256), F32)],
        2e9,
    )(idx, forget_offset, *toks, norm_gain[None], w_own, w_sib)

    q_sib = shift(q_own, "c", 1)
    q, pay = call(
        prepare_body, (sds((128, QS), BF16), sds((PAY, KEYS), BF16)), [SMEM] + [VMEM] * 4
    )(idx, q_own, q_sib, kv, cum_own)

    acc_t, m_t, sums_t = sds((2, 80, QS), F32), sds((2, 8, QS), F32), sds((8, BLK), F32)
    work = [
        pltpu.VMEM((2, KEYS, 128), BF16),
        pltpu.VMEM((2, 80, KEYS), BF16),
        pltpu.VMEM((2, 8, BLK), F32),
        pltpu.VMEM((KEYS, BLK), F32),
        pltpu.VMEM((KEYS, BLK), F32),
        pltpu.VMEM((8, BLK), F32),
        pltpu.VMEM((8, BLK), F32),
        pltpu.VMEM((KEYS, BLK), BF16),
        pltpu.VMEM((KEYS, BLK), BF16),
        pltpu.VMEM((8, BLK), F32),
        pltpu.VMEM((8, BLK), F32),
    ]
    right = step_right(pay, 1)
    left = step_left(pay, 1)
    acc, m, sums = call(
        first_body, (acc_t, m_t, sums_t), [SMEM, VMEM, VMEM], work, 3e9
    )(idx, q, pay)

    w_o = jnp.stack([w_own[:, 64:], w_sib[:, 64:]])
    w_o, _ = lax.optimization_barrier((w_o, sums))
    w_o = direct(w_o, "y")

    for k in range(1, 5):
        pays = (right, left) if k < 4 else (right,)
        if k < 4:
            right = step_right(pays[0], k + 1)
        if k < 3:
            left = step_left(pays[1], k + 1)
        ins = (idx, q) + pays + (acc, m, sums)
        if k < 4:
            outs, scratch, aliases = (acc_t, m_t, sums_t), work, {4: 0, 5: 1}
        else:
            outs, aliases = (sds((72, KEYS), F32), sds((72, KEYS), F32)), None
            scratch = work + [pltpu.VMEM(sums_t.shape, F32)]
        res = call(
            functools.partial(step_body, k),
            outs,
            [SMEM] + [VMEM] * (len(ins) - 1),
            scratch,
            6e9,
            aliases,
        )(*ins)
        if k < 4:
            acc, m, sums = res
    sib = shift(res[1], "c", 1)
    w_full = call(assemble_body, sds((D, D), BF16), [SMEM] + [VMEM] * 4)(idx, *w_o)
    att = call(merge_body, sds((KEYS, HD), BF16), [VMEM, VMEM])(res[0], sib)
    att = lax.all_to_all(att.reshape(16, 64, HD), ("x", "y"), 0, 0, tiled=True)
    return call(final_body, sds((OWN, D), BF16), [VMEM] * 3)(att, out_gain[None], w_full)


def solution(mesh):
    finer = Mesh(mesh.devices.reshape(NZ, NX, NC, NY), AXES)
    sp = ("z", "x", "c")

    return jax.shard_map(
        shards,
        mesh=finer,
        in_specs=(
            P(AXES, None),
            P(),
            P(sp, "y"),
            P(sp, "y"),
            P(sp, "y"),
            P(sp, "y"),
            P("y"),
            P(sp, "y"),
            P(),
        ),
        out_specs=P(AXES, None),
        check_vma=False,
    )
```

```python
import functools
import math

import jax
import jax.numpy as jnp
from jax import lax
from jax.experimental import pallas as pl
from jax.experimental.pallas import tpu as pltpu
from jax.sharding import Mesh
from jax.sharding import PartitionSpec as P


AXES = ("z", "x", "c", "y")
NZ, NX, NC, NY = 8, 4, 2, 4
SIZES = {"z": NZ, "x": NX, "c": NC, "y": NY}
D = 1024
HD = 64
TOTAL = 16384
OWN = 64
BLK = 256
KEYS = 1024
QS = 2048
PAY = 136
EPS = 1e-06
LOW = -1e30
F32 = jnp.float32
BF16 = jnp.bfloat16


VMEM = pl.BlockSpec(memory_space=pltpu.VMEM)
SMEM = pl.BlockSpec(memory_space=pltpu.SMEM)


def call(body, outs, ins, scratch=(), flops=1e8, aliases=None):
    return pl.pallas_call(
        body,
        out_shape=outs,
        in_specs=ins,
        out_specs=jax.tree.map(lambda _: VMEM, outs),
        scratch_shapes=list(scratch),
        input_output_aliases=aliases or {},
        cost_estimate=pl.CostEstimate(
            flops=int(flops), bytes_accessed=1 << 20, transcendentals=0
        ),
        compiler_params=pltpu.CompilerParams(vmem_limit_bytes=24 << 20),
    )


def shift(x, axis, k):
    n = SIZES[axis]
    return lax.ppermute(x, axis, [(i, (i + k) % n) for i in range(n)])


def direct(x, axis):
    return [x] + [shift(x, axis, k) for k in range(1, SIZES[axis])]


def gather(x, axis):
    one, three = shift(x, axis, 1), shift(x, axis, -1)
    two = shift(one, axis, 1)
    return [x, one, two, three]


def step_right(x, k):
    return lax.ppermute(x, "z", [(i, i + 1) for i in range(k - 1, NZ - 1)])


def step_left(x, k):
    return lax.ppermute(x, "z", [((i - k + 1) % NZ, (i - k) % NZ) for i in range(4)])


def three_parts(x):
    hi = x.astype(BF16)
    rest = x - hi.astype(F32)
    mid = rest.astype(BF16)
    low = (rest - mid.astype(F32)).astype(BF16)
    return hi, mid, low


def pack_body(idx, rows, lo, hi, p0, o0, s1, s2, s3, heads):
    x = idx[1]
    lo[...] = rows[0:32, :]
    hi[...] = rows[32:64, :]
    o0[...] = rows[64:80, 768:1024]
    head = lax.broadcasted_iota(jnp.int32, (16, HD), 0)
    gates = rows[80:96, 0:128].astype(F32)
    for h in range(NX):
        pick = jnp.where(head == h, 1.0, 0.0)
        gate = lax.dot_general(
            gates, pick, (((0,), (0,)), ((), ())), precision=lax.Precision.HIGHEST,
            preferred_element_type=F32,
        )[0:16]
        mine = [rows[64:80, i * 256 + h * HD : i * 256 + h * HD + HD] for i in range(3)]
        heads[h] = jnp.concatenate(mine + [gate.astype(BF16)], axis=1)
    p0[...] = heads[x]
    for k, s in enumerate((s1, s2, s3)):
        s[0:32, :] = rows[32:64, :]
        s[32:48, 0:256] = heads[lax.rem(x + k + 1, NX)]
        s[32:48, 256:512] = rows[64:80, 768:1024]
        s[32:48, 512:1024] = jnp.zeros((16, 512), BF16)


def spread_body(hi, p0, o0, r1, r2, r3, out, toks):
    toks[0:32, :] = hi[...]
    for k, r in enumerate((r1, r2, r3)):
        toks[32 * k + 32 : 32 * k + 64, :] = r[0:32, :]
    for z in range(NZ):
        out[z, 0:16, :] = p0[...]
        out[z, 64:80, :] = o0[...]
        for k, r in enumerate((r1, r2, r3)):
            out[z, 16 * k + 16 : 16 * k + 32, :] = r[32:48, 0:256]
            out[z, 16 * k + 80 : 16 * k + 96, :] = r[32:48, 256:512]


def project_body(idx, offs, *refs):
    toks = refs[:8]
    gain, w_own, w_sib = refs[8:11]
    qc_out, kv_out, cum_out = refs[11:14]
    w, rows = refs[14:]
    x, c, y = idx[1], idx[2], idx[3]
    for z in range(NZ):
        for xx in range(NX):
            base = z * 128 + lax.rem(x - xx + NX, NX) * 32
            own_at = pl.multiple_of(base + c * 16, 16)
            sib_at = pl.multiple_of(base + (1 - c) * 16, 16)
            w[pl.ds(own_at, 16), :] = w_own[z, xx * 16 : xx * 16 + 16, :]
            w[pl.ds(sib_at, 16), :] = w_sib[z, xx * 16 : xx * 16 + 16, :]
    for half in range(2):
        for outer in range(4):
            tok = toks[half * 4 + outer][...].astype(F32)
            scale = lax.rsqrt(jnp.mean(tok * tok, axis=-1, keepdims=True) + EPS)
            normed = (tok * scale * gain[...]).astype(BF16)
            out = jnp.dot(normed, w[...], preferred_element_type=F32)
            for inner in range(4):
                kx, ky = (outer, inner) if half == 0 else (inner, outer)
                xx = lax.rem(x - kx + NX, NX)
                yy = lax.rem(y - ky + NY, NY)
                at = pl.multiple_of(xx * BLK + yy * OWN + half * 32, 32)
                rows[pl.ds(at, 32), :] = out[inner * 32 : inner * 32 + 32, :]
    before = lax.broadcasted_iota(jnp.int32, (BLK, BLK), 0)
    after = lax.broadcasted_iota(jnp.int32, (BLK, BLK), 1)
    ones = jnp.where(before <= after, 1.0, 0.0).astype(BF16)
    for b in range(4):
        t = rows[b * BLK : (b + 1) * BLK, :].T
        lanes = slice(b * BLK, (b + 1) * BLK)
        qc_out[0:64, lanes] = t[:64].astype(BF16)
        kv_out[:, lanes] = t[64:192].astype(BF16)
        logit = t[192:200] + offs[x] + math.log(TOTAL)
        gate = jnp.minimum(logit, 0.0) - jnp.log1p(jnp.exp(-jnp.abs(logit)))
        hi, mid, low = three_parts(gate)
        cum = jnp.dot(hi, ones, preferred_element_type=F32)
        cum = cum + jnp.dot(mid, ones, preferred_element_type=F32)
        cum = cum + jnp.dot(low, ones, preferred_element_type=F32)
        cum_out[:, lanes] = cum
        row = lax.broadcasted_iota(jnp.int32, (16, BLK), 0)
        block = jnp.zeros((16, BLK), F32)
        for i, part in enumerate(three_parts(cum[0:1])):
            block = jnp.where(row == i, part.astype(F32), block)
        qc_out[64:80, lanes] = block.astype(BF16)


def prepare_body(idx, q_own, q_sib, kv, cum_own, q_out, pay_out):
    c = idx[2]
    q_out[80:128, :] = jnp.zeros((48, QS), BF16)
    row = lax.broadcasted_iota(jnp.int32, (16, QS), 0)
    q_out[64:80, :] = jnp.where(row < 3, 1.0, 0.0).astype(BF16)
    for b in range(4):
        lanes = slice(b * BLK, (b + 1) * BLK)
        own_at = pl.multiple_of((2 * b + c) * BLK, BLK)
        sib_at = pl.multiple_of((2 * b + 1 - c) * BLK, BLK)
        q_out[0:64, pl.ds(own_at, BLK)] = q_own[0:64, lanes] * jnp.asarray(0.125, BF16)
        q_out[0:64, pl.ds(sib_at, BLK)] = q_sib[0:64, lanes] * jnp.asarray(0.125, BF16)
    own, sib = [], []
    for b in range(4):
        end = slice(b * BLK + BLK - 1, b * BLK + BLK)
        own.append(cum_own[:, end])
        parts = q_sib[64:80, b * BLK + 128 : b * BLK + BLK].astype(F32)[:, 127:128]
        sib.append(jnp.broadcast_to(parts[0:1] + parts[1:2] + parts[2:3], (8, 1)))
    ahead = jnp.zeros_like(own[0])
    bases = []
    for b in range(4):
        bases.append(ahead + jnp.where(c == 1, sib[b], 0.0))
        ahead = ahead + (own[b] + sib[b])
    total = ahead
    pay_out[0:64, :] = kv[64:128, :]
    pay_out[64:128, :] = kv[0:64, :]
    row = lax.broadcasted_iota(jnp.int32, (8, BLK), 0)
    for b in range(4):
        lanes = slice(b * BLK, (b + 1) * BLK)
        bias = (total - bases[b]) - cum_own[:, lanes]
        parts = [p[0:1].astype(F32) for p in three_parts(bias)]
        totals = [p[0:1].astype(F32) for p in three_parts(jnp.broadcast_to(total, bias.shape))]
        block = jnp.zeros((8, BLK), F32)
        for i, part in enumerate(parts + totals):
            block = jnp.where(row == i, part, block)
        pay_out[128:136, lanes] = block.astype(BF16)


def chunk_total(pay):
    rows = pay[128:136, 0:BLK].astype(F32)
    return rows[3:4] + rows[4:5] + rows[5:6]


def place_chunk(pays, i, kx, vx):
    fill = jnp.zeros((56, 128), F32)
    tiles = 8 // len(pays)
    for r in range(8):
        pay, at = pays[r // tiles], r % tiles
        lanes = slice(at * 128, (at + 1) * 128)
        tile = jnp.concatenate([pay[64:136, lanes].astype(F32), fill], axis=0)
        kx[i, r * 128 : (r + 1) * 128, :] = tile.T.astype(BF16)
        vx[i, 0:64, r * 128 : (r + 1) * 128] = pay[0:64, lanes]
    vx[i, 64:80, :] = jnp.ones((16, KEYS), BF16)


def stages(q, acc, m, kx, vx, move, work):
    tiles = QS // BLK
    bufs, tops, probs, fades = work[0:2], work[2:4], work[4:6], work[6:8]

    def lanes_of(t):
        if isinstance(t, int):
            return slice((t % tiles) * BLK, (t % tiles + 1) * BLK)
        return pl.ds(pl.multiple_of((t % tiles) * BLK, BLK), BLK)

    def score(t, slot, n=KEYS, allowed=None):
        s = jnp.dot(kx[t // tiles, 0:n], q[:, lanes_of(t)], preferred_element_type=F32)
        if allowed is not None:
            last = jnp.where(allowed, s[n - BLK : n], LOW)
            s = last if n == BLK else jnp.concatenate([s[0 : n - BLK], last], axis=0)
        bufs[slot][0:n] = s
        tops[slot][...] = jnp.broadcast_to(jnp.max(s, axis=0, keepdims=True), (8, BLK))

    def weigh(t, slot, n=KEYS):
        i, lanes = t // tiles, lanes_of(t)
        by = move[i, 0:1]
        old = m[i, 0:1, lanes]
        new = jnp.maximum(old, tops[slot][0:1] + by)
        probs[slot][0:n] = jnp.exp(bufs[slot][0:n] - (new - by)).astype(BF16)
        fades[slot][...] = jnp.broadcast_to(jnp.exp(old - new), (8, BLK))
        m[i, :, lanes] = jnp.broadcast_to(new, (8, BLK))

    def add(t, slot, n=KEYS):
        i, lanes = t // tiles, lanes_of(t)
        part = jnp.dot(vx[i, :, 0:n], probs[slot][0:n], preferred_element_type=F32)
        acc[i, :, lanes] = acc[i, :, lanes] * fades[slot][0:1] + part

    return score, weigh, add


def absorb(count, q, acc, m, kx, vx, move, work):
    tiles = QS // BLK
    score, weigh, add = stages(q, acc, m, kx, vx, move, work)
    probs, fades = work[4:6], work[6:8]

    @pl.when(count > 0)
    def _():
        probs[1][...] = jnp.zeros((KEYS, BLK), BF16)
        fades[1][...] = jnp.ones((8, BLK), F32)
        score(0, 0)
        last = count * tiles - 1

        def two_tiles(j, carry):
            t = 2 * j
            add(jnp.maximum(t - 1, 0), 1)
            weigh(t, 0)
            score(t + 1, 1)
            add(t, 0)
            weigh(t + 1, 1)
            score(jnp.minimum(t + 2, last), 0)
            return carry

        lax.fori_loop(0, count * (tiles // 2), two_tiles, 0)
        add(last, 1)


def first_body(idx, q, pay, acc, m, sums, kx, vx, move, *bufs):
    acc[...] = jnp.zeros_like(acc)
    m[...] = jnp.full(m.shape, LOW, F32)
    move[...] = jnp.zeros_like(move)
    place_chunk((pay,), 0, kx, vx)
    score, weigh, add = stages(q, acc, m, kx, vx, move, bufs)
    key = lax.broadcasted_iota(jnp.int32, (BLK, BLK), 0)
    query = lax.broadcasted_iota(jnp.int32, (BLK, BLK), 1)
    tiles = QS // BLK
    meets = [(b // 2 + 1) * BLK for b in range(tiles)]
    masks = [key + (idx[2] - odd) * BLK <= query for odd in range(2)]
    for b in range(tiles + 2):
        if b < tiles:
            score(b, b % 2, meets[b], masks[b % 2])
        if 0 <= b - 1 < tiles:
            weigh(b - 1, (b - 1) % 2, meets[b - 1])
        if 0 <= b - 2:
            add(b - 2, (b - 2) % 2, meets[b - 2])
    sums[...] = jnp.broadcast_to(chunk_total(pay), sums.shape)


def step_body(k, idx, q, *refs):
    z = idx[0]
    pays, refs = refs[:2], refs[2:]
    acc0, m0, sums0, refs = refs[0], refs[1], refs[2], refs[3:]
    if k < 4:
        acc, m, sums, kx, vx, move, *bufs = refs
    else:
        out_own, out_sib, kx, vx, move, *bufs, sums = refs
        acc, m = acc0, m0
    sums[...] = sums0[...]
    count = (z >= k).astype(jnp.int32)

    @pl.when(z >= k)
    def _():
        place_chunk(pays[0:1] if k < 4 else pays, 0, kx, vx)
        move[0] = sums0[...]
        sums[...] = sums0[...] + jnp.broadcast_to(chunk_total(pays[0]), sums.shape)

    if k < 4:
        count = count + (z + k >= 8).astype(jnp.int32)

        @pl.when(z + k >= 8)
        def _():
            place_chunk(pays[1:2], 1, kx, vx)
            move[1] = jnp.zeros(sums.shape, F32)
            m[1] = m[1] + chunk_total(pays[1])[:, 0:1]

    absorb(count, q, acc, m, kx, vx, move, bufs)
    if k == 4:
        c = idx[2]
        row = lax.broadcasted_iota(jnp.int32, (8, BLK), 0)
        for b in range(4):
            for other in range(2):
                at = 2 * b + (c if other == 0 else 1 - c)
                lanes = pl.ds(pl.multiple_of(at * BLK, BLK), BLK)
                m_a = m[0, 0:1, lanes]
                m_b = m[1, 0:1, lanes] + sums[0:1]
                top = jnp.maximum(m_a, m_b)
                both = acc[0, :, lanes] * jnp.exp(m_a - top) + acc[1, :, lanes] * jnp.exp(m_b - top)
                to = slice(b * BLK, (b + 1) * BLK)
                out = out_own if other == 0 else out_sib
                out[0:64, to] = both[0:64]
                out[64:72, to] = jnp.where(row < 4, both[64:65], top)


def merge_body(own, sib, out):
    a, b = own[...], sib[...]
    m_a, m_b = a[68:69], b[68:69]
    top = jnp.maximum(m_a, m_b)
    f_a, f_b = jnp.exp(m_a - top), jnp.exp(m_b - top)
    total = a[64:65] * f_a + b[64:65] * f_b
    att = (a[0:64] * f_a + b[0:64] * f_b) / total
    att = jnp.concatenate([att, jnp.zeros_like(att)], axis=0)
    for r in range(8):
        out[r * 128 : (r + 1) * 128, :] = att[:, r * 128 : (r + 1) * 128].T[:, 0:64].astype(BF16)


def assemble_body(idx, w0, w1, w2, w3, w):
    x, c, y = idx[1], idx[2], idx[3]
    for ky, ref in enumerate((w0, w1, w2, w3)):
        cols = pl.ds(pl.multiple_of(lax.rem(y - ky + NY, NY) * 256, 256), 256)
        for kx in range(NX):
            xx = lax.rem(x - kx + NX, NX)
            for other in range(2):
                cc = c if other == 0 else 1 - c
                for z in range(NZ):
                    at = pl.multiple_of(z * 128 + xx * 32 + cc * 16, 16)
                    w[pl.ds(at, 16), cols] = ref[other, z, kx * 16 : kx * 16 + 16, :]


def final_body(att, gain, w, out):
    pieces = [att[xs * NY + ys] for ys in range(NY) for xs in range(NX)]
    joined = jnp.concatenate(pieces, axis=1)
    proj = lax.dot_general(joined, w[...], (((1,), (1,)), ((), ())), preferred_element_type=F32)
    scale = lax.rsqrt(jnp.mean(proj * proj, axis=-1, keepdims=True) + EPS)
    out[...] = (proj * scale * gain[...]).astype(BF16)


def shards(tokens, norm_gain, w_query, w_key, w_value, w_forget, forget_offset, w_out_t, out_gain):
    sds = jax.ShapeDtypeStruct
    idx = jnp.stack([lax.axis_index(a) for a in AXES]).astype(jnp.int32)

    half, piece, send = sds((32, D), BF16), sds((16, 256), BF16), sds((48, D), BF16)
    rows = jnp.pad(tokens, ((0, 32), (0, 0)))
    for i, w in enumerate((w_query, w_key, w_value, w_out_t)):
        rows = rows + jnp.pad(w, ((64, 16), (256 * i, 768 - 256 * i)))
    rows = rows + jnp.pad(w_forget.T, ((80, 16 - NX), (0, D - 16)))
    lo, hi, p0, o0, *sends = call(
        pack_body,
        (half, half, piece, piece, send, send, send),
        [SMEM, VMEM],
        [pltpu.VMEM((NX, 16, 256), BF16)],
    )(idx, rows)

    got = [shift(sends[k - 1], "x", k) for k in range(1, NX)]
    tok_a = direct(lo, "y")
    chunk, tok_b = call(
        spread_body, (sds((NZ, 128, 256), BF16), sds((128, D), BF16)), [VMEM] * 6
    )(hi, p0, o0, *got)
    w_own = lax.all_to_all(chunk, "z", 0, 0, tiled=True)
    toks_b = gather(tok_b, "y")
    toks = gather(jnp.concatenate(tok_a, axis=0), "x") + toks_b
    w_sib = shift(w_own, "c", 1)

    q_own, kv, cum_own = call(
        project_body,
        (sds((80, KEYS), BF16), sds((128, KEYS), BF16), sds((8, KEYS), F32)),
        [SMEM, SMEM] + [VMEM] * 11,
        [pltpu.VMEM((D, 256), BF16), pltpu.VMEM((KEYS, 256), F32)],
        2e9,
    )(idx, forget_offset, *toks, norm_gain[None], w_own, w_sib)

    q_sib = shift(q_own, "c", 1)
    q, pay = call(
        prepare_body, (sds((128, QS), BF16), sds((PAY, KEYS), BF16)), [SMEM] + [VMEM] * 4
    )(idx, q_own, q_sib, kv, cum_own)

    acc_t, m_t, sums_t = sds((2, 80, QS), F32), sds((2, 8, QS), F32), sds((8, BLK), F32)
    work = [
        pltpu.VMEM((2, KEYS, 128), BF16),
        pltpu.VMEM((2, 80, KEYS), BF16),
        pltpu.VMEM((2, 8, BLK), F32),
        pltpu.VMEM((KEYS, BLK), F32),
        pltpu.VMEM((KEYS, BLK), F32),
        pltpu.VMEM((8, BLK), F32),
        pltpu.VMEM((8, BLK), F32),
        pltpu.VMEM((KEYS, BLK), BF16),
        pltpu.VMEM((KEYS, BLK), BF16),
        pltpu.VMEM((8, BLK), F32),
        pltpu.VMEM((8, BLK), F32),
    ]
    right = step_right(pay, 1)
    left = step_left(pay, 1)
    acc, m, sums = call(
        first_body, (acc_t, m_t, sums_t), [SMEM, VMEM, VMEM], work, 3e9
    )(idx, q, pay)

    w_o = jnp.stack([w_own[:, 64:], w_sib[:, 64:]])
    w_o, _ = lax.optimization_barrier((w_o, sums))
    w_o = direct(w_o, "y")

    for k in range(1, 5):
        pays = (right, left)
        if k < 3:
            right, left = step_right(right, k + 1), step_left(left, k + 1)
        elif k == 3:
            right = step_right(right[:, : KEYS // 2], 4)
            left = step_left(left[:, KEYS // 2 :], 4)
        ins = (idx, q) + pays + (acc, m, sums)
        if k < 4:
            outs, scratch, aliases = (acc_t, m_t, sums_t), work, {4: 0, 5: 1}
        else:
            outs, aliases = (sds((72, KEYS), F32), sds((72, KEYS), F32)), None
            scratch = work + [pltpu.VMEM(sums_t.shape, F32)]
        res = call(
            functools.partial(step_body, k),
            outs,
            [SMEM] + [VMEM] * (len(ins) - 1),
            scratch,
            6e9,
            aliases,
        )(*ins)
        if k < 4:
            acc, m, sums = res
    sib = shift(res[1], "c", 1)
    w_full = call(assemble_body, sds((D, D), BF16), [SMEM] + [VMEM] * 4)(idx, *w_o)
    att = call(merge_body, sds((KEYS, HD), BF16), [VMEM, VMEM])(res[0], sib)
    att = lax.all_to_all(att.reshape(16, 64, HD), ("x", "y"), 0, 0, tiled=True)
    return call(final_body, sds((OWN, D), BF16), [VMEM] * 3)(att, out_gain[None], w_full)


def solution(mesh):
    finer = Mesh(mesh.devices.reshape(NZ, NX, NC, NY), AXES)
    sp = ("z", "x", "c")

    return jax.shard_map(
        shards,
        mesh=finer,
        in_specs=(
            P(AXES, None),
            P(),
            P(sp, "y"),
            P(sp, "y"),
            P(sp, "y"),
            P(sp, "y"),
            P("y"),
            P(sp, "y"),
            P(),
        ),
        out_specs=P(AXES, None),
        check_vma=False,
    )
```

```python
import functools
import math

import jax
import jax.numpy as jnp
from jax import lax
from jax.experimental import pallas as pl
from jax.experimental.pallas import tpu as pltpu
from jax.sharding import Mesh
from jax.sharding import PartitionSpec as P


AXES = ("z", "x", "c", "y")
NZ, NX, NC, NY = 8, 4, 2, 4
SIZES = {"z": NZ, "x": NX, "c": NC, "y": NY}
D = 1024
HD = 64
TOTAL = 16384
OWN = 64
BLK = 256
KEYS = 1024
QS = 2048
PAY = 136
EPS = 1e-06
LOW = -1e30
F32 = jnp.float32
BF16 = jnp.bfloat16


VMEM = pl.BlockSpec(memory_space=pltpu.VMEM)
SMEM = pl.BlockSpec(memory_space=pltpu.SMEM)


def call(body, outs, ins, scratch=(), flops=1e8, aliases=None):
    return pl.pallas_call(
        body,
        out_shape=outs,
        in_specs=ins,
        out_specs=jax.tree.map(lambda _: VMEM, outs),
        scratch_shapes=list(scratch),
        input_output_aliases=aliases or {},
        cost_estimate=pl.CostEstimate(
            flops=int(flops), bytes_accessed=1 << 20, transcendentals=0
        ),
        compiler_params=pltpu.CompilerParams(vmem_limit_bytes=24 << 20),
    )


def shift(x, axis, k):
    n = SIZES[axis]
    return lax.ppermute(x, axis, [(i, (i + k) % n) for i in range(n)])


def direct(x, axis):
    return [x] + [shift(x, axis, k) for k in range(1, SIZES[axis])]


def gather(x, axis):
    one, three = shift(x, axis, 1), shift(x, axis, -1)
    two = shift(one, axis, 1)
    return [x, one, two, three]


def step_right(x, k):
    return lax.ppermute(x, "z", [(i, i + 1) for i in range(k - 1, NZ - 1)])


def step_left(x, k):
    return lax.ppermute(x, "z", [((i - k + 1) % NZ, (i - k) % NZ) for i in range(3)])


def three_parts(x):
    hi = x.astype(BF16)
    rest = x - hi.astype(F32)
    mid = rest.astype(BF16)
    low = (rest - mid.astype(F32)).astype(BF16)
    return hi, mid, low


def pack_body(idx, rows, lo, hi, p0, o0, s1, s2, s3, heads):
    x = idx[1]
    lo[...] = rows[0:32, :]
    hi[...] = rows[32:64, :]
    o0[...] = rows[64:80, 768:1024]
    head = lax.broadcasted_iota(jnp.int32, (16, 256), 0)
    lane = lax.broadcasted_iota(jnp.int32, (16, 256), 1)
    pick = jnp.where(lane // HD == head, 1.0, 0.0).astype(BF16)
    gates = lax.dot_general(
        rows[80:96, 0:128], pick, (((0,), (0,)), ((), ())), preferred_element_type=F32
    )[0:16].astype(BF16)
    for h in range(NX):
        at = slice(h * HD, (h + 1) * HD)
        mine = [rows[64:80, i * 256 + h * HD : i * 256 + h * HD + HD] for i in range(3)]
        heads[h] = jnp.concatenate(mine + [gates[:, at]], axis=1)
    p0[...] = heads[x]
    for k, s in enumerate((s1, s2, s3)):
        s[0:32, :] = rows[32:64, :]
        s[32:48, 0:256] = heads[lax.rem(x + k + 1, NX)]
        s[32:48, 256:512] = rows[64:80, 768:1024]
        s[32:48, 512:1024] = jnp.zeros((16, 512), BF16)


def spread_body(hi, p0, o0, r1, r2, r3, out, toks):
    toks[0:32, :] = hi[...]
    for k, r in enumerate((r1, r2, r3)):
        toks[32 * k + 32 : 32 * k + 64, :] = r[0:32, :]
    for z in range(NZ):
        out[z, 0:16, :] = p0[...]
        out[z, 64:80, :] = o0[...]
        for k, r in enumerate((r1, r2, r3)):
            out[z, 16 * k + 16 : 16 * k + 32, :] = r[32:48, 0:256]
            out[z, 16 * k + 80 : 16 * k + 96, :] = r[32:48, 256:512]


def project_body(idx, offs, *refs):
    toks = refs[:8]
    gain, w_own, w_sib = refs[8:11]
    qc_out, kv_out, cum_out = refs[11:14]
    w, rows = refs[14:]
    x, c, y = idx[1], idx[2], idx[3]
    for z in range(NZ):
        for xx in range(NX):
            base = z * 128 + lax.rem(x - xx + NX, NX) * 32
            own_at = pl.multiple_of(base + c * 16, 16)
            sib_at = pl.multiple_of(base + (1 - c) * 16, 16)
            w[pl.ds(own_at, 16), :] = w_own[z, xx * 16 : xx * 16 + 16, :]
            w[pl.ds(sib_at, 16), :] = w_sib[z, xx * 16 : xx * 16 + 16, :]
    for half in range(2):
        for outer in range(4):
            tok = toks[half * 4 + outer][...].astype(F32)
            scale = lax.rsqrt(jnp.mean(tok * tok, axis=-1, keepdims=True) + EPS)
            normed = (tok * scale * gain[...]).astype(BF16)
            out = jnp.dot(normed, w[...], preferred_element_type=F32)
            for inner in range(4):
                kx, ky = (outer, inner) if half == 0 else (inner, outer)
                xx = lax.rem(x - kx + NX, NX)
                yy = lax.rem(y - ky + NY, NY)
                at = pl.multiple_of(xx * BLK + yy * OWN + half * 32, 32)
                rows[pl.ds(at, 32), :] = out[inner * 32 : inner * 32 + 32, :]
    before = lax.broadcasted_iota(jnp.int32, (BLK, BLK), 0)
    after = lax.broadcasted_iota(jnp.int32, (BLK, BLK), 1)
    ones = jnp.where(before <= after, 1.0, 0.0).astype(BF16)
    for b in range(4):
        t = rows[b * BLK : (b + 1) * BLK, :].T
        lanes = slice(b * BLK, (b + 1) * BLK)
        qc_out[0:64, lanes] = t[:64].astype(BF16)
        kv_out[:, lanes] = t[64:192].astype(BF16)
        logit = t[192:200] + offs[x] + math.log(TOTAL)
        gate = jnp.minimum(logit, 0.0) - jnp.log1p(jnp.exp(-jnp.abs(logit)))
        hi, mid, low = three_parts(gate)
        cum = jnp.dot(hi, ones, preferred_element_type=F32)
        cum = cum + jnp.dot(mid, ones, preferred_element_type=F32)
        cum = cum + jnp.dot(low, ones, preferred_element_type=F32)
        cum_out[:, lanes] = cum
        row = lax.broadcasted_iota(jnp.int32, (16, BLK), 0)
        block = jnp.zeros((16, BLK), F32)
        for i, part in enumerate(three_parts(cum[0:1])):
            block = jnp.where(row == i, part.astype(F32), block)
        qc_out[64:80, lanes] = block.astype(BF16)


def prepare_body(idx, q_own, q_sib, kv, cum_own, q_out, pay_out):
    c = idx[2]
    q_out[80:128, :] = jnp.zeros((48, QS), BF16)
    row = lax.broadcasted_iota(jnp.int32, (16, QS), 0)
    q_out[64:80, :] = jnp.where(row < 3, 1.0, 0.0).astype(BF16)
    for b in range(4):
        lanes = slice(b * BLK, (b + 1) * BLK)
        own_at = pl.multiple_of((2 * b + c) * BLK, BLK)
        sib_at = pl.multiple_of((2 * b + 1 - c) * BLK, BLK)
        q_out[0:64, pl.ds(own_at, BLK)] = q_own[0:64, lanes] * jnp.asarray(0.125, BF16)
        q_out[0:64, pl.ds(sib_at, BLK)] = q_sib[0:64, lanes] * jnp.asarray(0.125, BF16)
    own, sib = [], []
    for b in range(4):
        end = slice(b * BLK + BLK - 1, b * BLK + BLK)
        own.append(cum_own[:, end])
        parts = q_sib[64:80, b * BLK + 128 : b * BLK + BLK].astype(F32)[:, 127:128]
        sib.append(jnp.broadcast_to(parts[0:1] + parts[1:2] + parts[2:3], (8, 1)))
    ahead = jnp.zeros_like(own[0])
    bases = []
    for b in range(4):
        bases.append(ahead + jnp.where(c == 1, sib[b], 0.0))
        ahead = ahead + (own[b] + sib[b])
    total = ahead
    pay_out[0:64, :] = kv[64:128, :]
    pay_out[64:128, :] = kv[0:64, :]
    row = lax.broadcasted_iota(jnp.int32, (8, BLK), 0)
    for b in range(4):
        lanes = slice(b * BLK, (b + 1) * BLK)
        bias = (total - bases[b]) - cum_own[:, lanes]
        parts = [p[0:1].astype(F32) for p in three_parts(bias)]
        totals = [p[0:1].astype(F32) for p in three_parts(jnp.broadcast_to(total, bias.shape))]
        block = jnp.zeros((8, BLK), F32)
        for i, part in enumerate(parts + totals):
            block = jnp.where(row == i, part, block)
        pay_out[128:136, lanes] = block.astype(BF16)


def chunk_total(pay):
    rows = pay[128:136, 0:BLK].astype(F32)
    return rows[3:4] + rows[4:5] + rows[5:6]


def place_chunk(pay, i, kx, vx):
    n = pay.shape[1]
    fill = jnp.zeros((56, 128), F32)
    for r in range(n // 128):
        lanes = slice(r * 128, (r + 1) * 128)
        tile = jnp.concatenate([pay[64:136, lanes].astype(F32), fill], axis=0)
        kx[i, lanes, :] = tile.T.astype(BF16)
    vx[i, 0:64, 0:n] = pay[0:64, :]
    vx[i, 64:80, 0:n] = jnp.ones((16, n), BF16)


def stages(q, acc, m, kx, vx, move, work):
    tiles = QS // BLK
    bufs, tops, probs, fades = work[0:2], work[2:4], work[4:6], work[6:8]

    def lanes_of(t):
        if isinstance(t, int):
            return slice((t % tiles) * BLK, (t % tiles + 1) * BLK)
        return pl.ds(pl.multiple_of((t % tiles) * BLK, BLK), BLK)

    def score(t, slot, n=KEYS, allowed=None):
        s = jnp.dot(kx[t // tiles, 0:n], q[:, lanes_of(t)], preferred_element_type=F32)
        if allowed is not None:
            last = jnp.where(allowed, s[n - BLK : n], LOW)
            s = last if n == BLK else jnp.concatenate([s[0 : n - BLK], last], axis=0)
        bufs[slot][0:n] = s
        tops[slot][...] = jnp.broadcast_to(jnp.max(s, axis=0, keepdims=True), (8, BLK))

    def weigh(t, slot, n=KEYS):
        i, lanes = t // tiles, lanes_of(t)
        by = move[i, 0:1]
        old = m[i, 0:1, lanes]
        new = jnp.maximum(old, tops[slot][0:1] + by)
        probs[slot][0:n] = jnp.exp(bufs[slot][0:n] - (new - by)).astype(BF16)
        fades[slot][...] = jnp.broadcast_to(jnp.exp(old - new), (8, BLK))
        m[i, :, lanes] = jnp.broadcast_to(new, (8, BLK))

    def add(t, slot, n=KEYS):
        i, lanes = t // tiles, lanes_of(t)
        part = jnp.dot(vx[i, :, 0:n], probs[slot][0:n], preferred_element_type=F32)
        acc[i, :, lanes] = acc[i, :, lanes] * fades[slot][0:1] + part

    return score, weigh, add


def absorb(count, q, acc, m, kx, vx, move, work, n=KEYS):
    tiles = QS // BLK
    score, weigh, add = stages(q, acc, m, kx, vx, move, work)
    probs, fades = work[4:6], work[6:8]

    @pl.when(count > 0)
    def _():
        probs[1][0:n] = jnp.zeros((n, BLK), BF16)
        fades[1][...] = jnp.ones((8, BLK), F32)
        score(0, 0, n)
        last = count * tiles - 1

        def two_tiles(j, carry):
            t = 2 * j
            add(jnp.maximum(t - 1, 0), 1, n)
            weigh(t, 0, n)
            score(t + 1, 1, n)
            add(t, 0, n)
            weigh(t + 1, 1, n)
            score(jnp.minimum(t + 2, last), 0, n)
            return carry

        lax.fori_loop(0, count * (tiles // 2), two_tiles, 0)
        add(last, 1, n)


def first_body(idx, q, pay, acc, m, sums, kx, vx, move, *bufs):
    acc[...] = jnp.zeros_like(acc)
    m[...] = jnp.full(m.shape, LOW, F32)
    move[...] = jnp.zeros_like(move)
    place_chunk(pay, 0, kx, vx)
    score, weigh, add = stages(q, acc, m, kx, vx, move, bufs)
    key = lax.broadcasted_iota(jnp.int32, (BLK, BLK), 0)
    query = lax.broadcasted_iota(jnp.int32, (BLK, BLK), 1)
    tiles = QS // BLK
    meets = [(b // 2 + 1) * BLK for b in range(tiles)]
    masks = [key + (idx[2] - odd) * BLK <= query for odd in range(2)]
    for b in range(tiles + 2):
        if b < tiles:
            score(b, b % 2, meets[b], masks[b % 2])
        if 0 <= b - 1 < tiles:
            weigh(b - 1, (b - 1) % 2, meets[b - 1])
        if 0 <= b - 2:
            add(b - 2, (b - 2) % 2, meets[b - 2])
    sums[...] = jnp.broadcast_to(chunk_total(pay), sums.shape)


def step_body(k, part, idx, q, *refs):
    z = idx[0]
    n_pay = 2 if k < 4 else 1
    pays, refs = refs[:n_pay], refs[n_pay:]
    acc0, m0, sums0, refs = refs[0], refs[1], refs[2], refs[3:]
    if part < 2:
        acc, m, sums, kx, vx, move, *bufs = refs
    else:
        out_own, out_sib, kx, vx, move, *bufs, sums = refs
        acc, m = acc0, m0
    sums[...] = sums0[...]
    count = (z >= k).astype(jnp.int32)

    @pl.when(z >= k)
    def _():
        place_chunk(pays[0], 0, kx, vx)
        move[0] = sums0[...]
        if part != 1:
            sums[...] = sums0[...] + jnp.broadcast_to(chunk_total(pays[0]), sums.shape)

    if k < 4:
        count = count + (z + k >= 8).astype(jnp.int32)

        @pl.when(z + k >= 8)
        def _():
            place_chunk(pays[1], 1, kx, vx)
            move[1] = jnp.zeros(sums.shape, F32)
            m[1] = m[1] + chunk_total(pays[1])[:, 0:1]

    absorb(count, q, acc, m, kx, vx, move, bufs, pays[0].shape[1])
    if part == 2:
        c = idx[2]
        row = lax.broadcasted_iota(jnp.int32, (8, BLK), 0)
        for b in range(4):
            for other in range(2):
                at = 2 * b + (c if other == 0 else 1 - c)
                lanes = pl.ds(pl.multiple_of(at * BLK, BLK), BLK)
                m_a = m[0, 0:1, lanes]
                m_b = m[1, 0:1, lanes] + sums[0:1]
                top = jnp.maximum(m_a, m_b)
                both = acc[0, :, lanes] * jnp.exp(m_a - top) + acc[1, :, lanes] * jnp.exp(m_b - top)
                to = slice(b * BLK, (b + 1) * BLK)
                out = out_own if other == 0 else out_sib
                out[0:64, to] = both[0:64]
                out[64:72, to] = jnp.where(row < 4, both[64:65], top)


def merge_body(own, sib, out):
    a, b = own[...], sib[...]
    m_a, m_b = a[68:69], b[68:69]
    top = jnp.maximum(m_a, m_b)
    f_a, f_b = jnp.exp(m_a - top), jnp.exp(m_b - top)
    total = a[64:65] * f_a + b[64:65] * f_b
    att = (a[0:64] * f_a + b[0:64] * f_b) / total
    att = jnp.concatenate([att, jnp.zeros_like(att)], axis=0)
    for r in range(8):
        out[r * 128 : (r + 1) * 128, :] = att[:, r * 128 : (r + 1) * 128].T[:, 0:64].astype(BF16)


def assemble_body(idx, w0, w1, w2, w3, w):
    x, c, y = idx[1], idx[2], idx[3]
    for ky, ref in enumerate((w0, w1, w2, w3)):
        cols = pl.ds(pl.multiple_of(lax.rem(y - ky + NY, NY) * 256, 256), 256)
        for kx in range(NX):
            xx = lax.rem(x - kx + NX, NX)
            for other in range(2):
                cc = c if other == 0 else 1 - c
                for z in range(NZ):
                    at = pl.multiple_of(z * 128 + xx * 32 + cc * 16, 16)
                    w[pl.ds(at, 16), cols] = ref[other, z, kx * 16 : kx * 16 + 16, :]


def final_body(att, gain, w, out):
    pieces = [att[xs * NY + ys] for ys in range(NY) for xs in range(NX)]
    joined = jnp.concatenate(pieces, axis=1)
    proj = lax.dot_general(joined, w[...], (((1,), (1,)), ((), ())), preferred_element_type=F32)
    scale = lax.rsqrt(jnp.mean(proj * proj, axis=-1, keepdims=True) + EPS)
    out[...] = (proj * scale * gain[...]).astype(BF16)


def shards(tokens, norm_gain, w_query, w_key, w_value, w_forget, forget_offset, w_out_t, out_gain):
    sds = jax.ShapeDtypeStruct
    idx = jnp.stack([lax.axis_index(a) for a in AXES]).astype(jnp.int32)

    half, piece, send = sds((32, D), BF16), sds((16, 256), BF16), sds((48, D), BF16)
    rows = jnp.pad(tokens, ((0, 32), (0, 0)))
    for i, w in enumerate((w_query, w_key, w_value, w_out_t)):
        rows = rows + jnp.pad(w, ((64, 16), (256 * i, 768 - 256 * i)))
    rows = rows + jnp.pad(w_forget.T, ((80, 16 - NX), (0, D - 16)))
    lo, hi, p0, o0, *sends = call(
        pack_body,
        (half, half, piece, piece, send, send, send),
        [SMEM, VMEM],
        [pltpu.VMEM((NX, 16, 256), BF16)],
    )(idx, rows)

    got = [shift(sends[k - 1], "x", k) for k in range(1, NX)]
    tok_a = direct(lo, "y")
    chunk, tok_b = call(
        spread_body, (sds((NZ, 128, 256), BF16), sds((128, D), BF16)), [VMEM] * 6
    )(hi, p0, o0, *got)
    w_own = lax.all_to_all(chunk, "z", 0, 0, tiled=True)
    toks_b = gather(tok_b, "y")
    toks = gather(jnp.concatenate(tok_a, axis=0), "x") + toks_b
    w_sib = shift(w_own, "c", 1)

    q_own, kv, cum_own = call(
        project_body,
        (sds((80, KEYS), BF16), sds((128, KEYS), BF16), sds((8, KEYS), F32)),
        [SMEM, SMEM] + [VMEM] * 11,
        [pltpu.VMEM((D, 256), BF16), pltpu.VMEM((KEYS, 256), F32)],
        2e9,
    )(idx, forget_offset, *toks, norm_gain[None], w_own, w_sib)

    q_sib = shift(q_own, "c", 1)
    q, pay = call(
        prepare_body, (sds((128, QS), BF16), sds((PAY, KEYS), BF16)), [SMEM] + [VMEM] * 4
    )(idx, q_own, q_sib, kv, cum_own)

    acc_t, m_t, sums_t = sds((2, 80, QS), F32), sds((2, 8, QS), F32), sds((8, BLK), F32)
    work = [
        pltpu.VMEM((2, KEYS, 128), BF16),
        pltpu.VMEM((2, 80, KEYS), BF16),
        pltpu.VMEM((2, 8, BLK), F32),
        pltpu.VMEM((KEYS, BLK), F32),
        pltpu.VMEM((KEYS, BLK), F32),
        pltpu.VMEM((8, BLK), F32),
        pltpu.VMEM((8, BLK), F32),
        pltpu.VMEM((KEYS, BLK), BF16),
        pltpu.VMEM((KEYS, BLK), BF16),
        pltpu.VMEM((8, BLK), F32),
        pltpu.VMEM((8, BLK), F32),
    ]
    right = step_right(pay, 1)
    left = step_left(pay, 1)
    acc, m, sums = call(
        first_body, (acc_t, m_t, sums_t), [SMEM, VMEM, VMEM], work, 3e9
    )(idx, q, pay)

    w_o = jnp.stack([w_own[:, 64:], w_sib[:, 64:]])
    w_o, _ = lax.optimization_barrier((w_o, sums))
    w_o = direct(w_o, "y")

    for k, part in ((1, 0), (2, 0), (3, 0), (4, 1), (4, 2)):
        pays = (right, left) if k < 4 else (halves[part - 1],)
        if k < 3:
            right, left = step_right(right, k + 1), step_left(left, k + 1)
        elif k == 3:
            halves = [step_right(right[:, : KEYS // 2], 4), step_right(right[:, KEYS // 2 :], 4)]
        ins = (idx, q) + pays + (acc, m, sums)
        at = len(pays) + 2
        if part < 2:
            outs, scratch, aliases = (acc_t, m_t, sums_t), work, {at: 0, at + 1: 1}
        else:
            outs, aliases = (sds((72, KEYS), F32), sds((72, KEYS), F32)), None
            scratch = work + [pltpu.VMEM(sums_t.shape, F32)]
        res = call(
            functools.partial(step_body, k, part),
            outs,
            [SMEM] + [VMEM] * (len(ins) - 1),
            scratch,
            6e9 if k < 4 else 2e9,
            aliases,
        )(*ins)
        if part < 2:
            acc, m, sums = res
    sib = shift(res[1], "c", 1)
    w_full = call(assemble_body, sds((D, D), BF16), [SMEM] + [VMEM] * 4)(idx, *w_o)
    att = call(merge_body, sds((KEYS, HD), BF16), [VMEM, VMEM])(res[0], sib)
    att = lax.all_to_all(att.reshape(16, 64, HD), ("x", "y"), 0, 0, tiled=True)
    return call(final_body, sds((OWN, D), BF16), [VMEM] * 3)(att, out_gain[None], w_full)


def solution(mesh):
    finer = Mesh(mesh.devices.reshape(NZ, NX, NC, NY), AXES)
    sp = ("z", "x", "c")

    return jax.shard_map(
        shards,
        mesh=finer,
        in_specs=(
            P(AXES, None),
            P(),
            P(sp, "y"),
            P(sp, "y"),
            P(sp, "y"),
            P(sp, "y"),
            P("y"),
            P(sp, "y"),
            P(),
        ),
        out_specs=P(AXES, None),
        check_vma=False,
    )
```

```python
import functools
import math

import jax
import jax.numpy as jnp
from jax import lax
from jax.experimental import pallas as pl
from jax.experimental.pallas import tpu as pltpu
from jax.sharding import Mesh
from jax.sharding import PartitionSpec as P


AXES = ("z", "x", "c", "y")
NZ, NX, NC, NY = 8, 4, 2, 4
SIZES = {"z": NZ, "x": NX, "c": NC, "y": NY}
D = 1024
HD = 64
TOTAL = 16384
OWN = 64
BLK = 256
KEYS = 1024
QS = 2048
PAY = 136
EPS = 1e-06
LOW = -1e30
F32 = jnp.float32
BF16 = jnp.bfloat16


VMEM = pl.BlockSpec(memory_space=pltpu.VMEM)
SMEM = pl.BlockSpec(memory_space=pltpu.SMEM)


def call(body, outs, ins, scratch=(), flops=1e8, aliases=None):
    return pl.pallas_call(
        body,
        out_shape=outs,
        in_specs=ins,
        out_specs=jax.tree.map(lambda _: VMEM, outs),
        scratch_shapes=list(scratch),
        input_output_aliases=aliases or {},
        cost_estimate=pl.CostEstimate(
            flops=int(flops), bytes_accessed=1 << 20, transcendentals=0
        ),
        compiler_params=pltpu.CompilerParams(vmem_limit_bytes=24 << 20),
    )


def shift(x, axis, k):
    n = SIZES[axis]
    return lax.ppermute(x, axis, [(i, (i + k) % n) for i in range(n)])


def direct(x, axis):
    return [x] + [shift(x, axis, k) for k in range(1, SIZES[axis])]


def gather(x, axis):
    one, three = shift(x, axis, 1), shift(x, axis, -1)
    two = shift(one, axis, 1)
    return [x, one, two, three]


def step_right(x, k):
    return lax.ppermute(x, "z", [(i, i + 1) for i in range(k - 1, NZ - 1)])


def step_left(x, k):
    return lax.ppermute(x, "z", [((i - k + 1) % NZ, (i - k) % NZ) for i in range(3)])


def three_parts(x):
    hi = x.astype(BF16)
    rest = x - hi.astype(F32)
    mid = rest.astype(BF16)
    low = (rest - mid.astype(F32)).astype(BF16)
    return hi, mid, low


def pack_body(idx, rows, lo, hi, p0, o0, s1, s2, s3, heads):
    x = idx[1]
    lo[...] = rows[0:32, :]
    hi[...] = rows[32:64, :]
    o0[...] = rows[64:80, 768:1024]
    head = lax.broadcasted_iota(jnp.int32, (16, 256), 0)
    lane = lax.broadcasted_iota(jnp.int32, (16, 256), 1)
    pick = jnp.where(lane // HD == head, 1.0, 0.0).astype(BF16)
    gates = lax.dot_general(
        rows[80:96, 0:128], pick, (((0,), (0,)), ((), ())), preferred_element_type=F32
    )[0:16].astype(BF16)
    for h in range(NX):
        at = slice(h * HD, (h + 1) * HD)
        mine = [rows[64:80, i * 256 + h * HD : i * 256 + h * HD + HD] for i in range(3)]
        heads[h] = jnp.concatenate(mine + [gates[:, at]], axis=1)
    p0[...] = heads[x]
    for k, s in enumerate((s1, s2, s3)):
        s[0:32, :] = rows[32:64, :]
        s[32:48, 0:256] = heads[lax.rem(x + k + 1, NX)]
        s[32:48, 256:512] = rows[64:80, 768:1024]
        s[32:48, 512:1024] = jnp.zeros((16, 512), BF16)


def spread_body(hi, p0, o0, r1, r2, r3, out, toks):
    toks[0:32, :] = hi[...]
    for k, r in enumerate((r1, r2, r3)):
        toks[32 * k + 32 : 32 * k + 64, :] = r[0:32, :]
    for z in range(NZ):
        out[z, 0:16, :] = p0[...]
        out[z, 64:80, :] = o0[...]
        for k, r in enumerate((r1, r2, r3)):
            out[z, 16 * k + 16 : 16 * k + 32, :] = r[32:48, 0:256]
            out[z, 16 * k + 80 : 16 * k + 96, :] = r[32:48, 256:512]


def project_body(idx, offs, *refs):
    toks = refs[:8]
    gain, w_own, w_sib = refs[8:11]
    qc_out, kv_out, cum_out = refs[11:14]
    w, rows = refs[14:]
    x, c, y = idx[1], idx[2], idx[3]
    for z in range(NZ):
        for xx in range(NX):
            base = z * 128 + lax.rem(x - xx + NX, NX) * 32
            own_at = pl.multiple_of(base + c * 16, 16)
            sib_at = pl.multiple_of(base + (1 - c) * 16, 16)
            w[pl.ds(own_at, 16), :] = w_own[z, xx * 16 : xx * 16 + 16, :]
            w[pl.ds(sib_at, 16), :] = w_sib[z, xx * 16 : xx * 16 + 16, :]
    for half in range(2):
        for outer in range(4):
            tok = toks[half * 4 + outer][...].astype(F32)
            scale = lax.rsqrt(jnp.mean(tok * tok, axis=-1, keepdims=True) + EPS)
            normed = (tok * scale * gain[...]).astype(BF16)
            out = jnp.dot(normed, w[...], preferred_element_type=F32)
            for inner in range(4):
                kx, ky = (outer, inner) if half == 0 else (inner, outer)
                xx = lax.rem(x - kx + NX, NX)
                yy = lax.rem(y - ky + NY, NY)
                at = pl.multiple_of(xx * BLK + yy * OWN + half * 32, 32)
                rows[pl.ds(at, 32), :] = out[inner * 32 : inner * 32 + 32, :]
    before = lax.broadcasted_iota(jnp.int32, (BLK, BLK), 0)
    after = lax.broadcasted_iota(jnp.int32, (BLK, BLK), 1)
    ones = jnp.where(before <= after, 1.0, 0.0).astype(BF16)
    for b in range(4):
        t = rows[b * BLK : (b + 1) * BLK, :].T
        lanes = slice(b * BLK, (b + 1) * BLK)
        qc_out[0:64, lanes] = t[:64].astype(BF16)
        kv_out[:, lanes] = t[64:192].astype(BF16)
        logit = t[192:200] + offs[x] + math.log(TOTAL)
        gate = jnp.minimum(logit, 0.0) - jnp.log1p(jnp.exp(-jnp.abs(logit)))
        hi, mid, low = three_parts(gate)
        cum = jnp.dot(hi, ones, preferred_element_type=F32)
        cum = cum + jnp.dot(mid, ones, preferred_element_type=F32)
        cum = cum + jnp.dot(low, ones, preferred_element_type=F32)
        cum_out[:, lanes] = cum
        row = lax.broadcasted_iota(jnp.int32, (16, BLK), 0)
        block = jnp.zeros((16, BLK), F32)
        for i, part in enumerate(three_parts(cum[0:1])):
            block = jnp.where(row == i, part.astype(F32), block)
        qc_out[64:80, lanes] = block.astype(BF16)


def prepare_body(idx, q_own, q_sib, kv, cum_own, q_out, pay_out):
    c = idx[2]
    q_out[80:128, :] = jnp.zeros((48, QS), BF16)
    row = lax.broadcasted_iota(jnp.int32, (16, QS), 0)
    q_out[64:80, :] = jnp.where(row < 3, 1.0, 0.0).astype(BF16)
    for b in range(4):
        lanes = slice(b * BLK, (b + 1) * BLK)
        own_at = pl.multiple_of((2 * b + c) * BLK, BLK)
        sib_at = pl.multiple_of((2 * b + 1 - c) * BLK, BLK)
        q_out[0:64, pl.ds(own_at, BLK)] = q_own[0:64, lanes] * jnp.asarray(0.125, BF16)
        q_out[0:64, pl.ds(sib_at, BLK)] = q_sib[0:64, lanes] * jnp.asarray(0.125, BF16)
    own, sib = [], []
    for b in range(4):
        end = slice(b * BLK + BLK - 1, b * BLK + BLK)
        own.append(cum_own[:, end])
        parts = q_sib[64:80, b * BLK + 128 : b * BLK + BLK].astype(F32)[:, 127:128]
        sib.append(jnp.broadcast_to(parts[0:1] + parts[1:2] + parts[2:3], (8, 1)))
    ahead = jnp.zeros_like(own[0])
    bases = []
    for b in range(4):
        bases.append(ahead + jnp.where(c == 1, sib[b], 0.0))
        ahead = ahead + (own[b] + sib[b])
    total = ahead
    pay_out[0:64, :] = kv[64:128, :]
    pay_out[64:128, :] = kv[0:64, :]
    row = lax.broadcasted_iota(jnp.int32, (8, BLK), 0)
    for b in range(4):
        lanes = slice(b * BLK, (b + 1) * BLK)
        bias = (total - bases[b]) - cum_own[:, lanes]
        parts = [p[0:1].astype(F32) for p in three_parts(bias)]
        totals = [p[0:1].astype(F32) for p in three_parts(jnp.broadcast_to(total, bias.shape))]
        block = jnp.zeros((8, BLK), F32)
        for i, part in enumerate(parts + totals):
            block = jnp.where(row == i, part, block)
        pay_out[128:136, lanes] = block.astype(BF16)


def chunk_total(pay):
    rows = pay[128:136, 0:BLK].astype(F32)
    return rows[3:4] + rows[4:5] + rows[5:6]


def place_chunk(pay, i, kx, vx):
    fill = jnp.zeros((56, 128), F32)
    for r in range(8):
        lanes = slice(r * 128, (r + 1) * 128)
        tile = jnp.concatenate([pay[64:136, lanes].astype(F32), fill], axis=0)
        kx[i, lanes, :] = tile.T.astype(BF16)
    vx[i, 0:64, :] = pay[0:64, :]
    vx[i, 64:80, :] = jnp.ones((16, KEYS), BF16)


def stages(q, acc, m, kx, vx, move, work):
    tiles = QS // BLK
    bufs, tops, probs, fades = work[0:2], work[2:4], work[4:6], work[6:8]

    def lanes_of(t):
        if isinstance(t, int):
            return slice((t % tiles) * BLK, (t % tiles + 1) * BLK)
        return pl.ds(pl.multiple_of((t % tiles) * BLK, BLK), BLK)

    def score(t, slot, n=KEYS, allowed=None):
        s = jnp.dot(kx[t // tiles, 0:n], q[:, lanes_of(t)], preferred_element_type=F32)
        if allowed is not None:
            last = jnp.where(allowed, s[n - BLK : n], LOW)
            s = last if n == BLK else jnp.concatenate([s[0 : n - BLK], last], axis=0)
        bufs[slot][0:n] = s
        tops[slot][...] = jnp.broadcast_to(jnp.max(s, axis=0, keepdims=True), (8, BLK))

    def weigh(t, slot, n=KEYS):
        i, lanes = t // tiles, lanes_of(t)
        by = move[i, 0:1]
        old = m[i, 0:1, lanes]
        new = jnp.maximum(old, tops[slot][0:1] + by)
        probs[slot][0:n] = jnp.exp(bufs[slot][0:n] - (new - by)).astype(BF16)
        fades[slot][...] = jnp.broadcast_to(jnp.exp(old - new), (8, BLK))
        m[i, :, lanes] = jnp.broadcast_to(new, (8, BLK))

    def add(t, slot, n=KEYS):
        i, lanes = t // tiles, lanes_of(t)
        part = jnp.dot(vx[i, :, 0:n], probs[slot][0:n], preferred_element_type=F32)
        acc[i, :, lanes] = acc[i, :, lanes] * fades[slot][0:1] + part

    return score, weigh, add


def absorb(count, q, acc, m, kx, vx, move, work):
    tiles = QS // BLK
    score, weigh, add = stages(q, acc, m, kx, vx, move, work)
    probs, fades = work[4:6], work[6:8]

    @pl.when(count > 0)
    def _():
        probs[1][...] = jnp.zeros((KEYS, BLK), BF16)
        fades[1][...] = jnp.ones((8, BLK), F32)
        score(0, 0)
        last = count * tiles - 1

        def two_tiles(j, carry):
            t = 2 * j
            add(jnp.maximum(t - 1, 0), 1)
            weigh(t, 0)
            score(t + 1, 1)
            add(t, 0)
            weigh(t + 1, 1)
            score(jnp.minimum(t + 2, last), 0)
            return carry

        lax.fori_loop(0, count * (tiles // 2), two_tiles, 0)
        add(last, 1)


def first_body(idx, q, pay, acc, m, sums, kx, vx, move, *bufs):
    acc[...] = jnp.zeros_like(acc)
    m[...] = jnp.full(m.shape, LOW, F32)
    move[...] = jnp.zeros_like(move)
    place_chunk(pay, 0, kx, vx)
    score, weigh, add = stages(q, acc, m, kx, vx, move, bufs)
    key = lax.broadcasted_iota(jnp.int32, (BLK, BLK), 0)
    query = lax.broadcasted_iota(jnp.int32, (BLK, BLK), 1)
    tiles = QS // BLK
    meets = [(b // 2 + 1) * BLK for b in range(tiles)]
    masks = [key + (idx[2] - odd) * BLK <= query for odd in range(2)]
    for b in range(tiles + 2):
        if b < tiles:
            score(b, b % 2, meets[b], masks[b % 2])
        if 0 <= b - 1 < tiles:
            weigh(b - 1, (b - 1) % 2, meets[b - 1])
        if 0 <= b - 2:
            add(b - 2, (b - 2) % 2, meets[b - 2])
    sums[...] = jnp.broadcast_to(chunk_total(pay), sums.shape)


def step_body(k, idx, q, *refs):
    z = idx[0]
    n_pay = 2 if k < 4 else 1
    pays, refs = refs[:n_pay], refs[n_pay:]
    acc0, m0, sums0, refs = refs[0], refs[1], refs[2], refs[3:]
    if k < 4:
        acc, m, sums, kx, vx, move, *bufs = refs
    else:
        out_own, out_sib, kx, vx, move, *bufs, sums = refs
        acc, m = acc0, m0
    sums[...] = sums0[...]
    count = (z >= k).astype(jnp.int32)

    @pl.when(z >= k)
    def _():
        place_chunk(pays[0], 0, kx, vx)
        move[0] = sums0[...]
        sums[...] = sums0[...] + jnp.broadcast_to(chunk_total(pays[0]), sums.shape)

    if k < 4:
        count = count + (z + k >= 8).astype(jnp.int32)

        @pl.when(z + k >= 8)
        def _():
            place_chunk(pays[1], 1, kx, vx)
            move[1] = jnp.zeros(sums.shape, F32)
            m[1] = m[1] + chunk_total(pays[1])[:, 0:1]

    absorb(count, q, acc, m, kx, vx, move, bufs)
    if k == 4:
        c = idx[2]
        row = lax.broadcasted_iota(jnp.int32, (8, BLK), 0)
        for b in range(4):
            for other in range(2):
                at = 2 * b + (c if other == 0 else 1 - c)
                lanes = pl.ds(pl.multiple_of(at * BLK, BLK), BLK)
                m_a = m[0, 0:1, lanes]
                m_b = m[1, 0:1, lanes] + sums[0:1]
                top = jnp.maximum(m_a, m_b)
                both = acc[0, :, lanes] * jnp.exp(m_a - top) + acc[1, :, lanes] * jnp.exp(m_b - top)
                to = slice(b * BLK, (b + 1) * BLK)
                out = out_own if other == 0 else out_sib
                out[0:64, to] = both[0:64]
                out[64:72, to] = jnp.where(row < 4, both[64:65], top)


def merge_body(own, sib, out):
    a, b = own[...], sib[...]
    m_a, m_b = a[68:69], b[68:69]
    top = jnp.maximum(m_a, m_b)
    f_a, f_b = jnp.exp(m_a - top), jnp.exp(m_b - top)
    total = a[64:65] * f_a + b[64:65] * f_b
    att = (a[0:64] * f_a + b[0:64] * f_b) / total
    att = jnp.concatenate([att, jnp.zeros_like(att)], axis=0)
    for r in range(8):
        out[r * 128 : (r + 1) * 128, :] = att[:, r * 128 : (r + 1) * 128].T[:, 0:64].astype(BF16)


def assemble_body(idx, w0, w1, w2, w3, w):
    x, c, y = idx[1], idx[2], idx[3]
    for ky, ref in enumerate((w0, w1, w2, w3)):
        cols = pl.ds(pl.multiple_of(lax.rem(y - ky + NY, NY) * 256, 256), 256)
        for kx in range(NX):
            xx = lax.rem(x - kx + NX, NX)
            for other in range(2):
                cc = c if other == 0 else 1 - c
                for z in range(NZ):
                    at = pl.multiple_of(z * 128 + xx * 32 + cc * 16, 16)
                    w[pl.ds(at, 16), cols] = ref[other, z, kx * 16 : kx * 16 + 16, :]


def final_body(att, gain, w, out):
    pieces = [att[xs * NY + ys] for ys in range(NY) for xs in range(NX)]
    joined = jnp.concatenate(pieces, axis=1)
    proj = lax.dot_general(joined, w[...], (((1,), (1,)), ((), ())), preferred_element_type=F32)
    scale = lax.rsqrt(jnp.mean(proj * proj, axis=-1, keepdims=True) + EPS)
    out[...] = (proj * scale * gain[...]).astype(BF16)


def shards(tokens, norm_gain, w_query, w_key, w_value, w_forget, forget_offset, w_out_t, out_gain):
    sds = jax.ShapeDtypeStruct
    idx = jnp.stack([lax.axis_index(a) for a in AXES]).astype(jnp.int32)

    half, piece, send = sds((32, D), BF16), sds((16, 256), BF16), sds((48, D), BF16)
    rows = jnp.pad(tokens, ((0, 32), (0, 0)))
    for i, w in enumerate((w_query, w_key, w_value, w_out_t)):
        rows = rows + jnp.pad(w, ((64, 16), (256 * i, 768 - 256 * i)))
    rows = rows + jnp.pad(w_forget.T, ((80, 16 - NX), (0, D - 16)))
    lo, hi, p0, o0, *sends = call(
        pack_body,
        (half, half, piece, piece, send, send, send),
        [SMEM, VMEM],
        [pltpu.VMEM((NX, 16, 256), BF16)],
    )(idx, rows)

    got = [shift(sends[k - 1], "x", k) for k in range(1, NX)]
    tok_a = direct(lo, "y")
    chunk, tok_b = call(
        spread_body, (sds((NZ, 128, 256), BF16), sds((128, D), BF16)), [VMEM] * 6
    )(hi, p0, o0, *got)
    w_own = lax.all_to_all(chunk, "z", 0, 0, tiled=True)
    toks_b = gather(tok_b, "y")
    toks = gather(jnp.concatenate(tok_a, axis=0), "x") + toks_b
    w_sib = shift(w_own, "c", 1)

    q_own, kv, cum_own = call(
        project_body,
        (sds((80, KEYS), BF16), sds((128, KEYS), BF16), sds((8, KEYS), F32)),
        [SMEM, SMEM] + [VMEM] * 11,
        [pltpu.VMEM((D, 256), BF16), pltpu.VMEM((KEYS, 256), F32)],
        2e9,
    )(idx, forget_offset, *toks, norm_gain[None], w_own, w_sib)

    q_sib = shift(q_own, "c", 1)
    q, pay = call(
        prepare_body, (sds((128, QS), BF16), sds((PAY, KEYS), BF16)), [SMEM] + [VMEM] * 4
    )(idx, q_own, q_sib, kv, cum_own)

    acc_t, m_t, sums_t = sds((2, 80, QS), F32), sds((2, 8, QS), F32), sds((8, BLK), F32)
    work = [
        pltpu.VMEM((2, KEYS, 128), BF16),
        pltpu.VMEM((2, 80, KEYS), BF16),
        pltpu.VMEM((2, 8, BLK), F32),
        pltpu.VMEM((KEYS, BLK), F32),
        pltpu.VMEM((KEYS, BLK), F32),
        pltpu.VMEM((8, BLK), F32),
        pltpu.VMEM((8, BLK), F32),
        pltpu.VMEM((KEYS, BLK), BF16),
        pltpu.VMEM((KEYS, BLK), BF16),
        pltpu.VMEM((8, BLK), F32),
        pltpu.VMEM((8, BLK), F32),
    ]
    right = step_right(pay, 1)
    left = step_left(pay, 1)
    acc, m, sums = call(
        first_body, (acc_t, m_t, sums_t), [SMEM, VMEM, VMEM], work, 3e9
    )(idx, q, pay)

    w_o = jnp.stack([w_own[:, 64:], w_sib[:, 64:]])
    w_o, _ = lax.optimization_barrier((w_o, sums))
    w_o = direct(w_o, "y")

    for k in range(1, 5):
        pays = (right, left) if k < 4 else (right,)
        if k < 4:
            right = step_right(pays[0], k + 1)
        if k < 3:
            left = step_left(pays[1], k + 1)
        ins = (idx, q) + pays + (acc, m, sums)
        if k < 4:
            outs, scratch, aliases = (acc_t, m_t, sums_t), work, {4: 0, 5: 1}
        else:
            outs, aliases = (sds((72, KEYS), F32), sds((72, KEYS), F32)), None
            scratch = work + [pltpu.VMEM(sums_t.shape, F32)]
        res = call(
            functools.partial(step_body, k),
            outs,
            [SMEM] + [VMEM] * (len(ins) - 1),
            scratch,
            6e9,
            aliases,
        )(*ins)
        if k < 4:
            acc, m, sums = res
    sib = shift(res[1], "c", 1)
    w_full = call(assemble_body, sds((D, D), BF16), [SMEM] + [VMEM] * 4)(idx, *w_o)
    att = call(merge_body, sds((KEYS, HD), BF16), [VMEM, VMEM])(res[0], sib)
    att = lax.all_to_all(att.reshape(16, 64, HD), ("x", "y"), 0, 0, tiled=True)
    return call(final_body, sds((OWN, D), BF16), [VMEM] * 3)(att, out_gain[None], w_full)


def solution(mesh):
    finer = Mesh(mesh.devices.reshape(NZ, NX, NC, NY), AXES)
    sp = ("z", "x", "c")

    return jax.shard_map(
        shards,
        mesh=finer,
        in_specs=(
            P(AXES, None),
            P(),
            P(sp, "y"),
            P(sp, "y"),
            P(sp, "y"),
            P(sp, "y"),
            P("y"),
            P(sp, "y"),
            P(),
        ),
        out_specs=P(AXES, None),
        check_vma=False,
    )
```

```python
import functools
import math

import jax
import jax.numpy as jnp
from jax import lax
from jax.experimental import pallas as pl
from jax.experimental.pallas import tpu as pltpu
from jax.sharding import Mesh
from jax.sharding import PartitionSpec as P


AXES = ("z", "x", "c", "y")
NZ, NX, NC, NY = 8, 4, 2, 4
SIZES = {"z": NZ, "x": NX, "c": NC, "y": NY}
D = 1024
HD = 64
TOTAL = 16384
OWN = 64
BLK = 256
KEYS = 1024
QS = 2048
PAY = 136
EPS = 1e-06
LOW = -1e30
F32 = jnp.float32
BF16 = jnp.bfloat16


VMEM = pl.BlockSpec(memory_space=pltpu.VMEM)
SMEM = pl.BlockSpec(memory_space=pltpu.SMEM)


def call(body, outs, ins, scratch=(), flops=1e8, aliases=None):
    return pl.pallas_call(
        body,
        out_shape=outs,
        in_specs=ins,
        out_specs=jax.tree.map(lambda _: VMEM, outs),
        scratch_shapes=list(scratch),
        input_output_aliases=aliases or {},
        cost_estimate=pl.CostEstimate(
            flops=int(flops), bytes_accessed=1 << 20, transcendentals=0
        ),
        compiler_params=pltpu.CompilerParams(vmem_limit_bytes=24 << 20),
    )


def shift(x, axis, k):
    n = SIZES[axis]
    return lax.ppermute(x, axis, [(i, (i + k) % n) for i in range(n)])


def direct(x, axis):
    return [x] + [shift(x, axis, k) for k in range(1, SIZES[axis])]


def gather(x, axis):
    one = shift(x, axis, 1)
    three = shift(x, axis, -1)
    two = shift(one, axis, 1)
    return [x, one, two, three]


def step_right(x, k):
    return lax.ppermute(x, "z", [(i, i + 1) for i in range(k - 1, NZ - 1)])


def step_left(x, k):
    return lax.ppermute(x, "z", [((i - k + 1) % NZ, (i - k) % NZ) for i in range(3)])


def three_parts(x):
    hi = x.astype(BF16)
    rest = x - hi.astype(F32)
    mid = rest.astype(BF16)
    low = (rest - mid.astype(F32)).astype(BF16)
    return hi, mid, low


def pack_body(idx, rows, lo, hi, p0, o0, s1, s2, s3, heads):
    x = idx[1]
    lo[...] = rows[0:32, :]
    hi[...] = rows[32:64, :]
    o0[...] = rows[64:80, 768:1024]
    head = lax.broadcasted_iota(jnp.int32, (16, 256), 0)
    lane = lax.broadcasted_iota(jnp.int32, (16, 256), 1)
    pick = jnp.where(lane // HD == head, 1.0, 0.0).astype(BF16)
    gates = lax.dot_general(
        rows[80:96, 0:128], pick, (((0,), (0,)), ((), ())), preferred_element_type=F32
    )[0:16].astype(BF16)
    for h in range(NX):
        at = slice(h * HD, (h + 1) * HD)
        mine = [rows[64:80, i * 256 + h * HD : i * 256 + h * HD + HD] for i in range(3)]
        heads[h] = jnp.concatenate(mine + [gates[:, at]], axis=1)
    p0[...] = heads[x]
    for k, s in enumerate((s1, s2, s3)):
        s[0:32, :] = rows[32:64, :]
        s[32:48, 0:256] = heads[lax.rem(x + k + 1, NX)]
        s[32:48, 256:512] = rows[64:80, 768:1024]
        s[32:48, 512:1024] = jnp.zeros((16, 512), BF16)


def spread_body(hi, p0, o0, r1, r2, r3, out, toks):
    toks[0:32, :] = hi[...]
    for k, r in enumerate((r1, r2, r3)):
        toks[32 * k + 32 : 32 * k + 64, :] = r[0:32, :]
    for z in range(NZ):
        out[z, 0:16, :] = p0[...]
        out[z, 64:80, :] = o0[...]
        for k, r in enumerate((r1, r2, r3)):
            out[z, 16 * k + 16 : 16 * k + 32, :] = r[32:48, 0:256]
            out[z, 16 * k + 80 : 16 * k + 96, :] = r[32:48, 256:512]


def project_body(idx, offs, *refs):
    toks = refs[:8]
    gain, w_own, w_sib = refs[8:11]
    qc_out, kv_out, cum_out = refs[11:14]
    w, normed = refs[14:]
    x, c, y = idx[1], idx[2], idx[3]
    for z in range(NZ):
        for xx in range(NX):
            base = z * 128 + lax.rem(x - xx + NX, NX) * 32
            own_at = pl.multiple_of(base + c * 16, 16)
            sib_at = pl.multiple_of(base + (1 - c) * 16, 16)
            w[pl.ds(own_at, 16), :] = w_own[z, xx * 16 : xx * 16 + 16, :]
            w[pl.ds(sib_at, 16), :] = w_sib[z, xx * 16 : xx * 16 + 16, :]
    for half in range(2):
        for outer in range(4):
            tok = toks[half * 4 + outer][...].astype(F32)
            scale = lax.rsqrt(jnp.mean(tok * tok, axis=-1, keepdims=True) + EPS)
            out = (tok * scale * gain[...]).astype(BF16)
            for inner in range(4):
                kx, ky = (outer, inner) if half == 0 else (inner, outer)
                xx = lax.rem(x - kx + NX, NX)
                yy = lax.rem(y - ky + NY, NY)
                at = pl.multiple_of(xx * BLK + yy * OWN + half * 32, 32)
                normed[pl.ds(at, 32), :] = out[inner * 32 : inner * 32 + 32, :]
    before = lax.broadcasted_iota(jnp.int32, (BLK, BLK), 0)
    after = lax.broadcasted_iota(jnp.int32, (BLK, BLK), 1)
    ones = jnp.where(before <= after, 1.0, 0.0).astype(BF16)
    for b in range(4):
        if b % 2 == 0:
            pair = normed[b * BLK : (b + 2) * BLK, :]
            columns = jnp.dot(pair, w[...], preferred_element_type=F32)
        t = columns[b % 2 * BLK : (b % 2 + 1) * BLK].T
        lanes = slice(b * BLK, (b + 1) * BLK)
        qc_out[0:64, lanes] = t[:64].astype(BF16)
        kv_out[:, lanes] = t[64:192].astype(BF16)
        logit = t[192:200] + offs[x] + math.log(TOTAL)
        gate = jnp.minimum(logit, 0.0) - jnp.log1p(jnp.exp(-jnp.abs(logit)))
        hi, mid, low = three_parts(gate)
        cum = jnp.dot(hi, ones, preferred_element_type=F32)
        cum = cum + jnp.dot(mid, ones, preferred_element_type=F32)
        cum = cum + jnp.dot(low, ones, preferred_element_type=F32)
        cum_out[:, lanes] = cum
        row = lax.broadcasted_iota(jnp.int32, (16, BLK), 0)
        block = jnp.zeros((16, BLK), F32)
        for i, part in enumerate(three_parts(cum[0:1])):
            block = jnp.where(row == i, part.astype(F32), block)
        qc_out[64:80, lanes] = block.astype(BF16)


def prepare_body(idx, q_own, q_sib, kv, cum_own, q_out, pay_out):
    c = idx[2]
    q_out[80:128, :] = jnp.zeros((48, QS), BF16)
    row = lax.broadcasted_iota(jnp.int32, (16, QS), 0)
    q_out[64:80, :] = jnp.where(row < 3, 1.0, 0.0).astype(BF16)
    for b in range(4):
        lanes = slice(b * BLK, (b + 1) * BLK)
        own_at = pl.multiple_of((2 * b + c) * BLK, BLK)
        sib_at = pl.multiple_of((2 * b + 1 - c) * BLK, BLK)
        q_out[0:64, pl.ds(own_at, BLK)] = q_own[0:64, lanes] * jnp.asarray(0.125, BF16)
        q_out[0:64, pl.ds(sib_at, BLK)] = q_sib[0:64, lanes] * jnp.asarray(0.125, BF16)
    own, sib = [], []
    for b in range(4):
        end = slice(b * BLK + BLK - 1, b * BLK + BLK)
        own.append(cum_own[:, end])
        parts = q_sib[64:80, b * BLK + 128 : b * BLK + BLK].astype(F32)[:, 127:128]
        sib.append(jnp.broadcast_to(parts[0:1] + parts[1:2] + parts[2:3], (8, 1)))
    ahead = jnp.zeros_like(own[0])
    bases = []
    for b in range(4):
        bases.append(ahead + jnp.where(c == 1, sib[b], 0.0))
        ahead = ahead + (own[b] + sib[b])
    total = ahead
    pay_out[0:64, :] = kv[64:128, :]
    pay_out[64:128, :] = kv[0:64, :]
    row = lax.broadcasted_iota(jnp.int32, (8, BLK), 0)
    for b in range(4):
        lanes = slice(b * BLK, (b + 1) * BLK)
        bias = (total - bases[b]) - cum_own[:, lanes]
        parts = [p[0:1].astype(F32) for p in three_parts(bias)]
        totals = [p[0:1].astype(F32) for p in three_parts(jnp.broadcast_to(total, bias.shape))]
        block = jnp.zeros((8, BLK), F32)
        for i, part in enumerate(parts + totals):
            block = jnp.where(row == i, part, block)
        pay_out[128:136, lanes] = block.astype(BF16)


def chunk_total(pay):
    rows = pay[128:136, 0:BLK].astype(F32)
    return rows[3:4] + rows[4:5] + rows[5:6]


def place_chunk(pay, i, kx, vx):
    fill = jnp.zeros((56, 128), F32)
    for r in range(8):
        lanes = slice(r * 128, (r + 1) * 128)
        tile = jnp.concatenate([pay[64:136, lanes].astype(F32), fill], axis=0)
        kx[i, lanes, :] = tile.T.astype(BF16)
    vx[i, 0:64, :] = pay[0:64, :]
    vx[i, 64:80, :] = jnp.ones((16, KEYS), BF16)


def stages(q, acc, m, kx, vx, move, work):
    tiles = QS // BLK
    bufs, tops, probs, fades = work[0:2], work[2:4], work[4:6], work[6:8]

    def lanes_of(t):
        if isinstance(t, int):
            return slice((t % tiles) * BLK, (t % tiles + 1) * BLK)
        return pl.ds(pl.multiple_of((t % tiles) * BLK, BLK), BLK)

    def score(t, slot, n=KEYS, allowed=None):
        s = jnp.dot(kx[t // tiles, 0:n], q[:, lanes_of(t)], preferred_element_type=F32)
        if allowed is not None:
            last = jnp.where(allowed, s[n - BLK : n], LOW)
            s = last if n == BLK else jnp.concatenate([s[0 : n - BLK], last], axis=0)
        bufs[slot][0:n] = s
        tops[slot][...] = jnp.broadcast_to(jnp.max(s, axis=0, keepdims=True), (8, BLK))

    def weigh(t, slot, n=KEYS):
        i, lanes = t // tiles, lanes_of(t)
        by = move[i, 0:1]
        old = m[i, 0:1, lanes]
        new = jnp.maximum(old, tops[slot][0:1] + by)
        probs[slot][0:n] = jnp.exp(bufs[slot][0:n] - (new - by)).astype(BF16)
        fades[slot][...] = jnp.broadcast_to(jnp.exp(old - new), (8, BLK))
        m[i, :, lanes] = jnp.broadcast_to(new, (8, BLK))

    def add(t, slot, n=KEYS):
        i, lanes = t // tiles, lanes_of(t)
        part = jnp.dot(vx[i, :, 0:n], probs[slot][0:n], preferred_element_type=F32)
        acc[i, :, lanes] = acc[i, :, lanes] * fades[slot][0:1] + part

    return score, weigh, add


def absorb(count, q, acc, m, kx, vx, move, work):
    tiles = QS // BLK
    score, weigh, add = stages(q, acc, m, kx, vx, move, work)
    probs, fades = work[4:6], work[6:8]

    @pl.when(count > 0)
    def _():
        probs[1][...] = jnp.zeros((KEYS, BLK), BF16)
        fades[1][...] = jnp.ones((8, BLK), F32)
        score(0, 0)
        last = count * tiles - 1

        def two_tiles(j, carry):
            t = 2 * j
            add(jnp.maximum(t - 1, 0), 1)
            weigh(t, 0)
            score(t + 1, 1)
            add(t, 0)
            weigh(t + 1, 1)
            score(jnp.minimum(t + 2, last), 0)
            return carry

        lax.fori_loop(0, count * (tiles // 2), two_tiles, 0)
        add(last, 1)


def first_body(idx, q, pay, acc, m, sums, kx, vx, move, *bufs):
    acc[...] = jnp.zeros_like(acc)
    m[...] = jnp.full(m.shape, LOW, F32)
    move[...] = jnp.zeros_like(move)
    place_chunk(pay, 0, kx, vx)
    score, weigh, add = stages(q, acc, m, kx, vx, move, bufs)
    key = lax.broadcasted_iota(jnp.int32, (BLK, BLK), 0)
    query = lax.broadcasted_iota(jnp.int32, (BLK, BLK), 1)
    tiles = QS // BLK
    meets = [(b // 2 + 1) * BLK for b in range(tiles)]
    masks = [key + (idx[2] - odd) * BLK <= query for odd in range(2)]
    for b in range(tiles + 2):
        if b < tiles:
            score(b, b % 2, meets[b], masks[b % 2])
        if 0 <= b - 1 < tiles:
            weigh(b - 1, (b - 1) % 2, meets[b - 1])
        if 0 <= b - 2:
            add(b - 2, (b - 2) % 2, meets[b - 2])
    sums[...] = jnp.broadcast_to(chunk_total(pay), sums.shape)


def step_body(k, idx, q, *refs):
    z = idx[0]
    n_pay = 2 if k < 4 else 1
    pays, refs = refs[:n_pay], refs[n_pay:]
    acc0, m0, sums0, refs = refs[0], refs[1], refs[2], refs[3:]
    if k < 4:
        acc, m, sums, kx, vx, move, *bufs = refs
    else:
        out_own, out_sib, kx, vx, move, *bufs, sums = refs
        acc, m = acc0, m0
    sums[...] = sums0[...]
    count = (z >= k).astype(jnp.int32)

    @pl.when(z >= k)
    def _():
        place_chunk(pays[0], 0, kx, vx)
        move[0] = sums0[...]
        sums[...] = sums0[...] + jnp.broadcast_to(chunk_total(pays[0]), sums.shape)

    if k < 4:
        count = count + (z + k >= 8).astype(jnp.int32)

        @pl.when(z + k >= 8)
        def _():
            place_chunk(pays[1], 1, kx, vx)
            move[1] = jnp.zeros(sums.shape, F32)
            m[1] = m[1] + chunk_total(pays[1])[:, 0:1]

    absorb(count, q, acc, m, kx, vx, move, bufs)
    if k == 4:
        c = idx[2]
        row = lax.broadcasted_iota(jnp.int32, (8, BLK), 0)
        for b in range(4):
            for other in range(2):
                at = 2 * b + (c if other == 0 else 1 - c)
                lanes = pl.ds(pl.multiple_of(at * BLK, BLK), BLK)
                m_a = m[0, 0:1, lanes]
                m_b = m[1, 0:1, lanes] + sums[0:1]
                top = jnp.maximum(m_a, m_b)
                both = acc[0, :, lanes] * jnp.exp(m_a - top) + acc[1, :, lanes] * jnp.exp(m_b - top)
                to = slice(b * BLK, (b + 1) * BLK)
                out = out_own if other == 0 else out_sib
                out[0:64, to] = both[0:64]
                out[64:72, to] = jnp.where(row < 4, both[64:65], top)


def merge_body(own, sib, out):
    a, b = own[...], sib[...]
    m_a, m_b = a[68:69], b[68:69]
    top = jnp.maximum(m_a, m_b)
    f_a, f_b = jnp.exp(m_a - top), jnp.exp(m_b - top)
    total = a[64:65] * f_a + b[64:65] * f_b
    att = (a[0:64] * f_a + b[0:64] * f_b) / total
    att = jnp.concatenate([att, jnp.zeros_like(att)], axis=0)
    for r in range(8):
        out[r * 128 : (r + 1) * 128, :] = att[:, r * 128 : (r + 1) * 128].T[:, 0:64].astype(BF16)


def assemble_body(idx, w0, w1, w2, w3, w):
    x, c, y = idx[1], idx[2], idx[3]
    for ky, ref in enumerate((w0, w1, w2, w3)):
        cols = pl.ds(pl.multiple_of(lax.rem(y - ky + NY, NY) * 256, 256), 256)
        for kx in range(NX):
            xx = lax.rem(x - kx + NX, NX)
            for other in range(2):
                cc = c if other == 0 else 1 - c
                for z in range(NZ):
                    at = pl.multiple_of(z * 128 + xx * 32 + cc * 16, 16)
                    w[pl.ds(at, 16), cols] = ref[other, z, kx * 16 : kx * 16 + 16, :]


def final_body(att, gain, w, out):
    pieces = [att[xs * NY + ys] for ys in range(NY) for xs in range(NX)]
    joined = jnp.concatenate(pieces, axis=1)
    proj = lax.dot_general(joined, w[...], (((1,), (1,)), ((), ())), preferred_element_type=F32)
    scale = lax.rsqrt(jnp.mean(proj * proj, axis=-1, keepdims=True) + EPS)
    out[...] = (proj * scale * gain[...]).astype(BF16)


def shards(tokens, norm_gain, w_query, w_key, w_value, w_forget, forget_offset, w_out_t, out_gain):
    sds = jax.ShapeDtypeStruct
    idx = jnp.stack([lax.axis_index(a) for a in AXES]).astype(jnp.int32)

    half, piece, send = sds((32, D), BF16), sds((16, 256), BF16), sds((48, D), BF16)
    rows = jnp.pad(tokens, ((0, 32), (0, 0)))
    for i, w in enumerate((w_query, w_key, w_value, w_out_t)):
        rows = rows + jnp.pad(w, ((64, 16), (256 * i, 768 - 256 * i)))
    rows = rows + jnp.pad(w_forget.T, ((80, 16 - NX), (0, D - 16)))
    lo, hi, p0, o0, *sends = call(
        pack_body,
        (half, half, piece, piece, send, send, send),
        [SMEM, VMEM],
        [pltpu.VMEM((NX, 16, 256), BF16)],
    )(idx, rows)

    got = [shift(sends[k - 1], "x", k) for k in range(1, NX)]
    tok_a = direct(lo, "y")
    chunk, tok_b = call(
        spread_body, (sds((NZ, 128, 256), BF16), sds((128, D), BF16)), [VMEM] * 6
    )(hi, p0, o0, *got)
    w_own = lax.all_to_all(chunk, "z", 0, 0, tiled=True)
    toks_b = gather(tok_b, "y")
    toks = gather(jnp.concatenate(tok_a, axis=0), "x") + toks_b
    w_sib = shift(w_own, "c", 1)

    q_own, kv, cum_own = call(
        project_body,
        (sds((80, KEYS), BF16), sds((128, KEYS), BF16), sds((8, KEYS), F32)),
        [SMEM, SMEM] + [VMEM] * 11,
        [pltpu.VMEM((D, 256), BF16), pltpu.VMEM((KEYS, D), BF16)],
        2e9,
    )(idx, forget_offset, *toks, norm_gain[None], w_own, w_sib)

    q_sib = shift(q_own, "c", 1)
    q, pay = call(
        prepare_body, (sds((128, QS), BF16), sds((PAY, KEYS), BF16)), [SMEM] + [VMEM] * 4
    )(idx, q_own, q_sib, kv, cum_own)

    acc_t, m_t, sums_t = sds((2, 80, QS), F32), sds((2, 8, QS), F32), sds((8, BLK), F32)
    work = [
        pltpu.VMEM((2, KEYS, 128), BF16),
        pltpu.VMEM((2, 80, KEYS), BF16),
        pltpu.VMEM((2, 8, BLK), F32),
        pltpu.VMEM((KEYS, BLK), F32),
        pltpu.VMEM((KEYS, BLK), F32),
        pltpu.VMEM((8, BLK), F32),
        pltpu.VMEM((8, BLK), F32),
        pltpu.VMEM((KEYS, BLK), BF16),
        pltpu.VMEM((KEYS, BLK), BF16),
        pltpu.VMEM((8, BLK), F32),
        pltpu.VMEM((8, BLK), F32),
    ]
    right = step_right(pay, 1)
    left = step_left(pay, 1)
    acc, m, sums = call(
        first_body, (acc_t, m_t, sums_t), [SMEM, VMEM, VMEM], work, 3e9
    )(idx, q, pay)

    w_o = jnp.stack([w_own[:, 64:], w_sib[:, 64:]])
    w_o, _ = lax.optimization_barrier((w_o, sums))
    w_o = direct(w_o, "y")

    for k in range(1, 5):
        pays = (right, left) if k < 4 else (right,)
        if k < 4:
            right = step_right(pays[0], k + 1)
        if k < 3:
            left = step_left(pays[1], k + 1)
        ins = (idx, q) + pays + (acc, m, sums)
        if k < 4:
            outs, scratch, aliases = (acc_t, m_t, sums_t), work, {4: 0, 5: 1}
        else:
            outs, aliases = (sds((72, KEYS), F32), sds((72, KEYS), F32)), None
            scratch = work + [pltpu.VMEM(sums_t.shape, F32)]
        res = call(
            functools.partial(step_body, k),
            outs,
            [SMEM] + [VMEM] * (len(ins) - 1),
            scratch,
            6e9,
            aliases,
        )(*ins)
        if k < 4:
            acc, m, sums = res
    sib = shift(res[1], "c", 1)
    w_full = call(assemble_body, sds((D, D), BF16), [SMEM] + [VMEM] * 4)(idx, *w_o)
    att = call(merge_body, sds((KEYS, HD), BF16), [VMEM, VMEM])(res[0], sib)
    att = lax.all_to_all(att.reshape(16, 64, HD), ("x", "y"), 0, 0, tiled=True)
    return call(final_body, sds((OWN, D), BF16), [VMEM] * 3)(att, out_gain[None], w_full)


def solution(mesh):
    finer = Mesh(mesh.devices.reshape(NZ, NX, NC, NY), AXES)
    sp = ("z", "x", "c")

    return jax.shard_map(
        shards,
        mesh=finer,
        in_specs=(
            P(AXES, None),
            P(),
            P(sp, "y"),
            P(sp, "y"),
            P(sp, "y"),
            P(sp, "y"),
            P("y"),
            P(sp, "y"),
            P(),
        ),
        out_specs=P(AXES, None),
        check_vma=False,
    )
```

```python
import functools
import math

import jax
import jax.numpy as jnp
from jax import lax
from jax.experimental import pallas as pl
from jax.experimental.pallas import tpu as pltpu
from jax.sharding import Mesh
from jax.sharding import PartitionSpec as P


AXES = ("z", "x", "c", "y")
NZ, NX, NC, NY = 8, 4, 2, 4
SIZES = {"z": NZ, "x": NX, "c": NC, "y": NY}
D = 1024
HD = 64
TOTAL = 16384
OWN = 64
BLK = 256
KEYS = 1024
QS = 2048
PAY = 136
EPS = 1e-06
LOW = -1e30
F32 = jnp.float32
BF16 = jnp.bfloat16


VMEM = pl.BlockSpec(memory_space=pltpu.VMEM)
SMEM = pl.BlockSpec(memory_space=pltpu.SMEM)


def call(body, outs, ins, scratch=(), flops=1e8, aliases=None):
    return pl.pallas_call(
        body,
        out_shape=outs,
        in_specs=ins,
        out_specs=jax.tree.map(lambda _: VMEM, outs),
        scratch_shapes=list(scratch),
        input_output_aliases=aliases or {},
        cost_estimate=pl.CostEstimate(
            flops=int(flops), bytes_accessed=1 << 20, transcendentals=0
        ),
        compiler_params=pltpu.CompilerParams(vmem_limit_bytes=24 << 20),
    )


def shift(x, axis, k):
    n = SIZES[axis]
    return lax.ppermute(x, axis, [(i, (i + k) % n) for i in range(n)])


def direct(x, axis):
    return [x] + [shift(x, axis, k) for k in range(1, SIZES[axis])]


def gather(x, axis):
    one, three = shift(x, axis, 1), shift(x, axis, -1)
    two = shift(one, axis, 1)
    return [x, one, two, three]


def step_right(x, k):
    return lax.ppermute(x, "z", [(i, i + 1) for i in range(k - 1, NZ - 1)])


def step_left(x, k):
    return lax.ppermute(x, "z", [((i - k + 1) % NZ, (i - k) % NZ) for i in range(3)])


def three_parts(x):
    hi = x.astype(BF16)
    rest = x - hi.astype(F32)
    mid = rest.astype(BF16)
    low = (rest - mid.astype(F32)).astype(BF16)
    return hi, mid, low


def pack_body(idx, rows, lo, hi, p0, o0, s1, s2, s3, heads):
    x = idx[1]
    lo[...] = rows[0:32, :]
    hi[...] = rows[32:64, :]
    o0[...] = rows[64:80, 768:1024]
    head = lax.broadcasted_iota(jnp.int32, (16, 256), 0)
    lane = lax.broadcasted_iota(jnp.int32, (16, 256), 1)
    pick = jnp.where(lane // HD == head, 1.0, 0.0).astype(BF16)
    gates = lax.dot_general(
        rows[80:96, 0:128], pick, (((0,), (0,)), ((), ())), preferred_element_type=F32
    )[0:16].astype(BF16)
    for h in range(NX):
        at = slice(h * HD, (h + 1) * HD)
        mine = [rows[64:80, i * 256 + h * HD : i * 256 + h * HD + HD] for i in range(3)]
        heads[h] = jnp.concatenate(mine + [gates[:, at]], axis=1)
    p0[...] = heads[x]
    for k, s in enumerate((s1, s2, s3)):
        s[0:32, :] = rows[32:64, :]
        s[32:48, 0:256] = heads[lax.rem(x + k + 1, NX)]
        s[32:48, 256:512] = rows[64:80, 768:1024]
        s[32:48, 512:1024] = jnp.zeros((16, 512), BF16)


def spread_body(hi, p0, o0, r1, r2, r3, out, toks):
    toks[0:32, :] = hi[...]
    for k, r in enumerate((r1, r2, r3)):
        toks[32 * k + 32 : 32 * k + 64, :] = r[0:32, :]
    for z in range(NZ):
        out[z, 0:16, :] = p0[...]
        out[z, 64:80, :] = o0[...]
        for k, r in enumerate((r1, r2, r3)):
            out[z, 16 * k + 16 : 16 * k + 32, :] = r[32:48, 0:256]
            out[z, 16 * k + 80 : 16 * k + 96, :] = r[32:48, 256:512]


def project_body(idx, offs, *refs):
    toks = refs[:8]
    gain, w_own, w_sib = refs[8:11]
    qc_out, kv_out, cum_out = refs[11:14]
    w, rows = refs[14:]
    x, c, y = idx[1], idx[2], idx[3]
    for z in range(NZ):
        for xx in range(NX):
            base = z * 128 + lax.rem(x - xx + NX, NX) * 32
            own_at = pl.multiple_of(base + c * 16, 16)
            sib_at = pl.multiple_of(base + (1 - c) * 16, 16)
            w[pl.ds(own_at, 16), :] = w_own[z, xx * 16 : xx * 16 + 16, :]
            w[pl.ds(sib_at, 16), :] = w_sib[z, xx * 16 : xx * 16 + 16, :]
    for half in range(2):
        for two in range(2):
            parts = []
            for outer in (2 * two, 2 * two + 1):
                tok = toks[half * 4 + outer][...].astype(F32)
                scale = lax.rsqrt(jnp.mean(tok * tok, axis=-1, keepdims=True) + EPS)
                parts.append((tok * scale * gain[...]).astype(BF16))
            out = jnp.dot(jnp.concatenate(parts, axis=0), w[...], preferred_element_type=F32)
            for piece in range(8):
                outer, inner = 2 * two + piece // 4, piece % 4
                kx, ky = (outer, inner) if half == 0 else (inner, outer)
                xx = lax.rem(x - kx + NX, NX)
                yy = lax.rem(y - ky + NY, NY)
                at = pl.multiple_of(xx * BLK + yy * OWN + half * 32, 32)
                rows[pl.ds(at, 32), :] = out[piece * 32 : piece * 32 + 32, :]
    before = lax.broadcasted_iota(jnp.int32, (BLK, BLK), 0)
    after = lax.broadcasted_iota(jnp.int32, (BLK, BLK), 1)
    ones = jnp.where(before <= after, 1.0, 0.0).astype(BF16)
    for b in range(4):
        t = rows[b * BLK : (b + 1) * BLK, :].T
        lanes = slice(b * BLK, (b + 1) * BLK)
        qc_out[0:64, lanes] = t[:64].astype(BF16)
        kv_out[:, lanes] = t[64:192].astype(BF16)
        logit = t[192:200] + offs[x] + math.log(TOTAL)
        gate = jnp.minimum(logit, 0.0) - jnp.log1p(jnp.exp(-jnp.abs(logit)))
        hi, mid, low = three_parts(gate)
        cum = jnp.dot(hi, ones, preferred_element_type=F32)
        cum = cum + jnp.dot(mid, ones, preferred_element_type=F32)
        cum = cum + jnp.dot(low, ones, preferred_element_type=F32)
        cum_out[:, lanes] = cum
        row = lax.broadcasted_iota(jnp.int32, (16, BLK), 0)
        block = jnp.zeros((16, BLK), F32)
        for i, part in enumerate(three_parts(cum[0:1])):
            block = jnp.where(row == i, part.astype(F32), block)
        qc_out[64:80, lanes] = block.astype(BF16)


def prepare_body(idx, q_own, q_sib, kv, cum_own, q_out, pay_out):
    c = idx[2]
    q_out[80:128, :] = jnp.zeros((48, QS), BF16)
    row = lax.broadcasted_iota(jnp.int32, (16, QS), 0)
    q_out[64:80, :] = jnp.where(row < 3, 1.0, 0.0).astype(BF16)
    for b in range(4):
        lanes = slice(b * BLK, (b + 1) * BLK)
        own_at = pl.multiple_of((2 * b + c) * BLK, BLK)
        sib_at = pl.multiple_of((2 * b + 1 - c) * BLK, BLK)
        q_out[0:64, pl.ds(own_at, BLK)] = q_own[0:64, lanes] * jnp.asarray(0.125, BF16)
        q_out[0:64, pl.ds(sib_at, BLK)] = q_sib[0:64, lanes] * jnp.asarray(0.125, BF16)
    own, sib = [], []
    for b in range(4):
        end = slice(b * BLK + BLK - 1, b * BLK + BLK)
        own.append(cum_own[:, end])
        parts = q_sib[64:80, b * BLK + 128 : b * BLK + BLK].astype(F32)[:, 127:128]
        sib.append(jnp.broadcast_to(parts[0:1] + parts[1:2] + parts[2:3], (8, 1)))
    ahead = jnp.zeros_like(own[0])
    bases = []
    for b in range(4):
        bases.append(ahead + jnp.where(c == 1, sib[b], 0.0))
        ahead = ahead + (own[b] + sib[b])
    total = ahead
    pay_out[0:64, :] = kv[64:128, :]
    pay_out[64:128, :] = kv[0:64, :]
    row = lax.broadcasted_iota(jnp.int32, (8, BLK), 0)
    for b in range(4):
        lanes = slice(b * BLK, (b + 1) * BLK)
        bias = (total - bases[b]) - cum_own[:, lanes]
        parts = [p[0:1].astype(F32) for p in three_parts(bias)]
        totals = [p[0:1].astype(F32) for p in three_parts(jnp.broadcast_to(total, bias.shape))]
        block = jnp.zeros((8, BLK), F32)
        for i, part in enumerate(parts + totals):
            block = jnp.where(row == i, part, block)
        pay_out[128:136, lanes] = block.astype(BF16)


def chunk_total(pay):
    rows = pay[128:136, 0:BLK].astype(F32)
    return rows[3:4] + rows[4:5] + rows[5:6]


def place_chunk(pay, i, kx, vx):
    fill = jnp.zeros((56, 128), F32)
    for r in range(8):
        lanes = slice(r * 128, (r + 1) * 128)
        tile = jnp.concatenate([pay[64:136, lanes].astype(F32), fill], axis=0)
        kx[i, lanes, :] = tile.T.astype(BF16)
    vx[i, 0:64, :] = pay[0:64, :]
    vx[i, 64:80, :] = jnp.ones((16, KEYS), BF16)


def stages(q, acc, m, kx, vx, move, work):
    tiles = QS // BLK
    bufs, tops, probs, fades = work[0:2], work[2:4], work[4:6], work[6:8]

    def lanes_of(t):
        if isinstance(t, int):
            return slice((t % tiles) * BLK, (t % tiles + 1) * BLK)
        return pl.ds(pl.multiple_of((t % tiles) * BLK, BLK), BLK)

    def score(t, slot, n=KEYS, allowed=None):
        s = jnp.dot(kx[t // tiles, 0:n], q[:, lanes_of(t)], preferred_element_type=F32)
        if allowed is not None:
            last = jnp.where(allowed, s[n - BLK : n], LOW)
            s = last if n == BLK else jnp.concatenate([s[0 : n - BLK], last], axis=0)
        bufs[slot][0:n] = s
        tops[slot][...] = jnp.broadcast_to(jnp.max(s, axis=0, keepdims=True), (8, BLK))

    def weigh(t, slot, n=KEYS):
        i, lanes = t // tiles, lanes_of(t)
        by = move[i, 0:1]
        old = m[i, 0:1, lanes]
        new = jnp.maximum(old, tops[slot][0:1] + by)
        probs[slot][0:n] = jnp.exp(bufs[slot][0:n] - (new - by)).astype(BF16)
        fades[slot][...] = jnp.broadcast_to(jnp.exp(old - new), (8, BLK))
        m[i, :, lanes] = jnp.broadcast_to(new, (8, BLK))

    def add(t, slot, n=KEYS):
        i, lanes = t // tiles, lanes_of(t)
        part = jnp.dot(vx[i, :, 0:n], probs[slot][0:n], preferred_element_type=F32)
        acc[i, :, lanes] = acc[i, :, lanes] * fades[slot][0:1] + part

    return score, weigh, add


def absorb(count, q, acc, m, kx, vx, move, work):
    tiles = QS // BLK
    score, weigh, add = stages(q, acc, m, kx, vx, move, work)
    probs, fades = work[4:6], work[6:8]

    @pl.when(count > 0)
    def _():
        probs[1][...] = jnp.zeros((KEYS, BLK), BF16)
        fades[1][...] = jnp.ones((8, BLK), F32)
        score(0, 0)
        last = count * tiles - 1

        def two_tiles(j, carry):
            t = 2 * j
            add(jnp.maximum(t - 1, 0), 1)
            weigh(t, 0)
            score(t + 1, 1)
            add(t, 0)
            weigh(t + 1, 1)
            score(jnp.minimum(t + 2, last), 0)
            return carry

        lax.fori_loop(0, count * (tiles // 2), two_tiles, 0)
        add(last, 1)


def first_body(idx, q, pay, acc, m, sums, kx, vx, move, *bufs):
    acc[...] = jnp.zeros_like(acc)
    m[...] = jnp.full(m.shape, LOW, F32)
    move[...] = jnp.zeros_like(move)
    place_chunk(pay, 0, kx, vx)
    score, weigh, add = stages(q, acc, m, kx, vx, move, bufs)
    key = lax.broadcasted_iota(jnp.int32, (BLK, BLK), 0)
    query = lax.broadcasted_iota(jnp.int32, (BLK, BLK), 1)
    tiles = QS // BLK
    meets = [(b // 2 + 1) * BLK for b in range(tiles)]
    masks = [key + (idx[2] - odd) * BLK <= query for odd in range(2)]
    for b in range(tiles + 2):
        if b < tiles:
            score(b, b % 2, meets[b], masks[b % 2])
        if 0 <= b - 1 < tiles:
            weigh(b - 1, (b - 1) % 2, meets[b - 1])
        if 0 <= b - 2:
            add(b - 2, (b - 2) % 2, meets[b - 2])
    sums[...] = jnp.broadcast_to(chunk_total(pay), sums.shape)


def step_body(k, idx, q, *refs):
    z = idx[0]
    n_pay = 2 if k < 4 else 1
    pays, refs = refs[:n_pay], refs[n_pay:]
    acc0, m0, sums0, refs = refs[0], refs[1], refs[2], refs[3:]
    if k < 4:
        acc, m, sums, kx, vx, move, *bufs = refs
    else:
        out_own, out_sib, kx, vx, move, *bufs, sums = refs
        acc, m = acc0, m0
    sums[...] = sums0[...]
    count = (z >= k).astype(jnp.int32)

    @pl.when(z >= k)
    def _():
        place_chunk(pays[0], 0, kx, vx)
        move[0] = sums0[...]
        sums[...] = sums0[...] + jnp.broadcast_to(chunk_total(pays[0]), sums.shape)

    if k < 4:
        count = count + (z + k >= 8).astype(jnp.int32)

        @pl.when(z + k >= 8)
        def _():
            place_chunk(pays[1], 1, kx, vx)
            move[1] = jnp.zeros(sums.shape, F32)
            m[1] = m[1] + chunk_total(pays[1])[:, 0:1]

    absorb(count, q, acc, m, kx, vx, move, bufs)
    if k == 4:
        c = idx[2]
        row = lax.broadcasted_iota(jnp.int32, (8, BLK), 0)
        for b in range(4):
            for other in range(2):
                at = 2 * b + (c if other == 0 else 1 - c)
                lanes = pl.ds(pl.multiple_of(at * BLK, BLK), BLK)
                m_a = m[0, 0:1, lanes]
                m_b = m[1, 0:1, lanes] + sums[0:1]
                top = jnp.maximum(m_a, m_b)
                both = acc[0, :, lanes] * jnp.exp(m_a - top) + acc[1, :, lanes] * jnp.exp(m_b - top)
                to = slice(b * BLK, (b + 1) * BLK)
                out = out_own if other == 0 else out_sib
                out[0:64, to] = both[0:64]
                out[64:72, to] = jnp.where(row < 4, both[64:65], top)


def merge_body(own, sib, out):
    a, b = own[...], sib[...]
    m_a, m_b = a[68:69], b[68:69]
    top = jnp.maximum(m_a, m_b)
    f_a, f_b = jnp.exp(m_a - top), jnp.exp(m_b - top)
    total = a[64:65] * f_a + b[64:65] * f_b
    att = (a[0:64] * f_a + b[0:64] * f_b) / total
    att = jnp.concatenate([att, jnp.zeros_like(att)], axis=0)
    for r in range(8):
        out[r * 128 : (r + 1) * 128, :] = att[:, r * 128 : (r + 1) * 128].T[:, 0:64].astype(BF16)


def assemble_body(idx, w0, w1, w2, w3, w):
    x, c, y = idx[1], idx[2], idx[3]
    for ky, ref in enumerate((w0, w1, w2, w3)):
        cols = pl.ds(pl.multiple_of(lax.rem(y - ky + NY, NY) * 256, 256), 256)
        for kx in range(NX):
            xx = lax.rem(x - kx + NX, NX)
            for other in range(2):
                cc = c if other == 0 else 1 - c
                for z in range(NZ):
                    at = pl.multiple_of(z * 128 + xx * 32 + cc * 16, 16)
                    w[pl.ds(at, 16), cols] = ref[other, z, kx * 16 : kx * 16 + 16, :]


def final_body(att, gain, w, out):
    pieces = [att[xs * NY + ys] for ys in range(NY) for xs in range(NX)]
    joined = jnp.concatenate(pieces, axis=1)
    proj = lax.dot_general(joined, w[...], (((1,), (1,)), ((), ())), preferred_element_type=F32)
    scale = lax.rsqrt(jnp.mean(proj * proj, axis=-1, keepdims=True) + EPS)
    out[...] = (proj * scale * gain[...]).astype(BF16)


def shards(tokens, norm_gain, w_query, w_key, w_value, w_forget, forget_offset, w_out_t, out_gain):
    sds = jax.ShapeDtypeStruct
    idx = jnp.stack([lax.axis_index(a) for a in AXES]).astype(jnp.int32)

    half, piece, send = sds((32, D), BF16), sds((16, 256), BF16), sds((48, D), BF16)
    rows = jnp.pad(tokens, ((0, 32), (0, 0)))
    for i, w in enumerate((w_query, w_key, w_value, w_out_t)):
        rows = rows + jnp.pad(w, ((64, 16), (256 * i, 768 - 256 * i)))
    rows = rows + jnp.pad(w_forget.T, ((80, 16 - NX), (0, D - 16)))
    lo, hi, p0, o0, *sends = call(
        pack_body,
        (half, half, piece, piece, send, send, send),
        [SMEM, VMEM],
        [pltpu.VMEM((NX, 16, 256), BF16)],
    )(idx, rows)

    got = [shift(sends[k - 1], "x", k) for k in range(1, NX)]
    tok_a = direct(lo, "y")
    chunk, tok_b = call(
        spread_body, (sds((NZ, 128, 256), BF16), sds((128, D), BF16)), [VMEM] * 6
    )(hi, p0, o0, *got)
    w_own = lax.all_to_all(chunk, "z", 0, 0, tiled=True)
    toks_b = gather(tok_b, "y")
    toks = gather(jnp.concatenate(tok_a, axis=0), "x") + toks_b
    w_sib = shift(w_own, "c", 1)

    q_own, kv, cum_own = call(
        project_body,
        (sds((80, KEYS), BF16), sds((128, KEYS), BF16), sds((8, KEYS), F32)),
        [SMEM, SMEM] + [VMEM] * 11,
        [pltpu.VMEM((D, 256), BF16), pltpu.VMEM((KEYS, 256), F32)],
        2e9,
    )(idx, forget_offset, *toks, norm_gain[None], w_own, w_sib)

    q_sib = shift(q_own, "c", 1)
    q, pay = call(
        prepare_body, (sds((128, QS), BF16), sds((PAY, KEYS), BF16)), [SMEM] + [VMEM] * 4
    )(idx, q_own, q_sib, kv, cum_own)

    acc_t, m_t, sums_t = sds((2, 80, QS), F32), sds((2, 8, QS), F32), sds((8, BLK), F32)
    work = [
        pltpu.VMEM((2, KEYS, 128), BF16),
        pltpu.VMEM((2, 80, KEYS), BF16),
        pltpu.VMEM((2, 8, BLK), F32),
        pltpu.VMEM((KEYS, BLK), F32),
        pltpu.VMEM((KEYS, BLK), F32),
        pltpu.VMEM((8, BLK), F32),
        pltpu.VMEM((8, BLK), F32),
        pltpu.VMEM((KEYS, BLK), BF16),
        pltpu.VMEM((KEYS, BLK), BF16),
        pltpu.VMEM((8, BLK), F32),
        pltpu.VMEM((8, BLK), F32),
    ]
    right = step_right(pay, 1)
    left = step_left(pay, 1)
    acc, m, sums = call(
        first_body, (acc_t, m_t, sums_t), [SMEM, VMEM, VMEM], work, 3e9
    )(idx, q, pay)

    w_o = jnp.stack([w_own[:, 64:], w_sib[:, 64:]])
    w_o, _ = lax.optimization_barrier((w_o, sums))
    w_o = direct(w_o, "y")

    for k in range(1, 5):
        pays = (right, left) if k < 4 else (right,)
        if k < 4:
            right = step_right(pays[0], k + 1)
        if k < 3:
            left = step_left(pays[1], k + 1)
        ins = (idx, q) + pays + (acc, m, sums)
        if k < 4:
            outs, scratch, aliases = (acc_t, m_t, sums_t), work, {4: 0, 5: 1}
        else:
            outs, aliases = (sds((72, KEYS), F32), sds((72, KEYS), F32)), None
            scratch = work + [pltpu.VMEM(sums_t.shape, F32)]
        res = call(
            functools.partial(step_body, k),
            outs,
            [SMEM] + [VMEM] * (len(ins) - 1),
            scratch,
            6e9,
            aliases,
        )(*ins)
        if k < 4:
            acc, m, sums = res
    sib = shift(res[1], "c", 1)
    w_full = call(assemble_body, sds((D, D), BF16), [SMEM] + [VMEM] * 4)(idx, *w_o)
    att = call(merge_body, sds((KEYS, HD), BF16), [VMEM, VMEM])(res[0], sib)
    att = lax.all_to_all(att.reshape(16, 64, HD), ("x", "y"), 0, 0, tiled=True)
    return call(final_body, sds((OWN, D), BF16), [VMEM] * 3)(att, out_gain[None], w_full)


def solution(mesh):
    finer = Mesh(mesh.devices.reshape(NZ, NX, NC, NY), AXES)
    sp = ("z", "x", "c")

    return jax.shard_map(
        shards,
        mesh=finer,
        in_specs=(
            P(AXES, None),
            P(),
            P(sp, "y"),
            P(sp, "y"),
            P(sp, "y"),
            P(sp, "y"),
            P("y"),
            P(sp, "y"),
            P(),
        ),
        out_specs=P(AXES, None),
        check_vma=False,
    )
```
